32 devices in a mesh: fs: 4 (over y, x), tp: 8 (over z, core).
Axes of the slice: x: 2, y: 2, z: 4, core: 2. Of those that a mesh axis runs over, the one named last changes fastest.
Arguments:
- value_input: bfloat16 [8192, 2048], P('fs', 'tp'), may hold values from -50 to 50
- value_cotangent: bfloat16 [8192, 512], P('fs'), may hold values from -6 to 6
- value_factor: bfloat16 [512, 128], replicated, may hold values from -10 to 10
- value_master: float32 [512, 2048], P('fs', 'tp'), may hold values from -0.125 to 0.125
- value_first: float32 [128, 2048], P('fs', 'tp'), may hold values from -4 to 4
- value_second: float32 [128, 2048], P('fs', 'tp'), may hold values from 0.01 to 0.2
- mixed_heads: bfloat16 [8192, 1024], P('fs', 'tp'), may hold values from -6 to 6
- output_cotangent: bfloat16 [8192, 2048], P('fs', 'tp'), may hold values from -50 to 50
- output_factor: bfloat16 [1024, 128], replicated, may hold values from -10 to 10
- output_master: float32 [1024, 2048], P('fs', 'tp'), may hold values from -0.1875 to 0.1875
- output_first: float32 [128, 2048], P('fs', 'tp'), may hold values from -4 to 4
- output_second: float32 [128, 2048], P('fs', 'tp'), may hold values from 0.01 to 0.2
Outputs:
- value_step: float32 [512, 2048], P('fs', 'tp')
- value_new_master: float32 [512, 2048], P('fs', 'tp')
- value_copy: bfloat16 [512, 2048], P(None, 'tp')
- value_first_new: float32 [128, 2048], P('fs', 'tp')
- value_second_new: float32 [128, 2048], P('fs', 'tp')
- output_step: float32 [1024, 2048], P('fs', 'tp')
- output_new_master: float32 [1024, 2048], P('fs', 'tp')
- output_copy: bfloat16 [1024, 2048], P(None, 'tp')
- output_first_new: float32 [128, 2048], P('fs', 'tp')
- output_second_new: float32 [128, 2048], P('fs', 'tp')
The draws below stay inside these ranges and needn't reach their ends.
All inputs are finite; a program needn't handle non-finite values.
Results may differ from the reference program's by a relative error of at most 0.001.
Values may be sent and summed in bfloat16 or wider, within the bound.
A program may use at most 64 MiB of HBM per device.

```python
import math
import jax
import jax.numpy as jnp
from jax import lax

D = 2048
RANK = 128
HW = 1024
VW = 512
TOKENS = 8192


def column_scaled(key, rows, cols):
    key_rough, key_own = jax.random.split(key, 2)
    ramp = 10.0 ** (jnp.arange(cols, dtype=jnp.float32) / (cols - 1))
    rough = jnp.exp(jax.random.uniform(key_rough, (cols,), jnp.float32, -0.35, 0.35))
    base = jnp.clip(jax.random.normal(key_own, (rows, cols), jnp.float32), -3.5, 3.5)
    return base * ramp[None, :] * rough[None, :]


def draw_value_input(key, part):
    return column_scaled(jax.random.fold_in(key, 11), TOKENS, D).astype(jnp.bfloat16)


def draw_output_cotangent(key, part):
    return column_scaled(jax.random.fold_in(key, 12), TOKENS, D).astype(jnp.bfloat16)


def draw_value_factor(key, part):
    return (column_scaled(jax.random.fold_in(key, 13), VW, RANK) * VW ** (-0.5)).astype(jnp.bfloat16)


def draw_output_factor(key, part):
    return (column_scaled(jax.random.fold_in(key, 14), HW, RANK) * HW ** (-0.5)).astype(jnp.bfloat16)


def level_of(rng, dims, shards, least, largest):
    gain = 1.0
    for position, parts in shards:
        draws = jax.random.uniform(jax.random.fold_in(jax.random.fold_in(rng, 6), position), (parts,), jnp.float32, least / len(shards), largest / len(shards))
        gain = gain * jnp.repeat(jnp.exp(draws), dims[position] // parts).reshape((-1,) + (1,) * (len(dims) - 1 - position))
    return gain


def scatter_about(own_key, dims, scale, bound, cuts=(), kind=jnp.bfloat16):
    result = jax.random.normal(own_key, dims, jnp.float32) * scale
    if len(cuts) > 0:
        result = level_of(own_key, dims, cuts, -0.22, 0.18) * result
    return jnp.clip(result, min=-bound, max=bound).astype(kind)


def setup_inputs(seed: int = 0) -> dict:
    splits = jax.random.split(jax.random.key(seed), 13)
    value_input = draw_value_input(jax.random.fold_in(splits[12], 71), 0)
    value_cotangent = scatter_about(splits[1], (TOKENS, VW), 1.0, 6.0, ((0, 4),))
    value_factor = draw_value_factor(jax.random.fold_in(splits[12], 71), 0)
    value_master = scatter_about(splits[3], (VW, D), D ** -0.5, 0.125, ((0, 4), (1, 8)), jnp.float32)
    value_first = scatter_about(splits[4], (RANK, D), 0.3, 4.0, ((0, 4), (1, 8)), jnp.float32)
    value_second = jnp.clip(jnp.exp(math.log(0.2) - 2.9957323 * jax.random.uniform(splits[5], (RANK, D), jnp.float32) ** level_of(splits[5], (RANK, D), ((0, 4), (1, 8)), -0.2, 0.2)), 0.01, 0.2)
    mixed_heads = scatter_about(splits[6], (TOKENS, HW), 1.0, 6.0, ((0, 4), (1, 8)))
    output_cotangent = draw_output_cotangent(jax.random.fold_in(splits[12], 71), 0)
    output_factor = draw_output_factor(jax.random.fold_in(splits[12], 71), 0)
    output_master = scatter_about(splits[9], (HW, D), HW ** -0.5, 0.1875, ((0, 4), (1, 8)), jnp.float32)
    output_first = scatter_about(splits[10], (RANK, D), 0.3, 4.0, ((0, 4), (1, 8)), jnp.float32)
    output_second = jnp.clip(jnp.exp(math.log(0.2) - 2.9957323 * jax.random.uniform(splits[11], (RANK, D), jnp.float32) ** level_of(splits[11], (RANK, D), ((0, 4), (1, 8)), -0.2, 0.2)), 0.01, 0.2)
    return {"value_input": value_input, "value_cotangent": value_cotangent, "value_factor": value_factor, "value_master": value_master, "value_first": value_first, "value_second": value_second, "mixed_heads": mixed_heads, "output_cotangent": output_cotangent, "output_factor": output_factor, "output_master": output_master, "output_first": output_first, "output_second": output_second}


highest = lax.Precision.HIGHEST

def adam_part(projected, first, second, factor, master):
    scale = lax.rsqrt(jnp.mean(projected * projected) + 1e-06)
    scaled = scale * projected
    first_new = 0.9 * first + 0.1 * scaled
    second_new = 0.95 * second + 0.05 * scaled * scaled
    direction = first_new / (jnp.sqrt(second_new) + 1e-08)
    step = jnp.dot(factor.astype(jnp.float32), direction, precision=highest, preferred_element_type=jnp.float32)
    new_master = master - 0.002 * step
    return (step, new_master, new_master.astype(jnp.bfloat16), first_new, second_new)

def reference(value_input, value_cotangent, value_factor, value_master, value_first, value_second, mixed_heads, output_cotangent, output_factor, output_master, output_first, output_second):
    value_image = jnp.dot(value_cotangent.astype(jnp.float32), value_factor.astype(jnp.float32), precision=highest, preferred_element_type=jnp.float32)
    value_projected = jnp.dot(value_image.T, value_input.astype(jnp.float32), precision=highest, preferred_element_type=jnp.float32)
    output_image = jnp.dot(mixed_heads.astype(jnp.float32), output_factor.astype(jnp.float32), precision=highest, preferred_element_type=jnp.float32)
    output_projected = jnp.dot(output_image.T, output_cotangent.astype(jnp.float32), precision=highest, preferred_element_type=jnp.float32)
    value_out = adam_part(value_projected, value_first, value_second, value_factor, value_master)
    output_out = adam_part(output_projected, output_first, output_second, output_factor, output_master)
    return (value_out[0], value_out[1], value_out[2], value_out[3], value_out[4], output_out[0], output_out[1], output_out[2], output_out[3], output_out[4])
```

```python
import functools

import jax
import jax.numpy as jnp
from jax import lax
from jax.experimental import pallas as pl
from jax.experimental.pallas import tpu as pltpu
from jax.sharding import PartitionSpec as P

MESH = pl.DeviceIdType.MESH
ANY = pl.BlockSpec(memory_space=pl.ANY)
HBM = pl.BlockSpec(memory_space=pltpu.HBM)
VMEM = pl.BlockSpec(memory_space=pltpu.VMEM)
BF16 = jnp.bfloat16
F32 = jnp.float32
HOP = 4
POWER = 15
PEAK = 256.0
SCALE_ROWS = 16
PIECES = 4


def split(wide, axis):
    high = wide.astype(BF16)
    low = (wide - high.astype(F32)).astype(BF16)
    return jnp.concatenate([high, low], axis=axis)


def encode(x):
    top = jnp.max(jnp.abs(x), axis=0, keepdims=True)
    top = jnp.maximum(top * 1.01, 1e-30).astype(BF16)
    u = x * (PEAK / top.astype(F32))
    u3 = u * u * u
    u5 = u3 * u * u
    return (u5 * u5 * u5).astype(BF16), jnp.broadcast_to(top, (SCALE_ROWS, x.shape[1]))


def decode(ref, rows):
    y = ref[:rows, :].astype(F32)
    top = ref[rows:, :].astype(F32)[0:1, :]
    size = jnp.abs(y)
    root = jnp.exp(jnp.log(jnp.maximum(size, 1e-37)) * (1.0 / POWER))
    root = jnp.where(size < 2e-37, 0.0, root) * (top * (1.0 / PEAK))
    return jnp.where(y < 0.0, -root, root)


def gather_kernel(
    fs, tp,
    vin, vcot, vfac, vmas, vm1, vm2, heads, ocot, ofac, omas, om1, om2,
    o_all, o1_all, o2_all, om_all, totals, v_step, v_new, v_copy, v_first, v_second,
    vfac_v, ofac_v, vin_v, vcot_v, heads_v, heads_in, ocot_v, ocot_in, v1_v, v2_v, vm_v,
    own_v, left_v, right_v, pre_in, pre_out, suf_in, suf_out, acc_own, acc_pair, pair_out, pair_in,
    partial, partial_in, band_v, dir_all, first_sums, second_sums, all_sums,
    load_sem, heads_send, heads_recv, ocot_send, ocot_recv, pre_send, pre_recv, suf_send, suf_recv,
    pair_send, pair_recv, rs_send, rs_recv, all_send, all_recv, s1_send, s1_recv, s2_send, s2_recv,
    so_send, so_recv, mom_send, mom_recv, mas_send, mas_recv, copy_send, copy_recv,
):
    f = lax.axis_index("fs")
    t = lax.axis_index("tp")
    chip = t // 2
    core = t % 2
    chips = tp // 2
    last = chips - 1
    partner = {"tp": chip * 2 + (1 - core)}
    rank = vfac.shape[1]
    band = rank // fs
    tokens, width = heads.shape
    columns = vin.shape[1]
    half = tokens // 2
    blocks, _, block = own_v.shape
    mine_at = pl.multiple_of(core * half, half)
    pair_at = pl.multiple_of((1 - core) * half, half)

    def fs_peer(j):
        return lax.rem(f + j, fs)

    def tp_peer(j):
        return lax.rem(t + j, tp)

    def own_rows(ref):
        rows = ref.shape[0] // fs
        return ref.at[pl.ds(pl.multiple_of(f * rows, rows), rows)]

    jobs = [
        (heads.at[pl.ds(pair_at, half)], heads_v.at[pl.ds(pair_at, half)]),
        (ofac, ofac_v),
        (heads.at[pl.ds(mine_at, half)], heads_v.at[pl.ds(mine_at, half)]),
        (om1, own_rows(o1_all)), (om2, own_rows(o2_all)),
        (vfac, vfac_v), (vcot, vcot_v), (vin, vin_v),
        (ocot.at[pl.ds(pair_at, half)], ocot_v.at[pl.ds(pair_at, half)]),
        (ocot.at[pl.ds(mine_at, half)], ocot_v.at[pl.ds(mine_at, half)]),
        (omas, own_rows(om_all)),
        (vmas, vm_v), (vm1, v1_v), (vm2, v2_v),
    ]
    loads = [pltpu.make_async_copy(a, b, load_sem.at[i]) for i, (a, b) in enumerate(jobs)]
    for load in loads:
        load.start()

    barrier = pltpu.get_barrier_semaphore()
    for j in range(1, tp):
        pl.semaphore_signal(barrier, inc=1, device_id={"tp": tp_peer(j)}, device_id_type=MESH)
    for j in range(1, fs):
        pl.semaphore_signal(barrier, inc=1, device_id={"fs": fs_peer(j)}, device_id_type=MESH)
    pl.semaphore_wait(barrier, tp + fs - 2)

    sent = []

    def remote(src, dst, send_sem, recv_sem, where):
        return pltpu.make_async_remote_copy(
            src_ref=src, dst_ref=dst, send_sem=send_sem, recv_sem=recv_sem,
            device_id=where, device_id_type=MESH,
        )

    def send(src, dst, send_sem, recv_sem, where):
        copy = remote(src, dst, send_sem, recv_sem, where)
        copy.start()
        sent.append(copy)

    def landed(dst, send_sem, recv_sem, where):
        remote(dst, dst, send_sem, recv_sem, where).wait_recv()

    loads[0].wait()
    send(heads_v.at[pl.ds(pair_at, half)], heads_in, heads_send, heads_recv, partner)
    for i, whole in ((0, o1_all), (1, o2_all)):
        loads[3 + i].wait()
        here = own_rows(whole)
        for j in range(1, fs):
            send(here, here, mom_send.at[i, j], mom_recv.at[i, f], {"fs": fs_peer(j)})

    loads[5].wait()
    loads[6].wait()
    loads[7].wait()
    total = jnp.zeros((2 * rank, columns), F32)
    stride = 256 if tokens % 256 == 0 else tokens
    for i in range(tokens // stride):
        rows = pl.ds(i * stride, stride)
        image = jnp.dot(vcot_v[rows, :], vfac_v[...], preferred_element_type=F32)
        total = total + lax.dot_general(
            split(image, 1), vin_v[rows, :], (((0,), (0,)), ((), ())), preferred_element_type=F32
        )

    def scatter(k, whole):
        partial[k] = whole.reshape(fs, band, columns)
        for j in range(1, fs):
            d = fs_peer(j)
            send(partial.at[k, d], partial_in.at[k, f], rs_send.at[k, j], rs_recv.at[k, f], {"fs": d})

    def reduce(k):
        mine = partial[k, f]
        for j in range(1, fs):
            d = fs_peer(j)
            landed(partial_in.at[k, d], rs_send.at[k, j], rs_recv.at[k, d], {"fs": d})
            mine = mine + partial_in[k, d]
        return mine

    scatter(0, total[:rank] + total[rank:])

    loads[8].wait()
    send(ocot_v.at[pl.ds(pair_at, half)], ocot_in, ocot_send, ocot_recv, partner)

    loads[1].wait()
    loads[2].wait()

    def factor_of(s):
        rows = ofac_v[pl.ds(pl.multiple_of(s * width, width), width), :]
        return rows.astype(F32).T.astype(BF16)

    def against(left, right):
        return lax.dot_general(left, right, (((1,), (1,)), ((), ())), preferred_element_type=F32)

    factor_mine = factor_of(t)
    factor_pair = factor_of(chip * 2 + (1 - core))
    landed(heads_in, heads_send, heads_recv, partner)
    for k in range(blocks):
        here = heads_v[pl.ds(pl.multiple_of(mine_at + k * block, block), block), :]
        own_v[k] = against(factor_mine, here) + against(factor_pair, heads_in[pl.ds(k * block, block), :])
    acc_own[...] = jnp.zeros_like(acc_own)
    acc_pair[...] = jnp.zeros_like(acc_pair)
    loads[9].wait()
    landed(ocot_in, ocot_send, ocot_recv, partner)

    def to_right(k):
        return remote(pre_out.at[k], pre_in.at[k], pre_send.at[k], pre_recv.at[k], {"tp": lax.rem(t + 2, tp)})

    def to_left(k):
        return remote(suf_out.at[k], suf_in.at[k], suf_send.at[k], suf_recv.at[k], {"tp": lax.rem(t + tp - 2, tp)})

    def pack(ref, x):
        coded, top = encode(x)
        ref[:rank, :] = coded
        ref[rank:, :] = top

    def step(i, _):
        k = i - HOP * chip

        @pl.when((k >= 0) & (k < blocks))
        def _():
            @pl.when(chip > 0)
            def _():
                to_right(k).wait_recv()
                left_v[k] = decode(pre_in.at[k], rank)

            @pl.when(chip == 0)
            def _():
                left_v[k] = jnp.zeros((rank, block), F32)

            @pl.when(chip < last)
            def _():
                pack(pre_out.at[k], left_v[k] + own_v[k])
                to_right(k).start()

        m = i - HOP * (last - chip)

        @pl.when((m >= 0) & (m < blocks))
        def _():
            @pl.when(chip < last)
            def _():
                to_left(m).wait_recv()
                right_v[m] = decode(suf_in.at[m], rank)

            @pl.when(chip == last)
            def _():
                right_v[m] = jnp.zeros((rank, block), F32)

            @pl.when(chip > 0)
            def _():
                pack(suf_out.at[m], right_v[m] + own_v[m])
                to_left(m).start()

        n = i - HOP * jnp.maximum(chip, last - chip)

        @pl.when((n >= 0) & (n < blocks))
        def _():
            two = split(left_v[n] + own_v[n] + right_v[n], 0)
            here = pl.ds(pl.multiple_of(mine_at + n * block, block), block)
            there = pl.ds(pl.multiple_of(n * block, block), block)
            acc_own[...] += jnp.dot(two, ocot_v[here, :], preferred_element_type=F32)
            acc_pair[...] += jnp.dot(two, ocot_in[there, :], preferred_element_type=F32)

        return 0

    masters = own_rows(om_all)
    piece = masters.shape[0] // PIECES

    def send_masters(i):
        if i == 0:
            loads[10].wait()
        here = masters.at[pl.ds(i * piece, piece)]
        for j in range(1, fs):
            send(here, here, mas_send.at[i, j], mas_recv.at[i, f], {"fs": fs_peer(j)})

    def value_sums():
        mine = reduce(0)
        band_v[0] = mine
        first_sums[f] = jnp.full((1, 128), jnp.sum(mine * mine), F32)
        for j in range(1, fs):
            send(first_sums.at[f], first_sums.at[f], s1_send.at[j], s1_recv.at[f], {"fs": fs_peer(j)})

    def value_sums_on():
        mine = first_sums[f]
        for j in range(1, fs):
            d = fs_peer(j)
            landed(first_sums.at[d], s1_send.at[j], s1_recv.at[d], {"fs": d})
            mine = mine + first_sums[d]
        second_sums[t] = mine
        for j in range(1, tp):
            send(second_sums.at[t], second_sums.at[t], s2_send.at[j], s2_recv.at[t], {"tp": tp_peer(j)})

    def value_direction():
        mine = second_sums[t]
        for j in range(1, tp):
            d = tp_peer(j)
            landed(second_sums.at[d], s2_send.at[j], s2_recv.at[d], {"tp": d})
            mine = mine + second_sums[d]
        scale = lax.rsqrt(mine[0:1, 0:1] / (rank * columns * tp) + 1e-06)
        for i in (12, 13):
            loads[i].wait()
        scaled = scale * band_v[0]
        first_new = 0.9 * v1_v[...] + 0.1 * scaled
        second_new = 0.95 * v2_v[...] + 0.05 * scaled * scaled
        v_first[...] = first_new
        v_second[...] = second_new
        dir_all[f] = first_new / (jnp.sqrt(second_new) + 1e-08)
        for j in range(1, fs):
            send(dir_all.at[f], dir_all.at[f], all_send.at[0, j], all_recv.at[0, f], {"fs": fs_peer(j)})

    def value_finish():
        for j in range(1, fs):
            d = fs_peer(j)
            landed(dir_all.at[d], all_send.at[0, j], all_recv.at[0, d], {"fs": d})
        direction = split(dir_all[...].reshape(rank, columns), 0)
        count = v_step.shape[0]
        left = vfac_v[pl.ds(pl.multiple_of(f * count, count), count), :]
        move = jnp.dot(jnp.concatenate([left, left], axis=1), direction, preferred_element_type=F32)
        loads[11].wait()
        fresh = vm_v[...] - 0.002 * move
        v_step[...] = move
        v_new[...] = fresh
        here = own_rows(v_copy)
        here[...] = fresh.astype(BF16)
        for j in range(1, fs):
            send(here, here, copy_send.at[j], copy_recv.at[f], {"fs": fs_peer(j)})

    steps = blocks + HOP * last
    events = [(0, functools.partial(send_masters, 0))]
    plan = (
        (4, functools.partial(send_masters, 1)), (6, value_sums), (8, functools.partial(send_masters, 2)),
        (10, value_sums_on), (12, functools.partial(send_masters, 3)), (16, value_direction),
    )
    done = 0
    for at, event in events + list(plan):
        at = min(at, steps)
        if at > done:
            lax.fori_loop(done, at, step, 0)
            done = at
        event()
    lax.fori_loop(done, steps, step, 0)

    pair_out[...] = acc_pair[:rank, :] + acc_pair[rank:, :]
    send(pair_out, pair_in, pair_send, pair_recv, partner)
    mine = acc_own[:rank, :] + acc_own[rank:, :]
    landed(pair_in, pair_send, pair_recv, partner)
    scatter(1, mine + pair_in[...])

    value_finish()

    mine = reduce(1)
    o_all[f] = mine
    me = f * tp + t
    count = fs * tp
    all_sums[me] = jnp.full((1, 128), jnp.sum(mine * mine), F32)

    def spread(j):
        d = lax.rem(me + j, count)
        return remote(all_sums.at[me], all_sums.at[me], so_send.at[j], so_recv.at[me], {"fs": d // tp, "tp": d % tp})

    def spread_start(j, _):
        spread(j).start()
        return 0

    lax.fori_loop(1, count, spread_start, 0)
    for j in range(1, fs):
        send(o_all.at[f], o_all.at[f], all_send.at[1, j], all_recv.at[1, f], {"fs": fs_peer(j)})

    for j in range(1, fs):
        d = fs_peer(j)
        landed(o_all.at[d], all_send.at[1, j], all_recv.at[1, d], {"fs": d})
        for i, whole in ((0, o1_all), (1, o2_all)):
            there = whole.at[pl.ds(pl.multiple_of(d * band, band), band)]
            landed(there, mom_send.at[i, j], mom_recv.at[i, d], {"fs": d})
        for i in range(PIECES):
            there = om_all.at[pl.ds(pl.multiple_of(d * PIECES * piece + i * piece, piece), piece)]
            landed(there, mas_send.at[i, j], mas_recv.at[i, d], {"fs": d})
        rows = v_step.shape[0]
        there = v_copy.at[pl.ds(pl.multiple_of(d * rows, rows), rows)]
        landed(there, copy_send.at[j], copy_recv.at[d], {"fs": d})

    def spread_end(j, _):
        d = lax.rem(me + j, count)
        remote(all_sums.at[d], all_sums.at[d], so_send.at[j], so_recv.at[d], {"fs": d // tp, "tp": d % tp}).wait_recv()
        spread(j).wait_send()
        return 0

    lax.fori_loop(1, count, spread_end, 0)
    totals[...] = jnp.sum(all_sums[...], axis=0)

    def drain(k, _):
        @pl.when(chip < last)
        def _():
            to_right(k).wait_send()

        @pl.when(chip > 0)
        def _():
            to_left(k).wait_send()

        return 0

    lax.fori_loop(0, blocks, drain, 0)
    for copy in sent:
        copy.wait_send()


def finish_kernel(
    fs, tp,
    o_all, o1_all, o2_all, om_all, totals, ofac, v_step, v_new, v_copy, v_first, v_second,
    v_step_out, v_new_out, v_copy_out, v_first_out, v_second_out,
    o_step_out, o_new_out, o_copy_out, o_first_out, o_second_out,
    step_v, new_v, copy_v, first_v, second_v, out_sem,
):
    f = lax.axis_index("fs")
    puts = []

    def put(src, dst):
        copy = pltpu.make_async_copy(src, dst, out_sem.at[len(puts)])
        copy.start()
        puts.append(copy)

    for src, dst in (
        (v_step, v_step_out), (v_new, v_new_out), (v_copy, v_copy_out), (v_first, v_first_out), (v_second, v_second_out),
    ):
        put(src, dst)
    rank, columns = o1_all.shape
    band = rank // fs
    scale = lax.rsqrt(totals[0:1, 0:1] / (rank * columns * tp) + 1e-06)

    def moments(proj, rows):
        scaled = scale * proj
        first_new = 0.9 * o1_all[rows, :] + 0.1 * scaled
        second_new = 0.95 * o2_all[rows, :] + 0.05 * scaled * scaled
        return first_new, second_new

    first_v[...], second_v[...] = moments(o_all[f], pl.ds(pl.multiple_of(f * band, band), band))
    put(first_v, o_first_out)
    put(second_v, o_second_out)
    first_new, second_new = moments(o_all[...].reshape(rank, columns), pl.ds(0, rank))
    direction = split(first_new / (jnp.sqrt(second_new) + 1e-08), 0)

    def step_of(rows):
        left = ofac[rows, :]
        return jnp.dot(jnp.concatenate([left, left], axis=1), direction, preferred_element_type=F32)

    count = step_v.shape[0]
    own = pl.ds(pl.multiple_of(f * count, count), count)
    move = step_of(own)
    step_v[...] = move
    put(step_v, o_step_out)
    new_v[...] = om_all[own, :] - 0.002 * move
    put(new_v, o_new_out)
    for i in range(fs):
        rows = pl.ds(i * count, count)
        copy_v[rows, :] = (om_all[rows, :] - 0.002 * step_of(rows)).astype(BF16)
        put(copy_v.at[rows], o_copy_out.at[rows])
    for copy in puts:
        copy.wait()


def on_device(vin, vcot, vfac, vmas, vm1, vm2, heads, ocot, ofac, omas, om1, om2):
    fs = lax.axis_size("fs")
    tp = lax.axis_size("tp")
    rank = vfac.shape[1]
    band = rank // fs
    columns = vin.shape[1]
    tokens, width = heads.shape
    half = tokens // 2
    block = 128 if half % 128 == 0 else half
    blocks = half // block

    def like(array):
        return pltpu.VMEM(array.shape, array.dtype)

    def shape(*dims, kind=F32):
        return jax.ShapeDtypeStruct(dims, kind)

    def wide(*dims):
        return pltpu.VMEM(dims, F32)

    def coded():
        return pltpu.VMEM((blocks, rank + SCALE_ROWS, block), BF16)

    dma = pltpu.SemaphoreType.DMA
    v_rows, o_rows = vmas.shape[0], omas.shape[0]
    gathered = pl.pallas_call(
        functools.partial(gather_kernel, fs, tp),
        out_shape=(
            shape(fs, band, columns), shape(rank, columns), shape(rank, columns), shape(fs * o_rows, columns),
            shape(1, 128),
            shape(v_rows, columns), shape(v_rows, columns), shape(fs * v_rows, columns, kind=BF16),
            shape(band, columns), shape(band, columns),
        ),
        in_specs=[HBM] * 12,
        out_specs=(VMEM,) * 10,
        scratch_shapes=[
            like(vfac), like(ofac), like(vin), like(vcot), like(heads), pltpu.VMEM((half, width), BF16),
            like(ocot), pltpu.VMEM((half, columns), BF16), like(vm1), like(vm2), like(vmas),
            wide(blocks, rank, block), wide(blocks, rank, block), wide(blocks, rank, block),
            coded(), coded(), coded(), coded(),
            wide(2 * rank, columns), wide(2 * rank, columns), wide(rank, columns), wide(rank, columns),
            wide(2, fs, band, columns), wide(2, fs, band, columns), wide(1, band, columns),
            wide(fs, band, columns), wide(fs, 1, 128), wide(tp, 1, 128), wide(fs * tp, 1, 128),
            dma((14,)), dma, dma, dma, dma, dma((blocks,)), dma((blocks,)), dma((blocks,)), dma((blocks,)),
            dma, dma, dma((2, fs)), dma((2, fs)), dma((2, fs)), dma((2, fs)), dma((fs,)), dma((fs,)),
            dma((tp,)), dma((tp,)), dma((fs * tp,)), dma((fs * tp,)), dma((2, fs)), dma((2, fs)),
            dma((PIECES, fs)), dma((PIECES, fs)), dma((fs,)), dma((fs,)),
        ],
        compiler_params=pltpu.CompilerParams(
            collective_id=0, has_side_effects=True, vmem_limit_bytes=24 * 1024 * 1024
        ),
    )(*(pltpu.with_memory_space_constraint(a, pltpu.HBM) for a in (
        vin, vcot, vfac, vmas, vm1, vm2, heads, ocot, ofac, omas, om1, om2
    )))
    o_all, o1_all, o2_all, om_all, totals, *values = gathered

    return pl.pallas_call(
        functools.partial(finish_kernel, fs, tp),
        out_shape=(
            shape(v_rows, columns), shape(v_rows, columns), shape(fs * v_rows, columns, kind=BF16),
            shape(band, columns), shape(band, columns),
            shape(o_rows, columns), shape(o_rows, columns), shape(fs * o_rows, columns, kind=BF16),
            shape(band, columns), shape(band, columns),
        ),
        in_specs=[VMEM] * 11,
        out_specs=(HBM,) * 10,
        scratch_shapes=[
            wide(o_rows, columns), wide(o_rows, columns), pltpu.VMEM((fs * o_rows, columns), BF16),
            wide(band, columns), wide(band, columns), dma((9 + fs,)),
        ],
        compiler_params=pltpu.CompilerParams(vmem_limit_bytes=24 * 1024 * 1024),
    )(o_all, o1_all, o2_all, om_all, totals, ofac, *values)


def solution(mesh):
    both = P("fs", "tp")
    in_specs = (both, P("fs", None), P(), both, both, both, both, both, P(), both, both, both)
    out_specs = (
        both, both, P(None, "tp"), both, both, both, both, P(None, "tp"), both, both,
    )
    return jax.shard_map(
        on_device, mesh=mesh, in_specs=in_specs, out_specs=out_specs, check_vma=False
    )
```

```python
import functools

import jax
import jax.numpy as jnp
from jax import lax
from jax.experimental import pallas as pl
from jax.experimental.pallas import tpu as pltpu
from jax.sharding import PartitionSpec as P

MESH = pl.DeviceIdType.MESH
ANY = pl.BlockSpec(memory_space=pl.ANY)
HBM = pl.BlockSpec(memory_space=pltpu.HBM)
VMEM = pl.BlockSpec(memory_space=pltpu.VMEM)
BF16 = jnp.bfloat16
F32 = jnp.float32
PRE = 3
SUF = 4
LEVELS = 252.0
POWER = 15
PEAK = 320.0


def split(wide, axis):
    high = wide.astype(BF16)
    low = (wide - high.astype(F32)).astype(BF16)
    return jnp.concatenate([high, low], axis=axis)


def encode(x, top):
    u = x * (PEAK / top)
    u3 = u * u * u
    u5 = u3 * u * u
    return (u5 * u5 * u5).astype(BF16)


def decode(coded, top):
    y = coded.astype(F32)
    size = jnp.abs(y)
    root = jnp.exp(jnp.log(jnp.maximum(size, 1e-37)) * (1.0 / POWER))
    root = jnp.where(size < 2e-37, 0.0, root) * (top * (1.0 / PEAK))
    return jnp.where(y < 0.0, -root, root)


def encode_even(x, top):
    size = jnp.exp2(jnp.abs(x) * (LEVELS / top) - LEVELS / 2)
    return jnp.where(x < 0.0, -size, size).astype(BF16)


def decode_even(coded, top):
    y = coded.astype(F32)
    size = (jnp.log2(jnp.maximum(jnp.abs(y), 1e-38)) + LEVELS / 2) * (top * (1.0 / LEVELS))
    return jnp.where(y < 0.0, -size, size)


def top_of(x):
    return jnp.max(jnp.abs(x), axis=0, keepdims=True) * 1.02 + 1e-30


def gather_kernel(
    fs, tp,
    vin, vcot, vfac, vmas, vm1, vm2, heads, ocot, ofac, omas, om1, om2,
    o_all, o1_all, o2_all, om_all, totals, v_step, v_new, v_copy, v_first, v_second,
    vfac_v, ofac_v, vin_v, vcot_v, heads_v, heads_in, ocot_v, ocot_in, v1_v, v2_v, vm_v, om_v,
    own_v, left_v, right_v, pre_in, pre_out, suf_in, suf_out, tops, acc_own, acc_pair, pair_out, pair_in,
    swap, swap_top, proj_v, dir_all, sums, mas, mas_top,
    load_sem, heads_send, heads_recv, ocot_send, ocot_recv, pre_send, pre_recv, suf_send, suf_recv, tops_send, tops_recv,
    pair_send, pair_recv, swap_send, swap_recv, mark_send, mark_recv, dir_send, dir_recv, sum_send, sum_recv,
    mom_send, mom_recv, mas_send, mas_recv, mast_send, mast_recv, copy_send, copy_recv,
):
    f = lax.axis_index("fs")
    t = lax.axis_index("tp")
    chip = t // 2
    core = t % 2
    chips = tp // 2
    last = chips - 1
    rank = vfac.shape[1]
    band = rank // fs
    tokens, width = heads.shape
    columns = vin.shape[1]
    half = tokens // 2
    blocks, part, block = own_v.shape
    both = rank // part
    o_rows = omas.shape[0]
    mine_at = pl.multiple_of(core * half, half)
    pair_at = pl.multiple_of((1 - core) * half, half)
    scope = jax.named_scope

    fs_peers = [3 - f, f + 1 - 2 * (f % 2), lax.rem(f + 2, fs)] if fs == 4 else [lax.rem(f + j, fs) for j in range(1, fs)]

    def tp_peer(j):
        return lax.rem(t + j, tp)

    def own_rows(ref):
        rows = ref.shape[0] // fs
        return ref.at[pl.ds(pl.multiple_of(f * rows, rows), rows)]

    jobs = [
        (heads.at[pl.ds(pair_at, half)], heads_v.at[pl.ds(pair_at, half)]),
        (ofac, ofac_v),
        (heads.at[pl.ds(mine_at, half)], heads_v.at[pl.ds(mine_at, half)]),
        (om1, own_rows(o1_all)), (om2, own_rows(o2_all)),
        (vfac, vfac_v), (vcot, vcot_v), (vin, vin_v), (omas, om_v),
        (ocot.at[pl.ds(pair_at, half)], ocot_v.at[pl.ds(pair_at, half)]),
        (ocot.at[pl.ds(mine_at, half)], ocot_v.at[pl.ds(mine_at, half)]),
        (vmas, vm_v), (vm1, v1_v), (vm2, v2_v),
    ]
    loads = [pltpu.make_async_copy(a, b, load_sem.at[i]) for i, (a, b) in enumerate(jobs)]
    for load in loads:
        load.start()

    partner = {"tp": chip * 2 + (1 - core)}
    right = {"tp": lax.rem(t + 2, tp)}
    left = {"tp": lax.rem(t + tp - 2, tp)}
    barrier = pltpu.get_barrier_semaphore()

    def greet(where):
        pl.semaphore_signal(barrier, inc=1, device_id=where, device_id_type=MESH)

    greet(partner)
    for d in fs_peers:
        greet({"fs": d})

    @pl.when(chip > 0)
    def _():
        greet(left)

    @pl.when(chip < last)
    def _():
        greet(right)

    with scope("barrier"):
        pl.semaphore_wait(barrier, fs + (chip + last) // chips + (last - chip + last) // chips)

    def remote(src, dst, send_sem, recv_sem, where):
        return pltpu.make_async_remote_copy(
            src_ref=src, dst_ref=dst, send_sem=send_sem, recv_sem=recv_sem,
            device_id=where, device_id_type=MESH,
        )

    def send(src, dst, send_sem, recv_sem, where):
        remote(src, dst, send_sem, recv_sem, where).start()

    def landed(dst, sem):
        remote(dst, dst, sem, sem, partner).wait_recv()

    def left_here(src, sem):
        remote(src, src, sem, sem, partner).wait_send()

    with scope("heads_load"):
        loads[0].wait()
    send(heads_v.at[pl.ds(pair_at, half)], heads_in, heads_send, heads_recv, partner)
    for i, whole in ((3, o1_all), (4, o2_all)):
        loads[i].wait()
        here = own_rows(whole)
        for d in fs_peers:
            send(here, here, mom_send, mom_recv, {"fs": d})


    def masters_send(start, rows):
        here = mas.at[f, pl.ds(start, rows)]
        for d in fs_peers:
            send(here, here, mas_send, mas_recv, {"fs": d})

    def masters_first():
        loads[8].wait()
        top = top_of(om_v[...])
        mas_top[f] = top
        mas[f] = encode_even(om_v[...], top)
        for d in fs_peers:
            send(mas_top.at[f], mas_top.at[f], mast_send, mast_recv, {"fs": d})
        masters_send(0, o_rows)

    def masters_end():
        landed(mas_top.at[pl.ds(0, fs - 1)], mast_recv)
        landed(mas.at[pl.ds(0, fs - 1)], mas_recv)
        for g in range(fs):
            om_all[pl.ds(g * o_rows, o_rows), :] = decode_even(mas[g], mas_top[g])

    with scope("factor_load"):
        loads[1].wait()
        loads[2].wait()

    def factor_of(s):
        rows = ofac_v[pl.ds(pl.multiple_of(s * width, width), width), :]
        return rows.astype(F32).T.astype(BF16)

    def against(left, right):
        return lax.dot_general(left, right, (((1,), (1,)), ((), ())), preferred_element_type=F32)

    def to_right(k):
        return remote(pre_out.at[k], pre_in.at[k], pre_send, pre_recv.at[k], right)

    def to_left(k):
        return remote(suf_out.at[k], suf_in.at[k], suf_send, suf_recv.at[k], left)

    def top_right(top):
        tops[3] = top
        send(tops.at[3], tops.at[1], tops_send.at[0], tops_recv.at[0], right)

    def top_left(top):
        tops[4] = top
        send(tops.at[4], tops.at[2], tops_send.at[1], tops_recv.at[1], left)

    factor_mine = factor_of(t)
    factor_pair = factor_of(chip * 2 + (1 - core))
    with scope("heads_in"):
        landed(heads_in, heads_recv)
    with scope("own"):
        top = jnp.zeros((rank, block), F32)
        for k in range(half // block):
            here = heads_v[pl.ds(pl.multiple_of(mine_at + k * block, block), block), :]
            own = against(factor_mine, here) + against(factor_pair, heads_in[pl.ds(k * block, block), :])
            top = jnp.maximum(top, jnp.abs(own))
            own_v[pl.ds(k * both, both)] = own.reshape(both, part, block)
        top = top_of(top)
        tops[0] = top

    @pl.when(chip == 0)
    def _():
        top_right(top)
        left_v[...] = jnp.zeros_like(left_v)

        def first(k, _):
            pre_out[k] = encode(own_v[k], tops[3])
            to_right(k).start()
            return 0

        lax.fori_loop(0, blocks, first, 0)

    @pl.when(chip == last)
    def _():
        top_left(top)
        right_v[...] = jnp.zeros_like(right_v)

        def first(k, _):
            suf_out[k] = encode(own_v[k], tops[4])
            to_left(k).start()
            return 0

        lax.fori_loop(0, blocks, first, 0)

    with scope("ocot_load"):
        loads[9].wait()
        loads[10].wait()
    send(ocot_v.at[pl.ds(pair_at, half)], ocot_in, ocot_send, ocot_recv, partner)

    def exchange(k, mine):
        top = top_of(mine)
        swap_top[k, f] = top
        swap[k, f] = encode(mine, top)
        for d in fs_peers:
            send(swap_top.at[k, f], swap_top.at[k, f], mark_send.at[k], mark_recv.at[k], {"fs": d})
            send(swap.at[k, f], swap.at[k, f], swap_send.at[k], swap_recv.at[k], {"fs": d})

    def exchanged(k):
        landed(swap_top.at[k, pl.ds(0, fs - 1)], mark_recv.at[k])
        landed(swap.at[k, pl.ds(0, fs - 1)], swap_recv.at[k])
        whole = decode(swap[k, 0], swap_top[k, 0])
        for g in range(1, fs):
            whole = whole + decode(swap[k, g], swap_top[k, g])
        return whole

    def sum_out(k, whole):
        sums[k, t] = jnp.sum(whole * whole, axis=0, keepdims=True)
        for j in range(1, tp):
            send(sums.at[k, t], sums.at[k, t], sum_send.at[k], sum_recv.at[k], {"tp": tp_peer(j)})

    def sum_in(k):
        landed(sums.at[k, pl.ds(0, tp - 1)], sum_recv.at[k])
        return jnp.sum(sums[k], axis=0)

    with scope("value_load"):
        for i in (5, 6, 7):
            loads[i].wait()
    with scope("value_compute"):
        total = jnp.zeros((2 * rank, columns), F32)
        stride = 256 if tokens % 256 == 0 else tokens
        for i in range(tokens // stride):
            rows = pl.ds(i * stride, stride)
            image = jnp.dot(vcot_v[rows, :], vfac_v[...], preferred_element_type=F32)
            total = total + lax.dot_general(
                split(image, 1), vin_v[rows, :], (((0,), (0,)), ((), ())), preferred_element_type=F32
            )
        exchange(0, total[:rank] + total[rank:])
    with scope("masters_first"):
        masters_first()
    with scope("ocot_in"):
        landed(ocot_in, ocot_recv)
    acc_own[...] = jnp.zeros_like(acc_own)
    acc_pair[...] = jnp.zeros_like(acc_pair)

    def step(i, _):
        k = i - PRE * chip

        @pl.when((chip > 0) & (k >= 0) & (k < blocks))
        def _():
            @pl.when(k == 0)
            def _():
                landed(tops.at[1], tops_recv.at[0])

                @pl.when(chip < last)
                def _():
                    top_right(tops[0] + tops[1])

            with scope("pre_wait"):
                landed(pre_in.at[k], pre_recv.at[k])
            left_v[k] = decode(pre_in[k], tops[1])

            @pl.when(chip < last)
            def _():
                pre_out[k] = encode(left_v[k] + own_v[k], tops[3])
                to_right(k).start()

        m = i - SUF * (last - chip)

        @pl.when((chip < last) & (m >= 0) & (m < blocks))
        def _():
            @pl.when(m == 0)
            def _():
                landed(tops.at[2], tops_recv.at[1])

                @pl.when(chip > 0)
                def _():
                    top_left(tops[0] + tops[2])

            with scope("suf_wait"):
                landed(suf_in.at[m], suf_recv.at[m])
            right_v[m] = decode(suf_in[m], tops[2])

            @pl.when(chip > 0)
            def _():
                suf_out[m] = encode(right_v[m] + own_v[m], tops[4])
                to_left(m).start()

        n = i - jnp.maximum(PRE * chip, SUF * (last - chip))

        @pl.when((n >= 0) & (n < blocks) & (lax.rem(n + both, both) == both - 1))
        def _():
            with scope("acc"):
                group = lax.div(n, both)
                these = pl.ds(group * both, both)
                two = split((left_v[these] + own_v[these] + right_v[these]).reshape(rank, block), 0)
                here = pl.ds(pl.multiple_of(mine_at + group * block, block), block)
                there = pl.ds(pl.multiple_of(group * block, block), block)
                acc_own[...] += jnp.dot(two, ocot_v[here, :], preferred_element_type=F32)
                acc_pair[...] += jnp.dot(two, ocot_in[there, :], preferred_element_type=F32)

        return 0

    def value_sums():
        whole = exchanged(0)
        proj_v[...] = whole
        sum_out(0, whole)

    def value_direction():
        total = jnp.sum(sum_in(0), axis=1, keepdims=True)
        scale = lax.rsqrt(total / (rank * columns * tp) + 1e-06)
        for i in (12, 13):
            loads[i].wait()
        scaled = scale * own_rows(proj_v)[...]
        first_new = 0.9 * v1_v[...] + 0.1 * scaled
        second_new = 0.95 * v2_v[...] + 0.05 * scaled * scaled
        v_first[...] = first_new
        v_second[...] = second_new
        dir_all[f] = first_new / (jnp.sqrt(second_new) + 1e-08)
        for d in fs_peers:
            send(dir_all.at[f], dir_all.at[f], dir_send, dir_recv, {"fs": d})

    def value_finish():
        landed(dir_all.at[pl.ds(0, fs - 1)], dir_recv)
        direction = split(dir_all[...].reshape(rank, columns), 0)
        count = v_step.shape[0]
        left = vfac_v[pl.ds(pl.multiple_of(f * count, count), count), :]
        move = jnp.dot(jnp.concatenate([left, left], axis=1), direction, preferred_element_type=F32)
        loads[11].wait()
        fresh = vm_v[...] - 0.002 * move
        v_step[...] = move
        v_new[...] = fresh
        here = own_rows(v_copy)
        here[...] = fresh.astype(BF16)
        for d in fs_peers:
            send(here, here, copy_send, copy_recv, {"fs": d})

    steps = blocks + max(PRE, SUF) * last
    done = 0
    for at, event in ((13, value_sums), (steps - 2, value_direction)):
        at = min(at, steps)
        lax.fori_loop(done, at, step, 0)
        done = at
        with scope(f"event{at}"):
            event()
    lax.fori_loop(done, steps, step, 0)

    pair_out[...] = acc_pair[:rank, :] + acc_pair[rank:, :]
    send(pair_out, pair_in, pair_send, pair_recv, partner)
    mine = acc_own[:rank, :] + acc_own[rank:, :]
    with scope("pair_wait"):
        landed(pair_in, pair_recv)
    with scope("exchange"):
        exchange(1, mine + pair_in[...])
    with scope("value_finish"):
        value_finish()
    with scope("exchanged"):
        whole = exchanged(1)
        o_all[...] = whole
        sum_out(1, whole)
    with scope("mom_wait"):
        moments = om_all.at[pl.ds(0, 2 * (fs - 1) * band)]
        landed(moments, mom_recv)
        left_here(moments, mom_send)
    with scope("masters_wait"):
        masters_end()
    with scope("copy_wait"):
        copies = v_copy.at[pl.ds(0, (fs - 1) * v_step.shape[0])]
        landed(copies, copy_recv)
        left_here(copies, copy_send)
    with scope("drain"):
        left_here(heads_in, heads_send)
        left_here(mas.at[pl.ds(0, fs - 1)], mas_send)
        left_here(mas_top.at[pl.ds(0, fs - 1)], mast_send)
        left_here(ocot_in, ocot_send)
        left_here(pair_out, pair_send)

        @pl.when(chip < last)
        def _():
            left_here(pre_out, pre_send)
            left_here(tops.at[3], tops_send.at[0])

        @pl.when(chip > 0)
        def _():
            left_here(suf_out, suf_send)
            left_here(tops.at[4], tops_send.at[1])

        for k in range(2):
            left_here(swap.at[k, pl.ds(0, fs - 1)], swap_send.at[k])
            left_here(swap_top.at[k, pl.ds(0, fs - 1)], mark_send.at[k])
        left_here(dir_all.at[pl.ds(0, fs - 1)], dir_send)
        left_here(sums.at[0, pl.ds(0, tp - 1)], sum_send.at[0])
    with scope("sums_wait"):
        totals[...] = sum_in(1)
        left_here(sums.at[1, pl.ds(0, tp - 1)], sum_send.at[1])


def finish_kernel(
    fs, tp,
    o_all, o1_all, o2_all, om_all, totals, ofac, omas, v_step, v_new, v_copy, v_first, v_second,
    v_step_out, v_new_out, v_copy_out, v_first_out, v_second_out,
    o_step_out, o_new_out, o_copy_out, o_first_out, o_second_out,
    step_v, new_v, copy_v, first_v, second_v, out_sem,
):
    f = lax.axis_index("fs")
    puts = []

    def put(src, dst):
        copy = pltpu.make_async_copy(src, dst, out_sem.at[len(puts)])
        copy.start()
        puts.append(copy)

    for src, dst in (
        (v_step, v_step_out), (v_new, v_new_out), (v_copy, v_copy_out), (v_first, v_first_out), (v_second, v_second_out),
    ):
        put(src, dst)
    rank, columns = o1_all.shape
    band = rank // fs
    total = jnp.sum(totals[...], axis=1, keepdims=True)
    scale = lax.rsqrt(total / (rank * columns * tp) + 1e-06)

    def moments(proj, rows):
        scaled = scale * proj
        first_new = 0.9 * o1_all[rows, :] + 0.1 * scaled
        second_new = 0.95 * o2_all[rows, :] + 0.05 * scaled * scaled
        return first_new, second_new

    own_band = pl.ds(pl.multiple_of(f * band, band), band)
    first_v[...], second_v[...] = moments(o_all[own_band, :], pl.ds(pl.multiple_of(f * band, band), band))
    put(first_v, o_first_out)
    put(second_v, o_second_out)
    first_new, second_new = moments(o_all[...], pl.ds(0, rank))
    direction = split(first_new / (jnp.sqrt(second_new) + 1e-08), 0)

    def step_of(rows):
        left = ofac[rows, :]
        return jnp.dot(jnp.concatenate([left, left], axis=1), direction, preferred_element_type=F32)

    count = step_v.shape[0]
    own = pl.ds(pl.multiple_of(f * count, count), count)
    move = step_of(own)
    step_v[...] = move
    put(step_v, o_step_out)
    new_v[...] = omas[...] - 0.002 * move
    put(new_v, o_new_out)
    for i in range(fs):
        rows = pl.ds(i * count, count)
        copy_v[rows, :] = (om_all[rows, :] - 0.002 * step_of(rows)).astype(BF16)
        put(copy_v.at[rows], o_copy_out.at[rows])
    for copy in puts:
        copy.wait()


def on_device(vin, vcot, vfac, vmas, vm1, vm2, heads, ocot, ofac, omas, om1, om2):
    fs = lax.axis_size("fs")
    tp = lax.axis_size("tp")
    rank = vfac.shape[1]
    band = rank // fs
    columns = vin.shape[1]
    tokens, width = heads.shape
    half = tokens // 2
    block = 128 if half % 128 == 0 else half
    part = rank
    blocks = half // block * (rank // part)

    def like(array):
        return pltpu.VMEM(array.shape, array.dtype)

    def shape(*dims, kind=F32):
        return jax.ShapeDtypeStruct(dims, kind)

    def wide(*dims):
        return pltpu.VMEM(dims, F32)

    def coded():
        return pltpu.VMEM((blocks, part, block), BF16)

    dma = pltpu.SemaphoreType.DMA
    v_rows, o_rows = vmas.shape[0], omas.shape[0]
    gathered = pl.pallas_call(
        functools.partial(gather_kernel, fs, tp),
        out_shape=(
            shape(rank, columns), shape(rank, columns), shape(rank, columns), shape(fs * o_rows, columns),
            shape(1, columns),
            shape(v_rows, columns), shape(v_rows, columns), shape(fs * v_rows, columns, kind=BF16),
            shape(band, columns), shape(band, columns),
        ),
        in_specs=[HBM] * 12,
        out_specs=(VMEM,) * 10,
        scratch_shapes=[
            like(vfac), like(ofac), like(vin), like(vcot), like(heads), pltpu.VMEM((half, width), BF16),
            like(ocot), pltpu.VMEM((half, columns), BF16), like(vm1), like(vm2), like(vmas), like(omas),
            wide(blocks, part, block), wide(blocks, part, block), wide(blocks, part, block),
            coded(), coded(), coded(), coded(), wide(5, 1, block),
            wide(2 * rank, columns), wide(2 * rank, columns), wide(rank, columns), wide(rank, columns),
            pltpu.VMEM((2, fs, rank, columns), BF16), wide(2, fs, 1, columns), wide(rank, columns),
            wide(fs, band, columns), wide(2, tp, 1, columns),
            pltpu.VMEM((fs, o_rows, columns), BF16), wide(fs, 1, columns),
            dma((14,)), dma, dma, dma, dma, dma, dma((blocks,)), dma, dma((blocks,)), dma((2,)), dma((2,)),
            dma, dma, dma((2,)), dma((2,)), dma((2,)), dma((2,)), dma, dma, dma((2,)), dma((2,)),
            dma, dma, dma, dma, dma, dma, dma, dma,
        ],
        compiler_params=pltpu.CompilerParams(
            collective_id=0, has_side_effects=True, vmem_limit_bytes=24 * 1024 * 1024
        ),
    )(*(pltpu.with_memory_space_constraint(a, pltpu.HBM) for a in (
        vin, vcot, vfac, vmas, vm1, vm2, heads, ocot, ofac, omas, om1, om2
    )))
    o_all, o1_all, o2_all, om_all, totals, *values = gathered

    return pl.pallas_call(
        functools.partial(finish_kernel, fs, tp),
        out_shape=(
            shape(v_rows, columns), shape(v_rows, columns), shape(fs * v_rows, columns, kind=BF16),
            shape(band, columns), shape(band, columns),
            shape(o_rows, columns), shape(o_rows, columns), shape(fs * o_rows, columns, kind=BF16),
            shape(band, columns), shape(band, columns),
        ),
        in_specs=[VMEM] * 12,
        out_specs=(HBM,) * 10,
        scratch_shapes=[
            wide(o_rows, columns), wide(o_rows, columns), pltpu.VMEM((fs * o_rows, columns), BF16),
            wide(band, columns), wide(band, columns), dma((9 + fs,)),
        ],
        compiler_params=pltpu.CompilerParams(vmem_limit_bytes=24 * 1024 * 1024),
    )(o_all, o1_all, o2_all, om_all, totals, ofac, omas, *values)


def solution(mesh):
    both = P("fs", "tp")
    in_specs = (both, P("fs", None), P(), both, both, both, both, both, P(), both, both, both)
    out_specs = (
        both, both, P(None, "tp"), both, both, both, both, P(None, "tp"), both, both,
    )
    return jax.shard_map(
        on_device, mesh=mesh, in_specs=in_specs, out_specs=out_specs, check_vma=False
    )
```

```python
import functools

import jax
import jax.numpy as jnp
from jax import lax
from jax.experimental import pallas as pl
from jax.experimental.pallas import tpu as pltpu
from jax.sharding import PartitionSpec as P

MESH = pl.DeviceIdType.MESH
ANY = pl.BlockSpec(memory_space=pl.ANY)
HBM = pl.BlockSpec(memory_space=pltpu.HBM)
VMEM = pl.BlockSpec(memory_space=pltpu.VMEM)
BF16 = jnp.bfloat16
F32 = jnp.float32
PRE = 5
SUF = 7
LEVELS = 252.0
POWER = 7
PEAK = 240000.0
HEADS_BOUND = 6.0
HEADS_PIECES = 4


def split(wide, axis):
    high = wide.astype(BF16)
    low = (wide - high.astype(F32)).astype(BF16)
    return jnp.concatenate([high, low], axis=axis)


def encode(x, top):
    u = x * (PEAK / top)
    u2 = u * u
    return (u2 * u2 * u2 * u).astype(BF16)


def decode(coded, top):
    y = coded.astype(F32)
    size = jnp.abs(y)
    root = jnp.exp(jnp.log(jnp.maximum(size, 1e-37)) * (1.0 / POWER))
    root = jnp.where(size < 2e-37, 0.0, root) * (top * (1.0 / PEAK))
    return jnp.where(y < 0.0, -root, root)


def encode_even(x, top):
    size = jnp.exp2(jnp.abs(x) * (LEVELS / top) - LEVELS / 2)
    return jnp.where(x < 0.0, -size, size).astype(BF16)


def decode_even(coded, top):
    y = coded.astype(F32)
    size = (jnp.log2(jnp.maximum(jnp.abs(y), 1e-38)) + LEVELS / 2) * (top * (1.0 / LEVELS))
    return jnp.where(y < 0.0, -size, size)


def top_of(x):
    return jnp.max(jnp.abs(x), axis=0, keepdims=True) * 1.02 + 1e-30


def gather_kernel(
    fs, tp,
    vin, vcot, vfac, vmas, vm1, vm2, heads, ocot, ofac, omas, om1, om2,
    o_all, o1_all, o2_all, om_all, totals, v_step, v_new, v_copy, v_first, v_second,
    vfac_v, ofac_v, vin_v, vcot_v, image_v, heads_v, heads_in, ocot_v, ocot_in, v1_v, v2_v, vm_v, om_v, o1_v, o2_v,
    own_v, left_v, right_v, pre_in, pre_out, suf_in, suf_out, bound, acc_own, acc_pair,
    pair_out, pair_top, swap, swap_top, value_swap, value_top, proj_v, mom, mom_top, value_mom, value_momt, sums, value_sums, mas, mas_top,
    pair_mas, pair_mast, back_first, back_second, back_step, back_new, back_copy, stage,
    load_sem, heads_send, heads_recv, ocot_send, ocot_recv, gift_send, gift_recv, pre_send, pre_recv, suf_send, suf_recv,
    swap_send, swap_recv, mark_send, mark_recv, sum_send, sum_recv, seen,
    mom_send, mom_recv, momt_send, momt_recv, mas_send, mas_recv, mast_send, mast_recv, give_send, give_recv, back_send, back_recv, copy_send, copy_recv,
):
    f = lax.axis_index("fs")
    t = lax.axis_index("tp")
    chip = t // 2
    core = t % 2
    chips = tp // 2
    last = chips - 1
    rank = vfac.shape[1]
    band = rank // fs
    tokens, width = heads.shape
    columns = vin.shape[1]
    blocks, _, block = own_v.shape
    o_rows = omas.shape[0]
    v_rows = vmas.shape[0]
    piece = tokens // HEADS_PIECES
    scope = jax.named_scope
    hub = core == 1
    aide = core == 0
    at_last = (last - chip + last) // chips
    at_first = (chip + last) // chips

    fs_peers = [3 - f, f + 1 - 2 * (f % 2), lax.rem(f + 2, fs)] if fs == 4 else [lax.rem(f + j, fs) for j in range(1, fs)]
    partner = {"tp": chip * 2 + (1 - core)}
    right = {"tp": lax.rem(t + 2, tp)}
    left = {"tp": lax.rem(t + tp - 2, tp)}

    def own_rows(ref):
        rows = ref.shape[0] // fs
        return ref.at[pl.ds(pl.multiple_of(f * rows, rows), rows)]

    pieces = [pl.ds(i * piece, piece) for i in range(HEADS_PIECES)]
    count = HEADS_PIECES

    def loading(i, src, dst):
        return pltpu.make_async_copy(src, dst, load_sem.at[i])

    heads_load = [loading(i, heads.at[rows], heads_v.at[rows]) for i, rows in enumerate(pieces)]
    om1_load = loading(count, om1, o1_v)
    om2_load = loading(count + 1, om2, o2_v)
    omas_load = loading(count + 2, omas, om_v)
    ocot_load = loading(count + 3, ocot, ocot_v)
    ofac_load = loading(count + 4, ofac, ofac_v)
    vfac_load = loading(count + 4, vfac, vfac_v)
    vcot_load = loading(count + 5, vcot, vcot_v)
    vin_load = loading(count + 6, vin, vin_v.at[0])
    vm1_load = loading(count + 7, vm1, v1_v.at[0])
    vm2_load = loading(count + 8, vm2, v2_v.at[0])
    vmas_load = loading(count + 9, vmas, vm_v.at[0])

    heads_load[0].start()

    @pl.when(hub)
    def _():
        ofac_load.start()

    for load in (*heads_load[1:], om1_load, om2_load):
        load.start()

    @pl.when(hub)
    def _():
        for load in (omas_load, ocot_load):
            load.start()

    @pl.when(aide)
    def _():
        for load in (ocot_load, vfac_load, vcot_load, vin_load, omas_load, vm1_load, vm2_load, vmas_load):
            load.start()

    barrier = pltpu.get_barrier_semaphore()

    def signal(sem, where):
        pl.semaphore_signal(sem, inc=1, device_id=where, device_id_type=MESH)

    signal(barrier, partner)
    for d in fs_peers:
        signal(barrier, {"fs": d})

    @pl.when(chip > 0)
    def _():
        signal(barrier, left)

    @pl.when(chip < last)
    def _():
        signal(barrier, right)

    with scope("barrier"):
        pl.semaphore_wait(barrier, fs + at_first + at_last)

    def pass_right(where):
        @pl.when(where & (chip > 0))
        def _():
            pl.semaphore_wait(seen.at[0], 1)

        @pl.when(where & (chip < last))
        def _():
            signal(seen.at[0], right)

    def pass_left(where):
        @pl.when(where & (chip < last))
        def _():
            pl.semaphore_wait(seen.at[1], 1)

        @pl.when(where & (chip > 0))
        def _():
            signal(seen.at[1], left)

    near = chips // 2

    def remote(src, dst, send_sem, recv_sem, where):
        return pltpu.make_async_remote_copy(
            src_ref=src, dst_ref=dst, send_sem=send_sem, recv_sem=recv_sem,
            device_id=where, device_id_type=MESH,
        )

    def send(src, dst, send_sem, recv_sem, where):
        remote(src, dst, send_sem, recv_sem, where).start()

    def landed(dst, sem):
        remote(dst, dst, sem, sem, partner).wait_recv()

    def left_here(src, sem):
        remote(src, src, sem, sem, partner).wait_send()

    def factor_of(s):
        rows = ofac_v[pl.ds(pl.multiple_of(s * width, width), width), :]
        return rows.astype(F32).T.astype(BF16)

    def against(one, two):
        return lax.dot_general(one, two, (((1,), (1,)), ((), ())), preferred_element_type=F32)

    def to_right(k):
        return remote(pre_out.at[k], pre_in.at[k], pre_send, pre_recv.at[k], right)

    def to_left(k):
        return remote(suf_out.at[k], suf_in.at[k], suf_send, suf_recv.at[k], left)

    def send_moments():
        for i, (load, local) in enumerate(((om1_load, o1_v), (om2_load, o2_v))):
            load.wait()
            top = top_of(local[...])
            mom_top[f, i] = top
            mom[f, i] = encode_even(local[...], top)
        for d in fs_peers:
            send(mom_top.at[f], mom_top.at[f], momt_send.at[0], momt_recv.at[0], {"fs": d})
            send(mom.at[f], mom.at[f], mom_send.at[0], mom_recv.at[0], {"fs": d})

    def masters_encode():
        omas_load.wait()
        top = top_of(om_v[...])
        mas_top[f] = top
        mas[f] = encode_even(om_v[...], top)

    def masters_end():
        landed(mas_top.at[pl.ds(0, fs - 1)], mast_recv)
        landed(mas.at[pl.ds(0, fs - 1)], mas_recv)
        for g in range(fs):
            om_all[pl.ds(g * o_rows, o_rows), :] = decode_even(mas[g], mas_top[g])

    late = at_first * at_last * SUF

    def step(i, _):
        k = i - PRE * chip

        @pl.when((chip > 0) & (k >= 0) & (k < blocks))
        def _():
            with scope("pre_wait"):
                landed(pre_in.at[k], pre_recv.at[k])
            left_v[k] = decode(pre_in[k], bound[...])

            @pl.when(chip < last)
            def _():
                pre_out[k] = encode(left_v[k] + own_v[k], bound[...])
                to_right(k).start()

        m = i - SUF * (last - chip)

        @pl.when((chip < last) & (m >= 0) & (m < blocks))
        def _():
            with scope("suf_wait"):
                landed(suf_in.at[m], suf_recv.at[m])
            right_v[m] = decode(suf_in[m], bound[...])

            @pl.when(chip > 0)
            def _():
                suf_out[m] = encode(right_v[m] + own_v[m], bound[...])
                to_left(m).start()

        n = i - late - jnp.maximum(PRE * chip, SUF * (last - chip))

        @pl.when((n >= 0) & (n < blocks) & (lax.rem(n + 2, 2) == 1))
        def _():
            with scope("acc"):
                image = jnp.concatenate([left_v[j] + own_v[j] + right_v[j] for j in (n - 1, n)], axis=1)
                two = split(image, 0)
                here = pl.ds(pl.multiple_of((n - 1) * block, block), 2 * block)
                acc_own[...] += jnp.dot(two, ocot_v[here, :], preferred_element_type=F32)
                acc_pair[...] += jnp.dot(two, ocot_in[here, :], preferred_element_type=F32)

        return 0

    steps = blocks + SUF * last

    @pl.when(hub)
    def _():
        for i, (src, dst) in enumerate(((vin, vin_v), (vm1, v1_v), (vm2, v2_v), (vmas, vm_v))):
            send(src, dst.at[1], gift_send.at[i], gift_recv.at[i], partner)
        send_moments()
        with scope("factor"):
            ofac_load.wait()
            reach = jnp.sum(jnp.abs(ofac_v[...].astype(F32)), axis=0, keepdims=True)
            top = jnp.max(reach, axis=1, keepdims=True) * (1.02 * HEADS_BOUND) + 1e-30
            bound[...] = jnp.broadcast_to(top, bound.shape)
            factor = jnp.concatenate([factor_of(t - 1), factor_of(t)], axis=1)
        group = blocks // HEADS_PIECES
        for i, rows in enumerate(pieces):
            heads_load[i].wait()
            with scope("heads_in"):
                landed(heads_in.at[rows], heads_recv.at[i])
            with scope("own"):
                own = against(factor, jnp.concatenate([heads_in[rows, :], heads_v[rows, :]], axis=1))
                for k in range(group):
                    own_v[i * group + k] = own[:, k * block:(k + 1) * block]

            @pl.when(chip == 0)
            def _():
                for k in range(i * group, (i + 1) * group):
                    pre_out[k] = encode(own_v[k], bound[...])
                    to_right(k).start()

            @pl.when(chip == last)
            def _():
                for k in range(i * group, (i + 1) * group):
                    suf_out[k] = encode(own_v[k], bound[...])
                    to_left(k).start()

        @pl.when(chip == 0)
        def _():
            left_v[...] = jnp.zeros_like(left_v)

        @pl.when(chip == last)
        def _():
            right_v[...] = jnp.zeros_like(right_v)

        acc_own[...] = jnp.zeros_like(acc_own)
        acc_pair[...] = jnp.zeros_like(acc_pair)
        with scope("masters_encode"):
            masters_encode()
        send(mas_top.at[f], pair_mast, give_send.at[0], give_recv.at[0], partner)
        send(mas.at[f], pair_mas, give_send.at[1], give_recv.at[1], partner)

        def output_cotangents():
            ocot_load.wait()
            landed(ocot_in, ocot_recv)

        done = 0
        for at, event in ((13, output_cotangents),):
            at = min(at, steps)
            lax.fori_loop(done, at, step, 0)
            done = at
            with scope(f"event{at}"):
                event()
        lax.fori_loop(done, steps, step, 0)

        with scope("exchange"):
            mine = acc_own[:rank, :] + acc_own[rank:, :]
            pair = acc_pair[:rank, :] + acc_pair[rank:, :]
            top = top_of(pair)
            pair_top[...] = top
            pair_out[...] = encode_even(pair, top)
            top = top_of(mine)
            swap_top[f] = top
            swap[f] = encode_even(mine, top)
            for d in fs_peers:
                there = {"fs": d, "tp": t - 1}
                send(pair_top, swap_top.at[f], mark_send.at[1], mark_recv.at[0], there)
                send(pair_out, swap.at[f], swap_send.at[1], swap_recv.at[0], there)
                send(swap_top.at[f], swap_top.at[f], mark_send.at[0], mark_recv.at[0], {"fs": d})
                send(swap.at[f], swap.at[f], swap_send.at[0], swap_recv.at[0], {"fs": d})
            send(pair_top, swap_top.at[f], mark_send.at[1], mark_recv.at[0], partner)
            send(pair_out, swap.at[f], swap_send.at[1], swap_recv.at[0], partner)
        with scope("back_copy"):
            landed(v_copy.at[pl.ds(0, 2 * v_rows)], back_recv.at[2])
            here = own_rows(v_copy)
            for d in fs_peers:
                send(here, here, copy_send.at[0], copy_recv, {"fs": d})
                send(stage, here, copy_send.at[1], copy_recv, {"fs": d, "tp": t - 1})
        with scope("swap_wait"):
            landed(swap_top.at[pl.ds(0, fs - 1)], mark_recv.at[0])
            landed(swap.at[pl.ds(0, fs - 1)], swap_recv.at[0])

    @pl.when(aide)
    def _():
        pass_right(chip == 0)
        pass_left(chip == last)
        for i, rows in enumerate(pieces):
            heads_load[i].wait()
            send(heads_v.at[rows], heads_in.at[rows], heads_send, heads_recv.at[i], partner)
        send_moments()
        ocot_load.wait()
        send(ocot_v, ocot_in, ocot_send, ocot_recv, partner)
        pass_right((chip > 0) & (chip < near))
        pass_left((chip < last) & (chip >= near))
        with scope("value_load"):
            for load in (vfac_load, vcot_load, vin_load):
                load.wait()
        with scope("value_own"):
            total = jnp.zeros((2 * rank, columns), F32)
            stride = image_v.shape[2]
            value_factor = vfac_v[...].astype(F32).T.astype(BF16)
            for i in range(tokens // stride):
                rows = pl.ds(i * stride, stride)
                two = split(against(value_factor, vcot_v[rows, :]), 0)
                image_v[i] = two
                total = total + jnp.dot(two, vin_v[0, rows, :], preferred_element_type=F32)
            totals_v = [total]
        with scope("value_moments"):
            vm1_load.wait()
            vm2_load.wait()
            landed(v1_v.at[1], gift_recv.at[1])
            landed(v2_v.at[1], gift_recv.at[2])
            for i, local in enumerate((v1_v, v2_v)):
                for h in range(2):
                    top = top_of(local[h])
                    value_momt[f, i, h] = top
                    value_mom[f, i, h] = encode_even(local[h], top)
            for d in fs_peers:
                send(value_momt.at[f], value_momt.at[f], momt_send.at[1], momt_recv.at[1], {"fs": d})
                send(value_mom.at[f], value_mom.at[f], mom_send.at[1], mom_recv.at[1], {"fs": d})
        with scope("gift"):
            landed(vin_v.at[1], gift_recv.at[0])
        with scope("value_pair"):
            total = jnp.zeros((2 * rank, columns), F32)
            for i in range(tokens // stride):
                total = total + jnp.dot(image_v[i], vin_v[1, pl.ds(i * stride, stride), :], preferred_element_type=F32)
            totals_v.append(total)
            for h, total in enumerate(totals_v):
                mine = total[:rank] + total[rank:]
                top = top_of(mine)
                value_top[f, h] = top
                value_swap[f, h] = encode_even(mine, top)
            for d in fs_peers:
                send(value_top.at[f], value_top.at[f], mark_send.at[2], mark_recv.at[1], {"fs": d})
                send(value_swap.at[f], value_swap.at[f], swap_send.at[2], swap_recv.at[1], {"fs": d})
        masters_encode()
        for d in fs_peers:
            send(mas_top.at[f], mas_top.at[f], mast_send.at[0], mast_recv, {"fs": d})
            send(mas.at[f], mas.at[f], mas_send.at[0], mas_recv, {"fs": d})
        with scope("give"):
            landed(pair_mast, give_recv.at[0])
            landed(pair_mas, give_recv.at[1])
        for d in fs_peers:
            there = {"fs": d, "tp": t + 1}
            send(pair_mast, mas_top.at[f], mast_send.at[1], mast_recv, there)
            send(pair_mas, mas.at[f], mas_send.at[1], mas_recv, there)
        pass_right((chip >= near) & (chip < last))
        pass_left((chip > 0) & (chip < near))

        @pl.when(chip == 0)
        def _():
            pl.semaphore_wait(seen.at[1], 1)

        @pl.when(chip == last)
        def _():
            pl.semaphore_wait(seen.at[0], 1)

        with scope("value_swap_wait"):
            landed(value_top.at[pl.ds(0, fs - 1)], mark_recv.at[1])
            landed(value_swap.at[pl.ds(0, fs - 1)], swap_recv.at[1])
        power = jnp.zeros((1, columns), F32)
        for h in range(2):
            whole = decode_even(value_swap[0, h], value_top[0, h])
            for g in range(1, fs):
                whole = whole + decode_even(value_swap[g, h], value_top[g, h])
            proj_v[h] = whole
            power = power + jnp.sum(whole * whole, axis=0, keepdims=True)
        value_sums[chip] = power
        for j in range(1, chips):
            where = {"tp": lax.rem(t + 2 * j, tp)}
            send(value_sums.at[chip], value_sums.at[chip], sum_send.at[0], sum_recv.at[0], where)
        with scope("value_sums_wait"):
            landed(value_sums.at[pl.ds(0, chips - 1)], sum_recv.at[0])
        total = jnp.sum(jnp.sum(value_sums[...], axis=0), axis=1, keepdims=True)
        scale = lax.rsqrt(total / (rank * columns * tp) + 1e-06)
        for h, first_out, second_out in ((0, v_first, v_second), (1, back_first, back_second)):
            scaled = scale * proj_v[h, pl.ds(pl.multiple_of(f * band, band), band), :]
            first_out[...] = 0.9 * v1_v[h] + 0.1 * scaled
            second_out[...] = 0.95 * v2_v[h] + 0.05 * scaled * scaled
        send(back_first, v_first, back_send.at[0], back_recv.at[0], partner)
        send(back_second, v_second, back_send.at[0], back_recv.at[0], partner)
        vmas_load.wait()
        landed(vm_v.at[1], gift_recv.at[3])
        rows = vfac_v[pl.ds(pl.multiple_of(f * v_rows, v_rows), v_rows), :]
        rows = jnp.concatenate([rows, rows], axis=1)
        with scope("mom_wait"):
            landed(value_momt.at[pl.ds(0, fs - 1)], momt_recv.at[1])
            landed(value_mom.at[pl.ds(0, fs - 1)], mom_recv.at[1])
        here = own_rows(v_copy)

        def gathered(i, h):
            return jnp.concatenate([decode_even(value_mom[g, i, h], value_momt[g, i, h]) for g in range(fs)], axis=0)

        for h, step_out, new_out, copy_out in ((1, back_step, back_new, back_copy), (0, v_step, v_new, here)):
            scaled = scale * proj_v[h]
            first_new = 0.9 * gathered(0, h) + 0.1 * scaled
            second_new = 0.95 * gathered(1, h) + 0.05 * scaled * scaled
            direction = split(first_new / (jnp.sqrt(second_new) + 1e-08), 0)
            move = jnp.dot(rows, direction, preferred_element_type=F32)
            fresh = vm_v[h] - 0.002 * move
            step_out[...] = move
            new_out[...] = fresh
            copy_out[...] = fresh.astype(BF16)
            if h == 1:
                send(back_copy, here, back_send.at[2], back_recv.at[2], partner)
                send(back_step, v_step, back_send.at[1], back_recv.at[1], partner)
                send(back_new, v_new, back_send.at[1], back_recv.at[1], partner)
            else:
                send(here, stage, back_send.at[2], back_recv.at[2], partner)
        with scope("swap_wait"):
            landed(swap_top, mark_recv.at[0])
            landed(swap, swap_recv.at[0])

    with scope("sum_out"):
        whole = decode_even(swap[0], swap_top[0])
        for g in range(1, fs):
            whole = whole + decode_even(swap[g], swap_top[g])
        o_all[...] = whole
        sums[t] = jnp.sum(whole * whole, axis=0, keepdims=True)
        for j in range(1, tp):
            send(sums.at[t], sums.at[t], sum_send.at[1], sum_recv.at[1], {"tp": lax.rem(t + j, tp)})
    with scope("masters_wait"):
        masters_end()
    with scope("mom_wait"):
        landed(mom_top.at[pl.ds(0, fs - 1)], momt_recv.at[0])
        landed(mom.at[pl.ds(0, fs - 1)], mom_recv.at[0])
        for i, whole in ((0, o1_all), (1, o2_all)):
            for g in range(fs):
                whole[pl.ds(g * band, band), :] = decode_even(mom[g, i], mom_top[g, i])
        left_here(mom_top.at[pl.ds(0, fs - 1)], momt_send.at[0])
        left_here(mom.at[pl.ds(0, fs - 1)], mom_send.at[0])

    with scope("drain"):
        copies = v_copy.at[pl.ds(0, (fs - 1) * v_rows)]

        @pl.when(aide)
        def _():
            left_here(heads_in, heads_send)
            left_here(ocot_in, ocot_send)
            left_here(value_swap.at[pl.ds(0, fs - 1)], swap_send.at[2])
            left_here(value_top.at[pl.ds(0, fs - 1)], mark_send.at[2])
            left_here(value_momt.at[pl.ds(0, fs - 1)], momt_send.at[1])
            left_here(value_mom.at[pl.ds(0, fs - 1)], mom_send.at[1])
            left_here(value_sums.at[pl.ds(0, chips - 1)], sum_send.at[0])
            for i in range(2):
                left_here(mas.at[pl.ds(0, fs - 1)], mas_send.at[i])
                left_here(mas_top.at[pl.ds(0, fs - 1)], mast_send.at[i])
            left_here(v1_v, back_send.at[0])
            left_here(vm_v, back_send.at[1])
            left_here(v_copy.at[pl.ds(0, 2 * v_rows)], back_send.at[2])

        @pl.when(hub)
        def _():
            for i, ref in enumerate((vin_v, v1_v, v2_v, vm_v)):
                left_here(ref.at[1], gift_send.at[i])
            left_here(pair_mast, give_send.at[0])
            left_here(pair_mas, give_send.at[1])
            left_here(swap.at[pl.ds(0, fs - 1)], swap_send.at[0])
            left_here(swap_top.at[pl.ds(0, fs - 1)], mark_send.at[0])
            left_here(swap, swap_send.at[1])
            left_here(swap_top, mark_send.at[1])
            landed(v1_v, back_recv.at[0])
            landed(vm_v, back_recv.at[1])
            left_here(copies, copy_send.at[0])
            left_here(copies, copy_send.at[1])

        @pl.when(hub & (chip < last))
        def _():
            left_here(pre_out, pre_send)

        @pl.when(hub & (chip > 0))
        def _():
            left_here(suf_out, suf_send)

    with scope("copy_wait"):
        landed(copies, copy_recv)
    with scope("sums_wait"):
        landed(sums.at[pl.ds(0, tp - 1)], sum_recv.at[1])
        totals[...] = jnp.sum(sums[...], axis=0)
        left_here(sums.at[pl.ds(0, tp - 1)], sum_send.at[1])


def finish_kernel(
    fs, tp,
    o_all, o1_all, o2_all, om_all, totals, ofac, omas, om1, om2, v_step, v_new, v_copy, v_first, v_second,
    v_step_out, v_new_out, v_copy_out, v_first_out, v_second_out,
    o_step_out, o_new_out, o_copy_out, o_first_out, o_second_out,
    step_v, new_v, copy_v, first_v, second_v, out_sem,
):
    f = lax.axis_index("fs")
    puts = []

    def put(src, dst):
        copy = pltpu.make_async_copy(src, dst, out_sem.at[len(puts)])
        copy.start()
        puts.append(copy)

    for src, dst in (
        (v_step, v_step_out), (v_new, v_new_out), (v_copy, v_copy_out), (v_first, v_first_out), (v_second, v_second_out),
    ):
        put(src, dst)
    rank, columns = o1_all.shape
    band = rank // fs
    total = jnp.sum(totals[...], axis=1, keepdims=True)
    scale = lax.rsqrt(total / (rank * columns * tp) + 1e-06)

    def moments(proj, first, second):
        scaled = scale * proj
        first_new = 0.9 * first + 0.1 * scaled
        second_new = 0.95 * second + 0.05 * scaled * scaled
        return first_new, second_new

    own_band = pl.ds(pl.multiple_of(f * band, band), band)
    first_v[...], second_v[...] = moments(o_all[own_band, :], om1[...], om2[...])
    put(first_v, o_first_out)
    put(second_v, o_second_out)
    first_new, second_new = moments(o_all[...], o1_all[...], o2_all[...])
    direction = split(first_new / (jnp.sqrt(second_new) + 1e-08), 0)

    def step_of(rows):
        left = ofac[rows, :]
        return jnp.dot(jnp.concatenate([left, left], axis=1), direction, preferred_element_type=F32)

    count = step_v.shape[0]
    own = pl.ds(pl.multiple_of(f * count, count), count)
    move = step_of(own)
    step_v[...] = move
    put(step_v, o_step_out)
    new_v[...] = omas[...] - 0.002 * move
    put(new_v, o_new_out)
    for i in range(fs):
        rows = pl.ds(i * count, count)
        copy_v[rows, :] = (om_all[rows, :] - 0.002 * step_of(rows)).astype(BF16)
        put(copy_v.at[rows], o_copy_out.at[rows])
    for copy in puts:
        copy.wait()


def on_device(vin, vcot, vfac, vmas, vm1, vm2, heads, ocot, ofac, omas, om1, om2):
    fs = lax.axis_size("fs")
    tp = lax.axis_size("tp")
    rank = vfac.shape[1]
    band = rank // fs
    columns = vin.shape[1]
    tokens, width = heads.shape
    block = 128
    blocks = tokens // block
    stride = 256 if tokens % 256 == 0 else tokens

    def twice(array):
        return pltpu.VMEM((2, *array.shape), array.dtype)

    def like(array):
        return pltpu.VMEM(array.shape, array.dtype)

    def shape(*dims, kind=F32):
        return jax.ShapeDtypeStruct(dims, kind)

    def wide(*dims):
        return pltpu.VMEM(dims, F32)

    def coded():
        return pltpu.VMEM((blocks, rank, block), BF16)

    dma = pltpu.SemaphoreType.DMA
    v_rows, o_rows = vmas.shape[0], omas.shape[0]
    gathered = pl.pallas_call(
        functools.partial(gather_kernel, fs, tp),
        out_shape=(
            shape(rank, columns), shape(rank, columns), shape(rank, columns), shape(fs * o_rows, columns),
            shape(1, columns),
            shape(v_rows, columns), shape(v_rows, columns), shape(fs * v_rows, columns, kind=BF16),
            shape(band, columns), shape(band, columns),
        ),
        in_specs=[HBM] * 12,
        out_specs=(VMEM,) * 10,
        scratch_shapes=[
            like(vfac), like(ofac), twice(vin), like(vcot), pltpu.VMEM((tokens // stride, 2 * rank, stride), BF16),
            like(heads), like(heads), like(ocot), like(ocot), twice(vm1), twice(vm2), twice(vmas), like(omas), like(om1), like(om2),
            wide(blocks, rank, block), wide(blocks, rank, block), wide(blocks, rank, block),
            coded(), coded(), coded(), coded(), wide(1, block),
            wide(2 * rank, columns), wide(2 * rank, columns),
            pltpu.VMEM((rank, columns), BF16), wide(1, columns),
            pltpu.VMEM((fs, rank, columns), BF16), wide(fs, 1, columns),
            pltpu.VMEM((fs, 2, rank, columns), BF16), wide(fs, 2, 1, columns),
            wide(2, rank, columns),
            pltpu.VMEM((fs, 2, band, columns), BF16), wide(fs, 2, 1, columns),
            pltpu.VMEM((fs, 2, 2, band, columns), BF16), wide(fs, 2, 2, 1, columns), wide(tp, 1, columns), wide(tp // 2, 1, columns),
            pltpu.VMEM((fs, o_rows, columns), BF16), wide(fs, 1, columns),
            pltpu.VMEM((o_rows, columns), BF16), wide(1, columns),
            wide(band, columns), wide(band, columns), wide(v_rows, columns), wide(v_rows, columns),
            pltpu.VMEM((v_rows, columns), BF16), pltpu.VMEM((v_rows, columns), BF16),
            dma((10 + HEADS_PIECES,)), dma, dma((HEADS_PIECES,)), dma, dma, dma((4,)), dma((4,)),
            dma, dma((blocks,)), dma, dma((blocks,)),
            dma((3,)), dma((2,)), dma((3,)), dma((2,)), dma((2,)), dma((2,)), pltpu.SemaphoreType.REGULAR((2,)),
            dma((2,)), dma((2,)), dma((2,)), dma((2,)), dma((2,)), dma, dma((2,)), dma, dma((2,)), dma((2,)), dma((3,)), dma((3,)), dma((2,)), dma,
        ],
        compiler_params=pltpu.CompilerParams(
            collective_id=0, has_side_effects=True, vmem_limit_bytes=32 * 1024 * 1024
        ),
    )(*(pltpu.with_memory_space_constraint(a, pltpu.HBM) for a in (
        vin, vcot, vfac, vmas, vm1, vm2, heads, ocot, ofac, omas, om1, om2
    )))
    o_all, o1_all, o2_all, om_all, totals, *values = gathered

    return pl.pallas_call(
        functools.partial(finish_kernel, fs, tp),
        out_shape=(
            shape(v_rows, columns), shape(v_rows, columns), shape(fs * v_rows, columns, kind=BF16),
            shape(band, columns), shape(band, columns),
            shape(o_rows, columns), shape(o_rows, columns), shape(fs * o_rows, columns, kind=BF16),
            shape(band, columns), shape(band, columns),
        ),
        in_specs=[VMEM] * 14,
        out_specs=(HBM,) * 10,
        scratch_shapes=[
            wide(o_rows, columns), wide(o_rows, columns), pltpu.VMEM((fs * o_rows, columns), BF16),
            wide(band, columns), wide(band, columns), dma((9 + fs,)),
        ],
        compiler_params=pltpu.CompilerParams(vmem_limit_bytes=24 * 1024 * 1024),
    )(o_all, o1_all, o2_all, om_all, totals, ofac, omas, om1, om2, *values)


def solution(mesh):
    both = P("fs", "tp")
    in_specs = (both, P("fs", None), P(), both, both, both, both, both, P(), both, both, both)
    out_specs = (
        both, both, P(None, "tp"), both, both, both, both, P(None, "tp"), both, both,
    )
    return jax.shard_map(
        on_device, mesh=mesh, in_specs=in_specs, out_specs=out_specs, check_vma=False
    )
```

```python
import functools

import jax
import jax.numpy as jnp
from jax import lax
from jax.experimental import pallas as pl
from jax.experimental.pallas import tpu as pltpu
from jax.sharding import PartitionSpec as P

MESH = pl.DeviceIdType.MESH
ANY = pl.BlockSpec(memory_space=pl.ANY)
HBM = pl.BlockSpec(memory_space=pltpu.HBM)
VMEM = pl.BlockSpec(memory_space=pltpu.VMEM)
BF16 = jnp.bfloat16
F32 = jnp.float32
PRE = 6
SUF = 7
LEVELS = 252.0
POWER = 7
PEAK = 240000.0
HEADS_BOUND = 6.0


def split(wide, axis):
    high = wide.astype(BF16)
    low = (wide - high.astype(F32)).astype(BF16)
    return jnp.concatenate([high, low], axis=axis)


def encode(x, top):
    u = x * (PEAK / top)
    u2 = u * u
    return (u2 * u2 * u2 * u).astype(BF16)


def decode(coded, top):
    y = coded.astype(F32)
    size = jnp.abs(y)
    root = jnp.exp(jnp.log(jnp.maximum(size, 1e-37)) * (1.0 / POWER))
    root = jnp.where(size < 2e-37, 0.0, root) * (top * (1.0 / PEAK))
    return jnp.where(y < 0.0, -root, root)


def encode_even(x, top):
    size = jnp.exp2(jnp.abs(x) * (LEVELS / top) - LEVELS / 2)
    return jnp.where(x < 0.0, -size, size).astype(BF16)


def decode_even(coded, top):
    y = coded.astype(F32)
    size = (jnp.log2(jnp.maximum(jnp.abs(y), 1e-38)) + LEVELS / 2) * (top * (1.0 / LEVELS))
    return jnp.where(y < 0.0, -size, size)


def top_of(x):
    return jnp.max(jnp.abs(x), axis=0, keepdims=True) * 1.02 + 1e-30


def growing(blocks):
    sizes = [1]
    while sum(sizes) < blocks:
        sizes.append(min(sum(sizes), blocks - sum(sizes)))
    return sizes


def gather_kernel(
    fs, tp,
    vin, vcot, vfac, vmas, vm1, vm2, heads, ocot, ofac, omas, om1, om2,
    o_all, o1_all, o2_all, om_all, totals, v_step, v_new, v_copy, v_first, v_second,
    vfac_v, ofac_v, vin_v, vcot_v, image_v, heads_v, heads_in, ocot_v, ocot_in, v1_v, v2_v, vm_v, om_v, o1_v, o2_v,
    own_v, left_v, right_v, pre_in, pre_out, suf_in, suf_out, bound, acc_own, acc_pair,
    part, part_out, part_top, part_in, part_top_in, stage, value_swap, value_top, proj_v, mom, mom_top, value_mom, value_momt, sums, value_sums, mas, mas_top,
    pair_mas, pair_mast, back_first, back_second, back_step, back_new, back_copy, value_mas, value_mast, move_v,
    load_sem, heads_recv, ocot_recv, gift_send, pre_send, pre_recv, suf_send, suf_recv,
    part_send, part_recv, mark_send, mark_recv, all_send, all_recv, sum_send, sum_recv, seen,
    mom_send, mom_recv, momt_send, momt_recv, mas_recv, mast_recv, give_send, back_recv, copy_recv,
):
    f = lax.axis_index("fs")
    t = lax.axis_index("tp")
    chip = t // 2
    core = t % 2
    chips = tp // 2
    last = chips - 1
    rank = vfac.shape[1]
    band = rank // fs
    tokens, width = heads.shape
    columns = vin.shape[1]
    blocks, _, block = own_v.shape
    o_rows = omas.shape[0]
    v_rows = vmas.shape[0]
    scope = jax.named_scope
    hub = core == 1
    aide = core == 0
    at_last = (last - chip + last) // chips
    at_first = (chip + last) // chips

    spare = iter([sems.at[i] for sems in (pre_recv, suf_recv) for i in range(blocks)])
    heads_send, ocot_send = next(spare), next(spare)
    gift_recv = [next(spare) for _ in range(4)]
    value_swap_send, value_swap_recv, value_mark_send, value_mark_recv = (next(spare) for _ in range(4))
    value_sum_send, value_sum_recv = next(spare), next(spare)
    value_mom_send, value_mom_recv, value_momt_send, value_momt_recv = (next(spare) for _ in range(4))
    mas_send, mast_send, give_recv = ([next(spare) for _ in range(2)] for _ in range(3))
    back_send = [next(spare) for _ in range(2)]
    copy_send = next(spare)
    value_mas_send, value_mas_recv, value_mast_send, value_mast_recv = (next(spare) for _ in range(4))

    fs_peers = [3 - f, f + 1 - 2 * (f % 2), lax.rem(f + 2, fs)] if fs == 4 else [lax.rem(f + j, fs) for j in range(1, fs)]
    partner = {"tp": chip * 2 + (1 - core)}
    right = {"tp": lax.rem(t + 2, tp)}
    left = {"tp": lax.rem(t + tp - 2, tp)}

    def own_rows(ref):
        rows = ref.shape[0] // fs
        return ref.at[pl.ds(pl.multiple_of(f * rows, rows), rows)]

    sizes = growing(blocks)
    count = len(sizes)
    starts = [sum(sizes[:i]) for i in range(count)]
    pieces = [pl.ds(a * block, n * block) for a, n in zip(starts, sizes)]

    def loading(i, src, dst):
        return pltpu.make_async_copy(src, dst, load_sem.at[i])

    heads_load = [loading(i, heads.at[rows], heads_v.at[rows]) for i, rows in enumerate(pieces)]
    om1_load = loading(count, om1, o1_v)
    om2_load = loading(count, om2, o2_v)
    om12_load = loading(count, om_v.at[pl.ds(0, 2 * band)], om_v.at[pl.ds(0, 2 * band)])
    omas_load = loading(count + 2, omas, om_v)
    ocot_load = loading(count + 3, ocot, ocot_v)
    ofac_load = loading(count + 4, ofac, ofac_v)
    vfac_load = loading(count + 4, vfac, vfac_v)
    vcot_load = loading(count + 5, vcot, vcot_v)
    vin_load = loading(count + 6, vin, vin_v.at[0])
    vm1_load = loading(count + 1, vm1, v1_v.at[0])
    vm2_load = loading(count + 1, vm2, v2_v.at[0])
    vm12_load = loading(count + 1, v1_v, v1_v)
    vmas_load = loading(count + 7, vmas, vm_v.at[0])

    heads_load[0].start()

    @pl.when(hub)
    def _():
        ofac_load.start()

    for load in (*heads_load[1:], om1_load, om2_load):
        load.start()

    @pl.when(hub)
    def _():
        for load in (omas_load, ocot_load):
            load.start()

    @pl.when(aide)
    def _():
        for load in (omas_load, ocot_load, vfac_load, vcot_load, vin_load, vm1_load, vm2_load, vmas_load):
            load.start()

    barrier = pltpu.get_barrier_semaphore()

    def signal(sem, where):
        pl.semaphore_signal(sem, inc=1, device_id=where, device_id_type=MESH)

    signal(barrier, partner)
    for d in fs_peers:
        signal(barrier, {"fs": d})

    @pl.when(chip > 0)
    def _():
        signal(barrier, left)

    @pl.when(chip < last)
    def _():
        signal(barrier, right)

    with scope("barrier"):
        pl.semaphore_wait(barrier, fs + at_first + at_last)

    def pass_right(where):
        @pl.when(where & (chip > 0))
        def _():
            pl.semaphore_wait(seen.at[0], 1)

        @pl.when(where & (chip < last))
        def _():
            signal(seen.at[0], right)

    def pass_left(where):
        @pl.when(where & (chip < last))
        def _():
            pl.semaphore_wait(seen.at[1], 1)

        @pl.when(where & (chip > 0))
        def _():
            signal(seen.at[1], left)

    near = chips // 2

    def remote(src, dst, send_sem, recv_sem, where):
        return pltpu.make_async_remote_copy(
            src_ref=src, dst_ref=dst, send_sem=send_sem, recv_sem=recv_sem,
            device_id=where, device_id_type=MESH,
        )

    def send(src, dst, send_sem, recv_sem, where):
        remote(src, dst, send_sem, recv_sem, where).start()

    def landed(dst, sem):
        remote(dst, dst, sem, sem, partner).wait_recv()

    def left_here(src, sem):
        remote(src, src, sem, sem, partner).wait_send()

    def factor_of(s):
        rows = ofac_v[pl.ds(pl.multiple_of(s * width, width), width), :]
        return rows.astype(F32).T.astype(BF16)

    def against(one, two):
        return lax.dot_general(one, two, (((1,), (1,)), ((), ())), preferred_element_type=F32)

    def to_right(k):
        return remote(pre_out.at[k], pre_in.at[k], pre_send, pre_recv.at[k], right)

    def to_left(k):
        return remote(suf_out.at[k], suf_in.at[k], suf_send, suf_recv.at[k], left)

    def send_moments():
        om12_load.wait()
        for i, local in enumerate((o1_v, o2_v)):
            top = top_of(local[...])
            mom_top[f, i] = top
            mom[f, i] = encode_even(local[...], top)
        for d in fs_peers:
            send(mom_top.at[f], mom_top.at[f], momt_send, momt_recv, {"fs": d})
            send(mom.at[f], mom.at[f], mom_send, mom_recv, {"fs": d})

    def masters_encode():
        omas_load.wait()
        top = top_of(om_v[...])
        mas_top[f] = top
        mas[f] = encode_even(om_v[...], top)

    def masters_end():
        landed(mas_top.at[pl.ds(0, fs - 1)], mast_recv)
        landed(mas.at[pl.ds(0, fs - 1)], mas_recv)
        for g in range(fs):
            om_all[pl.ds(g * o_rows, o_rows), :] = decode_even(mas[g], mas_top[g])

    late = at_first * at_last * SUF

    def step(i, _):
        k = i - PRE * chip

        @pl.when((chip > 0) & (k >= 0) & (k < blocks))
        def _():
            with scope("pre_wait"):
                landed(pre_in.at[k], pre_recv.at[k])
            left_v[k] = decode(pre_in[k], bound[...])

            @pl.when(chip < last)
            def _():
                pre_out[k] = encode(left_v[k] + own_v[k], bound[...])
                to_right(k).start()

        m = i - SUF * (last - chip)

        @pl.when((chip < last) & (m >= 0) & (m < blocks))
        def _():
            with scope("suf_wait"):
                landed(suf_in.at[m], suf_recv.at[m])
            right_v[m] = decode(suf_in[m], bound[...])

            @pl.when(chip > 0)
            def _():
                suf_out[m] = encode(right_v[m] + own_v[m], bound[...])
                to_left(m).start()

        n = i - late - jnp.maximum(PRE * chip, SUF * (last - chip))

        @pl.when((n >= 0) & (n < blocks) & (lax.rem(n + 2, 2) == 1))
        def _():
            with scope("acc"):
                image = jnp.concatenate([left_v[j] + own_v[j] + right_v[j] for j in (n - 1, n)], axis=1)
                two = split(image, 0)
                here = pl.ds(pl.multiple_of((n - 1) * block, block), 2 * block)
                acc_own[...] += jnp.dot(two, ocot_v[here, :], preferred_element_type=F32)
                acc_pair[...] += jnp.dot(two, ocot_in[here, :], preferred_element_type=F32)

        return 0

    steps = blocks + SUF * last

    @pl.when(hub)
    def _():
        for i, (src, dst) in enumerate(((vin, vin_v), (vm1, v1_v), (vm2, v2_v), (vmas, vm_v))):
            send(src, dst.at[1], gift_send.at[i], gift_recv[i], partner)
        send_moments()
        with scope("factor"):
            ofac_load.wait()
            reach = jnp.sum(jnp.abs(ofac_v[...].astype(F32)), axis=0, keepdims=True)
            top = jnp.max(reach, axis=1, keepdims=True) * (1.02 * HEADS_BOUND) + 1e-30
            bound[...] = jnp.broadcast_to(top, bound.shape)
            factor = jnp.concatenate([factor_of(t - 1), factor_of(t)], axis=1)
        for i, rows in enumerate(pieces):
            heads_load[i].wait()
            with scope("heads_in"):
                landed(heads_in.at[rows], heads_recv.at[i])
            with scope("own"):
                own = against(factor, jnp.concatenate([heads_in[rows, :], heads_v[rows, :]], axis=1))
                for k in range(sizes[i]):
                    own_v[starts[i] + k] = own[:, k * block:(k + 1) * block]

            @pl.when(chip == 0)
            def _():
                for k in range(starts[i], starts[i] + sizes[i]):
                    pre_out[k] = encode(own_v[k], bound[...])
                    to_right(k).start()

            @pl.when(chip == last)
            def _():
                for k in range(starts[i], starts[i] + sizes[i]):
                    suf_out[k] = encode(own_v[k], bound[...])
                    to_left(k).start()

        @pl.when(chip == 0)
        def _():
            left_v[...] = jnp.zeros_like(left_v)

        @pl.when(chip == last)
        def _():
            right_v[...] = jnp.zeros_like(right_v)

        acc_own[...] = jnp.zeros_like(acc_own)
        acc_pair[...] = jnp.zeros_like(acc_pair)
        with scope("masters_encode"):
            masters_encode()
        send(mas_top.at[f], pair_mast, give_send.at[0], give_recv[0], partner)
        send(mas.at[f], pair_mas, give_send.at[1], give_recv[1], partner)

        def output_cotangents():
            ocot_load.wait()
            landed(ocot_in, ocot_recv)

        done = 0
        for at, event in ((13, output_cotangents),):
            at = min(at, steps)
            lax.fori_loop(done, at, step, 0)
            done = at
            with scope(f"event{at}"):
                event()
        lax.fori_loop(done, steps, step, 0)

        with scope("exchange"):
            mine = acc_own[:rank, :] + acc_own[rank:, :]
            pair = acc_pair[:rank, :] + acc_pair[rank:, :]
            for h, whole in enumerate((pair, mine)):
                part[h] = whole
                top = top_of(whole)
                part_top[h] = top
                coded_part = encode_even(whole, top)
                for g in range(fs):
                    part_out[g, h] = coded_part[g * band:(g + 1) * band]
            for d in fs_peers:
                send(part_top, part_top_in.at[f], mark_send, mark_recv, {"fs": d})
                send(part_out.at[d], part_in.at[f], part_send, part_recv, {"fs": d})
        with scope("part_wait"):
            landed(part_top_in.at[pl.ds(0, fs - 1)], mark_recv)
            landed(part_in.at[pl.ds(0, fs - 1)], part_recv)
        with scope("sum_out"):
            power = jnp.zeros((1, columns), F32)
            for h, out in ((0, stage), (1, own_rows(o_all))):
                whole = part[h, pl.ds(pl.multiple_of(f * band, band), band), :]
                for d in fs_peers:
                    whole = whole + decode_even(part_in[d, h], part_top_in[d, h])
                out[...] = whole
                power = power + jnp.sum(whole * whole, axis=0, keepdims=True)
            me = f * chips + chip
            sums[me] = power

            def spread(i, j, c):
                where = {"fs": lax.rem(f + i, fs), "tp": 2 * lax.rem(chip + j, chips) + c}
                send(sums.at[me], sums.at[me], sum_send, sum_recv, where)

            if fs * chips <= 16:
                for i in range(fs - 1, -1, -1):
                    for j in range(chips):
                        for c in range(2):
                            if (i, j, c) != (0, 0, 1):
                                spread(i, j, c)
            else:
                def spread_one(k, _):
                    spread(k // (2 * chips), (k // 2) % chips, k % 2)
                    return 0

                spread(0, 0, 0)
                lax.fori_loop(2, 2 * fs * chips, spread_one, 0)
            here = own_rows(o_all)
            for d in fs_peers:
                send(here, here, all_send.at[0], all_recv, {"fs": d})
                send(stage, here, all_send.at[1], all_recv, {"fs": d, "tp": t - 1})
            send(stage, here, all_send.at[1], all_recv, partner)

    @pl.when(aide)
    def _():
        pass_right(chip == 0)
        pass_left(chip == last)
        for i, rows in enumerate(pieces):
            heads_load[i].wait()
            send(heads_v.at[rows], heads_in.at[rows], heads_send, heads_recv.at[i], partner)
        send_moments()
        with scope("masters_encode"):
            masters_encode()
        for d in fs_peers:
            send(mas_top.at[f], mas_top.at[f], mast_send[0], mast_recv, {"fs": d})
            send(mas.at[f], mas.at[f], mas_send[0], mas_recv, {"fs": d})
        ocot_load.wait()
        send(ocot_v, ocot_in, ocot_send, ocot_recv, partner)
        pass_right((chip > 0) & (chip < near))
        pass_left((chip < last) & (chip >= near))
        with scope("value_load"):
            for load in (vfac_load, vcot_load, vin_load):
                load.wait()
        with scope("value_own"):
            total = jnp.zeros((2 * rank, columns), F32)
            stride = image_v.shape[2]
            value_factor = vfac_v[...].astype(F32).T.astype(BF16)
            for i in range(tokens // stride):
                rows = pl.ds(i * stride, stride)
                two = split(against(value_factor, vcot_v[rows, :]), 0)
                image_v[i] = two
                total = total + jnp.dot(two, vin_v[0, rows, :], preferred_element_type=F32)
            totals_v = [total]
        with scope("gift"):
            landed(vin_v.at[1], gift_recv[0])
        with scope("value_pair"):
            total = jnp.zeros((2 * rank, columns), F32)
            for i in range(tokens // stride):
                total = total + jnp.dot(image_v[i], vin_v[1, pl.ds(i * stride, stride), :], preferred_element_type=F32)
            totals_v.append(total)
            for h, total in enumerate(totals_v):
                mine = total[:rank] + total[rank:]
                top = top_of(mine)
                value_top[f, h] = top
                value_swap[f, h] = encode_even(mine, top)
            for d in fs_peers:
                send(value_top.at[f], value_top.at[f], value_mark_send, value_mark_recv, {"fs": d})
                send(value_swap.at[f], value_swap.at[f], value_swap_send, value_swap_recv, {"fs": d})
        with scope("value_moments"):
            vm12_load.wait()
            landed(v1_v.at[1], gift_recv[1])
            landed(v2_v.at[1], gift_recv[2])
            for i, local in enumerate((v1_v, v2_v)):
                for h in range(2):
                    top = top_of(local[h])
                    value_momt[f, i, h] = top
                    value_mom[f, i, h] = encode_even(local[h], top)
            for d in fs_peers:
                send(value_momt.at[f], value_momt.at[f], value_momt_send, value_momt_recv, {"fs": d})
                send(value_mom.at[f], value_mom.at[f], value_mom_send, value_mom_recv, {"fs": d})
        with scope("give"):
            landed(pair_mast, give_recv[0])
            landed(pair_mas, give_recv[1])
        for d in fs_peers:
            there = {"fs": d, "tp": t + 1}
            send(pair_mast, mas_top.at[f], mast_send[1], mast_recv, there)
            send(pair_mas, mas.at[f], mas_send[1], mas_recv, there)
        with scope("value_masters"):
            vmas_load.wait()
            landed(vm_v.at[1], gift_recv[3])
            for h in range(2):
                top = top_of(vm_v[h])
                value_mast[f, h] = top
                value_mas[f, h] = encode_even(vm_v[h], top)
            for d in fs_peers:
                send(value_mast.at[f], value_mast.at[f], value_mast_send, value_mast_recv, {"fs": d})
                send(value_mas.at[f], value_mas.at[f], value_mas_send, value_mas_recv, {"fs": d})
        pass_right((chip >= near) & (chip < last))
        pass_left((chip > 0) & (chip < near))

        @pl.when(chip == 0)
        def _():
            pl.semaphore_wait(seen.at[1], 1)

        @pl.when(chip == last)
        def _():
            pl.semaphore_wait(seen.at[0], 1)

        with scope("value_swap_wait"):
            landed(value_top.at[pl.ds(0, fs - 1)], value_mark_recv)
            landed(value_swap.at[pl.ds(0, fs - 1)], value_swap_recv)
        power = jnp.zeros((1, columns), F32)
        for h in range(2):
            whole = decode_even(value_swap[0, h], value_top[0, h])
            for g in range(1, fs):
                whole = whole + decode_even(value_swap[g, h], value_top[g, h])
            proj_v[h] = whole
            power = power + jnp.sum(whole * whole, axis=0, keepdims=True)
        value_sums[chip] = power
        for j in range(1, chips):
            where = {"tp": lax.rem(t + 2 * j, tp)}
            send(value_sums.at[chip], value_sums.at[chip], value_sum_send, value_sum_recv, where)
        with scope("value_sums_wait"):
            landed(value_sums.at[pl.ds(0, chips - 1)], value_sum_recv)
        total = jnp.sum(jnp.sum(value_sums[...], axis=0), axis=1, keepdims=True)
        scale = lax.rsqrt(total / (rank * columns * tp) + 1e-06)
        for h, first_out, second_out in ((0, v_first, v_second), (1, back_first, back_second)):
            scaled = scale * proj_v[h, pl.ds(pl.multiple_of(f * band, band), band), :]
            first_out[...] = 0.9 * v1_v[h] + 0.1 * scaled
            second_out[...] = 0.95 * v2_v[h] + 0.05 * scaled * scaled
        send(back_first, v_first, back_send[0], back_recv.at[0], partner)
        send(back_second, v_second, back_send[0], back_recv.at[0], partner)
        rows = vfac_v[...]
        rows = jnp.concatenate([rows, rows], axis=1)
        with scope("mom_wait"):
            landed(value_momt.at[pl.ds(0, fs - 1)], value_momt_recv)
            landed(value_mom.at[pl.ds(0, fs - 1)], value_mom_recv)
            landed(value_mast.at[pl.ds(0, fs - 1)], value_mast_recv)
            landed(value_mas.at[pl.ds(0, fs - 1)], value_mas_recv)

        def gathered(i, h):
            return jnp.concatenate([decode_even(value_mom[g, i, h], value_momt[g, i, h]) for g in range(fs)], axis=0)

        for h, step_out, new_out, copy_out in ((1, back_step, back_new, back_copy), (0, v_step, v_new, v_copy)):
            scaled = scale * proj_v[h]
            first_new = 0.9 * gathered(0, h) + 0.1 * scaled
            second_new = 0.95 * gathered(1, h) + 0.05 * scaled * scaled
            direction = split(first_new / (jnp.sqrt(second_new) + 1e-08), 0)
            move_v[...] = jnp.dot(rows, direction, preferred_element_type=F32)
            move = own_rows(move_v)[...]
            step_out[...] = move
            new_out[...] = vm_v[h] - 0.002 * move
            for g in range(fs):
                these = pl.ds(g * v_rows, v_rows)
                old = decode_even(value_mas[g, h], value_mast[g, h])
                copy_out[these, :] = (old - 0.002 * move_v[these, :]).astype(BF16)
            if h == 1:
                send(back_copy, v_copy, copy_send, copy_recv, partner)
                send(back_step, v_step, back_send[1], back_recv.at[1], partner)
                send(back_new, v_new, back_send[1], back_recv.at[1], partner)

    with scope("masters_wait"):
        masters_end()
    with scope("mom_wait"):
        landed(mom_top.at[pl.ds(0, fs - 1)], momt_recv)
        landed(mom.at[pl.ds(0, fs - 1)], mom_recv)
        for i, whole in ((0, o1_all), (1, o2_all)):
            for g in range(fs):
                whole[pl.ds(g * band, band), :] = decode_even(mom[g, i], mom_top[g, i])
        left_here(mom_top.at[pl.ds(0, fs - 1)], momt_send)
        left_here(mom.at[pl.ds(0, fs - 1)], mom_send)

    n_sums = fs * chips
    bands = o_all.at[pl.ds(0, (fs - 1) * band)]
    with scope("drain"):
        @pl.when(aide)
        def _():
            left_here(heads_in, heads_send)
            left_here(ocot_in, ocot_send)
            left_here(value_swap.at[pl.ds(0, fs - 1)], value_swap_send)
            left_here(value_top.at[pl.ds(0, fs - 1)], value_mark_send)
            left_here(value_momt.at[pl.ds(0, fs - 1)], value_momt_send)
            left_here(value_mom.at[pl.ds(0, fs - 1)], value_mom_send)
            left_here(value_sums.at[pl.ds(0, chips - 1)], value_sum_send)
            for i in range(2):
                left_here(mas.at[pl.ds(0, fs - 1)], mas_send[i])
                left_here(mas_top.at[pl.ds(0, fs - 1)], mast_send[i])
            left_here(v1_v, back_send[0])
            left_here(vm_v, back_send[1])
            left_here(v_copy, copy_send)
            left_here(value_mast.at[pl.ds(0, fs - 1)], value_mast_send)
            left_here(value_mas.at[pl.ds(0, fs - 1)], value_mas_send)
            landed(o_all, all_recv)
            landed(sums.at[pl.ds(0, n_sums)], sum_recv)

        @pl.when(hub & (chip < last))
        def _():
            left_here(pre_out, pre_send)

        @pl.when(hub & (chip > 0))
        def _():
            left_here(suf_out, suf_send)

        @pl.when(hub)
        def _():
            for i, ref in enumerate((vin_v, v1_v, v2_v, vm_v)):
                left_here(ref.at[1], gift_send.at[i])
            left_here(pair_mast, give_send.at[0])
            left_here(pair_mas, give_send.at[1])
            left_here(part_top_in.at[pl.ds(0, fs - 1)], mark_send)
            left_here(part_in.at[pl.ds(0, fs - 1)], part_send)
            landed(v1_v, back_recv.at[0])
            landed(vm_v, back_recv.at[1])
            with scope("copy_wait"):
                landed(v_copy, copy_recv)
            with scope("all_wait"):
                landed(bands, all_recv)
                left_here(bands, all_send.at[0])
                left_here(o_all, all_send.at[1])
            with scope("sums_wait"):
                left_here(sums.at[pl.ds(0, 2 * n_sums - 1)], sum_send)
                landed(sums.at[pl.ds(0, n_sums - 1)], sum_recv)

    totals[...] = jnp.sum(sums[pl.ds(0, n_sums)], axis=0)


def finish_kernel(
    fs, tp,
    o_all, o1_all, o2_all, om_all, totals, ofac, omas, om1, om2, v_step, v_new, v_copy, v_first, v_second,
    v_step_out, v_new_out, v_copy_out, v_first_out, v_second_out,
    o_step_out, o_new_out, o_copy_out, o_first_out, o_second_out,
    step_v, new_v, copy_v, first_v, second_v, out_sem,
):
    f = lax.axis_index("fs")
    puts = []

    def put(src, dst):
        copy = pltpu.make_async_copy(src, dst, out_sem.at[len(puts)])
        copy.start()
        puts.append(copy)

    for src, dst in (
        (v_step, v_step_out), (v_new, v_new_out), (v_copy, v_copy_out), (v_first, v_first_out), (v_second, v_second_out),
    ):
        put(src, dst)
    rank, columns = o1_all.shape
    band = rank // fs
    total = jnp.sum(totals[...], axis=1, keepdims=True)
    scale = lax.rsqrt(total / (rank * columns * tp) + 1e-06)

    def moments(proj, first, second):
        scaled = scale * proj
        first_new = 0.9 * first + 0.1 * scaled
        second_new = 0.95 * second + 0.05 * scaled * scaled
        return first_new, second_new

    own_band = pl.ds(pl.multiple_of(f * band, band), band)
    with jax.named_scope("f_own"):
     first_v[...], second_v[...] = moments(o_all[own_band, :], om1[...], om2[...])
    put(first_v, o_first_out)
    put(second_v, o_second_out)
    first_new, second_new = moments(o_all[...], o1_all[...], o2_all[...])
    direction = split(first_new / (jnp.sqrt(second_new) + 1e-08), 0)

    def step_of(rows):
        left = ofac[rows, :]
        return jnp.dot(jnp.concatenate([left, left], axis=1), direction, preferred_element_type=F32)

    count = step_v.shape[0]
    own = pl.ds(pl.multiple_of(f * count, count), count)
    with jax.named_scope("f_step"):
        move = step_of(own)
        step_v[...] = move
    put(step_v, o_step_out)
    new_v[...] = omas[...] - 0.002 * move
    put(new_v, o_new_out)
    for i in range(fs):
        rows = pl.ds(i * count, count)
        copy_v[rows, :] = (om_all[rows, :] - 0.002 * step_of(rows)).astype(BF16)
        put(copy_v.at[rows], o_copy_out.at[rows])
    with jax.named_scope("f_wait"):
        for copy in puts:
            copy.wait()


def on_device(vin, vcot, vfac, vmas, vm1, vm2, heads, ocot, ofac, omas, om1, om2):
    fs = lax.axis_size("fs")
    tp = lax.axis_size("tp")
    rank = vfac.shape[1]
    band = rank // fs
    columns = vin.shape[1]
    tokens, width = heads.shape
    block = 128
    blocks = tokens // block
    stride = 256 if tokens % 256 == 0 else tokens

    def twice(array):
        return pltpu.VMEM((2, *array.shape), array.dtype)

    def like(array):
        return pltpu.VMEM(array.shape, array.dtype)

    def shape(*dims, kind=F32):
        return jax.ShapeDtypeStruct(dims, kind)

    def wide(*dims):
        return pltpu.VMEM(dims, F32)

    def coded():
        return pltpu.VMEM((blocks, rank, block), BF16)

    dma = pltpu.SemaphoreType.DMA
    v_rows, o_rows = vmas.shape[0], omas.shape[0]
    gathered = pl.pallas_call(
        functools.partial(gather_kernel, fs, tp),
        out_shape=(
            shape(rank, columns), shape(rank, columns), shape(rank, columns), shape(fs * o_rows, columns),
            shape(1, columns),
            shape(v_rows, columns), shape(v_rows, columns), shape(fs * v_rows, columns, kind=BF16),
            shape(band, columns), shape(band, columns),
        ),
        in_specs=[HBM] * 12,
        out_specs=(VMEM,) * 10,
        scratch_shapes=[
            like(vfac), like(ofac), twice(vin), like(vcot), pltpu.VMEM((tokens // stride, 2 * rank, stride), BF16),
            like(heads), like(heads), like(ocot), like(ocot), twice(vm1), twice(vm2), twice(vmas), like(omas), like(om1), like(om2),
            wide(blocks, rank, block), wide(blocks, rank, block), wide(blocks, rank, block),
            coded(), coded(), coded(), coded(), wide(1, block),
            wide(2 * rank, columns), wide(2 * rank, columns),
            wide(2, rank, columns), pltpu.VMEM((fs, 2, band, columns), BF16), wide(2, 1, columns),
            pltpu.VMEM((fs, 2, band, columns), BF16), wide(fs, 2, 1, columns), wide(band, columns),
            pltpu.VMEM((fs, 2, rank, columns), BF16), wide(fs, 2, 1, columns),
            wide(2, rank, columns),
            pltpu.VMEM((fs, 2, band, columns), BF16), wide(fs, 2, 1, columns),
            pltpu.VMEM((fs, 2, 2, band, columns), BF16), wide(fs, 2, 2, 1, columns), wide(fs * tp, 1, columns), wide(tp // 2, 1, columns),
            pltpu.VMEM((fs, o_rows, columns), BF16), wide(fs, 1, columns),
            pltpu.VMEM((o_rows, columns), BF16), wide(1, columns),
            wide(band, columns), wide(band, columns), wide(v_rows, columns), wide(v_rows, columns),
            pltpu.VMEM((fs * v_rows, columns), BF16),
            pltpu.VMEM((fs, 2, v_rows, columns), BF16), wide(fs, 2, 1, columns), wide(fs * v_rows, columns),
            dma((8 + len(growing(blocks)),)), dma((len(growing(blocks)),)), dma, dma((4,)),
            dma, dma((blocks,)), dma, dma((blocks,)),
            dma, dma, dma, dma, dma((2,)), dma, dma, dma, pltpu.SemaphoreType.REGULAR((2,)),
            dma, dma, dma, dma, dma, dma, dma((2,)), dma((2,)), dma,
        ],
        compiler_params=pltpu.CompilerParams(
            collective_id=0, has_side_effects=True, vmem_limit_bytes=32 * 1024 * 1024
        ),
    )(*(pltpu.with_memory_space_constraint(a, pltpu.HBM) for a in (
        vin, vcot, vfac, vmas, vm1, vm2, heads, ocot, ofac, omas, om1, om2
    )))
    o_all, o1_all, o2_all, om_all, totals, *values = gathered

    return pl.pallas_call(
        functools.partial(finish_kernel, fs, tp),
        out_shape=(
            shape(v_rows, columns), shape(v_rows, columns), shape(fs * v_rows, columns, kind=BF16),
            shape(band, columns), shape(band, columns),
            shape(o_rows, columns), shape(o_rows, columns), shape(fs * o_rows, columns, kind=BF16),
            shape(band, columns), shape(band, columns),
        ),
        in_specs=[VMEM] * 14,
        out_specs=(HBM,) * 10,
        scratch_shapes=[
            wide(o_rows, columns), wide(o_rows, columns), pltpu.VMEM((fs * o_rows, columns), BF16),
            wide(band, columns), wide(band, columns), dma((9 + fs,)),
        ],
        compiler_params=pltpu.CompilerParams(vmem_limit_bytes=24 * 1024 * 1024),
    )(o_all, o1_all, o2_all, om_all, totals, ofac, omas, om1, om2, *values)


def solution(mesh):
    both = P("fs", "tp")
    in_specs = (both, P("fs", None), P(), both, both, both, both, both, P(), both, both, both)
    out_specs = (
        both, both, P(None, "tp"), both, both, both, both, P(None, "tp"), both, both,
    )
    return jax.shard_map(
        on_device, mesh=mesh, in_specs=in_specs, out_specs=out_specs, check_vma=False
    )
```

```python
import functools

import jax
import jax.numpy as jnp
from jax import lax
from jax.experimental import pallas as pl
from jax.experimental.pallas import tpu as pltpu
from jax.sharding import PartitionSpec as P

MESH = pl.DeviceIdType.MESH
ANY = pl.BlockSpec(memory_space=pl.ANY)
HBM = pl.BlockSpec(memory_space=pltpu.HBM)
VMEM = pl.BlockSpec(memory_space=pltpu.VMEM)
BF16 = jnp.bfloat16
F32 = jnp.float32
PRE = 6
SUF = 7
LEVELS = 252.0
POWER = 7
PEAK = 240000.0
HEADS_BOUND = 6.0


def split(wide, axis):
    high = wide.astype(BF16)
    low = (wide - high.astype(F32)).astype(BF16)
    return jnp.concatenate([high, low], axis=axis)


def encode(x, top):
    u = x * (PEAK / top)
    u2 = u * u
    return (u2 * u2 * u2 * u).astype(BF16)


def decode(coded, top):
    y = coded.astype(F32)
    size = jnp.abs(y)
    root = jnp.exp(jnp.log(jnp.maximum(size, 1e-37)) * (1.0 / POWER))
    root = jnp.where(size < 2e-37, 0.0, root) * (top * (1.0 / PEAK))
    return jnp.where(y < 0.0, -root, root)


def encode_even(x, top):
    size = jnp.exp2(jnp.abs(x) * (LEVELS / top) - LEVELS / 2)
    return jnp.where(x < 0.0, -size, size).astype(BF16)


def decode_even(coded, top):
    y = coded.astype(F32)
    size = (jnp.log2(jnp.maximum(jnp.abs(y), 1e-38)) + LEVELS / 2) * (top * (1.0 / LEVELS))
    return jnp.where(y < 0.0, -size, size)


def top_of(x):
    return jnp.max(jnp.abs(x), axis=0, keepdims=True) * 1.02 + 1e-30


def growing(blocks):
    sizes = [1]
    while sum(sizes) < blocks:
        sizes.append(min(sum(sizes), blocks - sum(sizes)))
    return sizes


def gather_kernel(
    fs, tp,
    vin, vcot, vfac, vmas, vm1, vm2, heads, ocot, ofac, omas, om1, om2,
    o_all, o1_all, o2_all, om_all, totals, v_step, v_new, v_copy, v_first, v_second,
    vfac_v, ofac_v, vin_v, vcot_v, image_v, heads_v, heads_in, ocot_v, ocot_in, v1_v, v2_v, vm_v, om_v, o1_v, o2_v,
    own_v, left_v, right_v, pre_in, pre_out, suf_in, suf_out, bound, acc_own, acc_pair,
    part, part_out, part_top, part_in, part_top_in, stage, value_out, value_top, value_in, value_top_in, proj_v, mom, mom_top, dir_code, dir_top, sums, value_sums, mas, mas_top,
    pair_mas, pair_mast, back_first, back_second, back_step, back_new, back_copy, value_mas, value_mast, move_v,
    load_sem, heads_recv, ocot_recv, gift_send, pre_send, pre_recv, suf_send, suf_recv,
    part_send, part_recv, mark_send, mark_recv, all_send, all_recv, sum_send, sum_recv, seen,
    mom_send, mom_recv, momt_send, momt_recv, mas_recv, mast_recv, give_send, back_recv, copy_recv,
):
    f = lax.axis_index("fs")
    t = lax.axis_index("tp")
    chip = t // 2
    core = t % 2
    chips = tp // 2
    last = chips - 1
    rank = vfac.shape[1]
    band = rank // fs
    tokens, width = heads.shape
    columns = vin.shape[1]
    blocks, _, block = own_v.shape
    o_rows = omas.shape[0]
    v_rows = vmas.shape[0]
    scope = jax.named_scope
    hub = core == 1
    aide = core == 0
    at_last = (last - chip + last) // chips
    at_first = (chip + last) // chips

    spare = iter([sems.at[i] for sems in (pre_recv, suf_recv) for i in range(blocks)])
    heads_send, ocot_send = next(spare), next(spare)
    gift_recv = [next(spare) for _ in range(4)]
    value_swap_send, value_swap_recv, value_mark_send, value_mark_recv = (next(spare) for _ in range(4))
    value_sum_send, value_sum_recv = next(spare), next(spare)
    dir_send, dir_recv, dirt_send, dirt_recv = (next(spare) for _ in range(4))
    mas_send, mast_send, give_recv = ([next(spare) for _ in range(2)] for _ in range(3))
    back_send = [next(spare) for _ in range(2)]
    copy_send = next(spare)
    value_mas_send, value_mas_recv, value_mast_send, value_mast_recv = (next(spare) for _ in range(4))

    fs_peers = [3 - f, f + 1 - 2 * (f % 2), lax.rem(f + 2, fs)] if fs == 4 else [lax.rem(f + j, fs) for j in range(1, fs)]
    partner = {"tp": chip * 2 + (1 - core)}
    right = {"tp": lax.rem(t + 2, tp)}
    left = {"tp": lax.rem(t + tp - 2, tp)}

    def own_rows(ref):
        rows = ref.shape[0] // fs
        return ref.at[pl.ds(pl.multiple_of(f * rows, rows), rows)]

    sizes = growing(blocks)
    count = len(sizes)
    starts = [sum(sizes[:i]) for i in range(count)]
    pieces = [pl.ds(a * block, n * block) for a, n in zip(starts, sizes)]

    def loading(i, src, dst):
        return pltpu.make_async_copy(src, dst, load_sem.at[i])

    heads_load = [loading(i, heads.at[rows], heads_v.at[rows]) for i, rows in enumerate(pieces)]
    om1_load = loading(count, om1, o1_v)
    om2_load = loading(count, om2, o2_v)
    om12_load = loading(count, om_v.at[pl.ds(0, 2 * band)], om_v.at[pl.ds(0, 2 * band)])
    omas_load = loading(count + 2, omas, om_v)
    ocot_load = loading(count + 3, ocot, ocot_v)
    ofac_load = loading(count + 4, ofac, ofac_v)
    vfac_load = loading(count + 4, vfac, vfac_v)
    vcot_load = loading(count + 5, vcot, vcot_v)
    vin_load = loading(count + 6, vin, vin_v.at[0])
    vm1_load = loading(count + 1, vm1, v1_v.at[0])
    vm2_load = loading(count + 1, vm2, v2_v.at[0])
    vm12_load = loading(count + 1, v1_v, v1_v)
    vmas_load = loading(count + 7, vmas, vm_v.at[0])

    heads_load[0].start()

    @pl.when(hub)
    def _():
        ofac_load.start()

    for load in (*heads_load[1:], om1_load, om2_load):
        load.start()

    @pl.when(hub)
    def _():
        for load in (omas_load, ocot_load):
            load.start()

    @pl.when(aide)
    def _():
        for load in (omas_load, ocot_load, vfac_load, vcot_load, vin_load, vm1_load, vm2_load, vmas_load):
            load.start()

    barrier = pltpu.get_barrier_semaphore()

    def signal(sem, where):
        pl.semaphore_signal(sem, inc=1, device_id=where, device_id_type=MESH)

    signal(barrier, partner)
    for d in fs_peers:
        signal(barrier, {"fs": d})

    @pl.when(chip > 0)
    def _():
        signal(barrier, left)

    @pl.when(chip < last)
    def _():
        signal(barrier, right)

    with scope("barrier"):
        pl.semaphore_wait(barrier, fs + at_first + at_last)

    def pass_right(where):
        @pl.when(where & (chip > 0))
        def _():
            pl.semaphore_wait(seen.at[0], 1)

        @pl.when(where & (chip < last))
        def _():
            signal(seen.at[0], right)

    def pass_left(where):
        @pl.when(where & (chip < last))
        def _():
            pl.semaphore_wait(seen.at[1], 1)

        @pl.when(where & (chip > 0))
        def _():
            signal(seen.at[1], left)

    near = chips // 2

    def remote(src, dst, send_sem, recv_sem, where):
        return pltpu.make_async_remote_copy(
            src_ref=src, dst_ref=dst, send_sem=send_sem, recv_sem=recv_sem,
            device_id=where, device_id_type=MESH,
        )

    def send(src, dst, send_sem, recv_sem, where):
        remote(src, dst, send_sem, recv_sem, where).start()

    def landed(dst, sem):
        remote(dst, dst, sem, sem, partner).wait_recv()

    def left_here(src, sem):
        remote(src, src, sem, sem, partner).wait_send()

    def factor_of(s):
        rows = ofac_v[pl.ds(pl.multiple_of(s * width, width), width), :]
        return rows.astype(F32).T.astype(BF16)

    def against(one, two):
        return lax.dot_general(one, two, (((1,), (1,)), ((), ())), preferred_element_type=F32)

    def to_right(k):
        return remote(pre_out.at[k], pre_in.at[k], pre_send, pre_recv.at[k], right)

    def to_left(k):
        return remote(suf_out.at[k], suf_in.at[k], suf_send, suf_recv.at[k], left)

    def send_moments():
        om12_load.wait()
        for i, local in enumerate((o1_v, o2_v)):
            top = top_of(local[...])
            mom_top[f, i] = top
            mom[f, i] = encode_even(local[...], top)
        for d in fs_peers:
            send(mom_top.at[f], mom_top.at[f], momt_send, momt_recv, {"fs": d})
            send(mom.at[f], mom.at[f], mom_send, mom_recv, {"fs": d})

    def masters_encode():
        omas_load.wait()
        top = top_of(om_v[...])
        mas_top[f] = top
        mas[f] = encode_even(om_v[...], top)

    def masters_end():
        landed(mas_top.at[pl.ds(0, fs - 1)], mast_recv)
        landed(mas.at[pl.ds(0, fs - 1)], mas_recv)
        for g in range(fs):
            om_all[pl.ds(g * o_rows, o_rows), :] = decode_even(mas[g], mas_top[g])

    late = at_first * at_last * SUF

    def step(i, _):
        k = i - PRE * chip

        @pl.when((chip > 0) & (k >= 0) & (k < blocks))
        def _():
            with scope("pre_wait"):
                landed(pre_in.at[k], pre_recv.at[k])
            left_v[k] = decode(pre_in[k], bound[...])

            @pl.when(chip < last)
            def _():
                pre_out[k] = encode(left_v[k] + own_v[k], bound[...])
                to_right(k).start()

        m = i - SUF * (last - chip)

        @pl.when((chip < last) & (m >= 0) & (m < blocks))
        def _():
            with scope("suf_wait"):
                landed(suf_in.at[m], suf_recv.at[m])
            right_v[m] = decode(suf_in[m], bound[...])

            @pl.when(chip > 0)
            def _():
                suf_out[m] = encode(right_v[m] + own_v[m], bound[...])
                to_left(m).start()

        n = i - late - jnp.maximum(PRE * chip, SUF * (last - chip))

        @pl.when((n >= 0) & (n < blocks) & (lax.rem(n + 2, 2) == 1))
        def _():
            with scope("acc"):
                image = jnp.concatenate([left_v[j] + own_v[j] + right_v[j] for j in (n - 1, n)], axis=1)
                two = split(image, 0)
                here = pl.ds(pl.multiple_of((n - 1) * block, block), 2 * block)
                acc_own[...] += jnp.dot(two, ocot_v[here, :], preferred_element_type=F32)
                acc_pair[...] += jnp.dot(two, ocot_in[here, :], preferred_element_type=F32)

        return 0

    steps = blocks + SUF * last

    @pl.when(hub)
    def _():
        for i, (src, dst) in enumerate(((vin, vin_v), (vm1, v1_v), (vm2, v2_v), (vmas, vm_v))):
            send(src, dst.at[1], gift_send.at[i], gift_recv[i], partner)
        send_moments()
        with scope("factor"):
            ofac_load.wait()
            reach = jnp.sum(jnp.abs(ofac_v[...].astype(F32)), axis=0, keepdims=True)
            top = jnp.max(reach, axis=1, keepdims=True) * (1.02 * HEADS_BOUND) + 1e-30
            bound[...] = jnp.broadcast_to(top, bound.shape)
            factor = jnp.concatenate([factor_of(t - 1), factor_of(t)], axis=1)
        for i, rows in enumerate(pieces):
            heads_load[i].wait()
            with scope("heads_in"):
                landed(heads_in.at[rows], heads_recv.at[i])
            with scope("own"):
                own = against(factor, jnp.concatenate([heads_in[rows, :], heads_v[rows, :]], axis=1))
                for k in range(sizes[i]):
                    own_v[starts[i] + k] = own[:, k * block:(k + 1) * block]

            @pl.when(chip == 0)
            def _():
                for k in range(starts[i], starts[i] + sizes[i]):
                    pre_out[k] = encode(own_v[k], bound[...])
                    to_right(k).start()

            @pl.when(chip == last)
            def _():
                for k in range(starts[i], starts[i] + sizes[i]):
                    suf_out[k] = encode(own_v[k], bound[...])
                    to_left(k).start()

        @pl.when(chip == 0)
        def _():
            left_v[...] = jnp.zeros_like(left_v)

        @pl.when(chip == last)
        def _():
            right_v[...] = jnp.zeros_like(right_v)

        acc_own[...] = jnp.zeros_like(acc_own)
        acc_pair[...] = jnp.zeros_like(acc_pair)
        with scope("masters_encode"):
            masters_encode()
        send(mas_top.at[f], pair_mast, give_send.at[0], give_recv[0], partner)
        send(mas.at[f], pair_mas, give_send.at[1], give_recv[1], partner)

        def output_cotangents():
            ocot_load.wait()
            landed(ocot_in, ocot_recv)

        done = 0
        for at, event in ((13, output_cotangents),):
            at = min(at, steps)
            lax.fori_loop(done, at, step, 0)
            done = at
            with scope(f"event{at}"):
                event()
        lax.fori_loop(done, steps, step, 0)

        with scope("exchange"):
            mine = acc_own[:rank, :] + acc_own[rank:, :]
            pair = acc_pair[:rank, :] + acc_pair[rank:, :]
            for h, whole in enumerate((pair, mine)):
                part[h] = whole
                top = top_of(whole)
                part_top[h] = top
                coded_part = encode_even(whole, top)
                for g in range(fs):
                    part_out[g, h] = coded_part[g * band:(g + 1) * band]
            for d in fs_peers:
                send(part_top, part_top_in.at[f], mark_send, mark_recv, {"fs": d})
                send(part_out.at[d], part_in.at[f], part_send, part_recv, {"fs": d})
        with scope("part_wait"):
            landed(part_top_in.at[pl.ds(0, fs - 1)], mark_recv)
            landed(part_in.at[pl.ds(0, fs - 1)], part_recv)
        with scope("sum_out"):
            power = jnp.zeros((1, columns), F32)
            for h, out in ((0, stage), (1, own_rows(o_all))):
                whole = part[h, pl.ds(pl.multiple_of(f * band, band), band), :]
                for d in fs_peers:
                    whole = whole + decode_even(part_in[d, h], part_top_in[d, h])
                out[...] = whole
                power = power + jnp.sum(whole * whole, axis=0, keepdims=True)
            me = f * chips + chip
            sums[me] = power

            def spread(i, j, c):
                where = {"fs": lax.rem(f + i, fs), "tp": 2 * lax.rem(chip + j, chips) + c}
                send(sums.at[me], sums.at[me], sum_send, sum_recv, where)

            if fs * chips <= 16:
                for i in range(fs - 1, -1, -1):
                    for j in range(chips):
                        for c in range(2):
                            if (i, j, c) != (0, 0, 1):
                                spread(i, j, c)
            else:
                def spread_one(k, _):
                    spread(k // (2 * chips), (k // 2) % chips, k % 2)
                    return 0

                spread(0, 0, 0)
                lax.fori_loop(2, 2 * fs * chips, spread_one, 0)
            here = own_rows(o_all)
            for d in fs_peers:
                send(here, here, all_send.at[0], all_recv, {"fs": d})
                send(stage, here, all_send.at[1], all_recv, {"fs": d, "tp": t - 1})
            send(stage, here, all_send.at[1], all_recv, partner)

    @pl.when(aide)
    def _():
        pass_right(chip == 0)
        pass_left(chip == last)
        for i, rows in enumerate(pieces):
            heads_load[i].wait()
            send(heads_v.at[rows], heads_in.at[rows], heads_send, heads_recv.at[i], partner)
        send_moments()
        with scope("masters_encode"):
            masters_encode()
        for d in fs_peers:
            send(mas_top.at[f], mas_top.at[f], mast_send[0], mast_recv, {"fs": d})
            send(mas.at[f], mas.at[f], mas_send[0], mas_recv, {"fs": d})
        ocot_load.wait()
        send(ocot_v, ocot_in, ocot_send, ocot_recv, partner)
        pass_right((chip > 0) & (chip < near))
        pass_left((chip < last) & (chip >= near))
        with scope("value_load"):
            for load in (vfac_load, vcot_load, vin_load):
                load.wait()
        with scope("pass"):
            pass_right((chip >= near) & (chip < last))
            pass_left((chip > 0) & (chip < near))
        with scope("value_own"):
            total = jnp.zeros((2 * rank, columns), F32)
            stride = image_v.shape[2]
            value_factor = vfac_v[...].astype(F32).T.astype(BF16)
            for i in range(tokens // stride):
                rows = pl.ds(i * stride, stride)
                two = split(against(value_factor, vcot_v[rows, :]), 0)
                image_v[i] = two
                total = total + jnp.dot(two, vin_v[0, rows, :], preferred_element_type=F32)
            totals_v = [total]
        with scope("gift"):
            landed(vin_v.at[1], gift_recv[0])
        with scope("value_pair"):
            total = jnp.zeros((2 * rank, columns), F32)
            for i in range(tokens // stride):
                total = total + jnp.dot(image_v[i], vin_v[1, pl.ds(i * stride, stride), :], preferred_element_type=F32)
            totals_v.append(total)
            for h, total in enumerate(totals_v):
                mine = total[:rank] + total[rank:]
                proj_v[h] = mine
                top = top_of(mine)
                value_top[h] = top
                coded_part = encode_even(mine, top)
                for g in range(fs):
                    value_out[g, h] = coded_part[g * band:(g + 1) * band]
        with scope("seen"):
            @pl.when(chip == 0)
            def _():
                pl.semaphore_wait(seen.at[1], 1)

            @pl.when(chip == last)
            def _():
                pl.semaphore_wait(seen.at[0], 1)

        for d in fs_peers:
            send(value_top, value_top_in.at[f], value_mark_send, value_mark_recv, {"fs": d})
            send(value_out.at[d], value_in.at[f], value_swap_send, value_swap_recv, {"fs": d})
        with scope("give"):
            landed(pair_mast, give_recv[0])
            landed(pair_mas, give_recv[1])
        for d in fs_peers:
            there = {"fs": d, "tp": t + 1}
            send(pair_mast, mas_top.at[f], mast_send[1], mast_recv, there)
            send(pair_mas, mas.at[f], mas_send[1], mas_recv, there)
        with scope("value_masters"):
            vmas_load.wait()
            landed(vm_v.at[1], gift_recv[3])
            for h in range(2):
                top = top_of(vm_v[h])
                value_mast[f, h] = top
                value_mas[f, h] = encode_even(vm_v[h], top)
        with scope("value_swap_wait"):
            landed(value_top_in.at[pl.ds(0, fs - 1)], value_mark_recv)
            landed(value_in.at[pl.ds(0, fs - 1)], value_swap_recv)
        power = jnp.zeros((1, columns), F32)
        own_band = pl.ds(pl.multiple_of(f * band, band), band)
        for h in range(2):
            whole = proj_v[h, own_band, :]
            for d in fs_peers:
                whole = whole + decode_even(value_in[d, h], value_top_in[d, h])
            proj_v[h, own_band, :] = whole
            power = power + jnp.sum(whole * whole, axis=0, keepdims=True)
        value_me = f * chips + chip
        value_sums[value_me] = power

        def value_spread(i, j):
            where = {"fs": lax.rem(f + i, fs), "tp": 2 * lax.rem(chip + j, chips)}
            send(value_sums.at[value_me], value_sums.at[value_me], value_sum_send, value_sum_recv, where)

        if fs * chips <= 16:
            for i in range(fs - 1, -1, -1):
                for j in range(chips):
                    if (i, j) != (0, 0):
                        value_spread(i, j)
        else:
            def value_spread_one(k, _):
                value_spread(k // chips, k % chips)
                return 0

            lax.fori_loop(1, fs * chips, value_spread_one, 0)
        for d in fs_peers:
            send(value_mast.at[f], value_mast.at[f], value_mast_send, value_mast_recv, {"fs": d})
            send(value_mas.at[f], value_mas.at[f], value_mas_send, value_mas_recv, {"fs": d})
        vm12_load.wait()
        landed(v1_v.at[1], gift_recv[1])
        landed(v2_v.at[1], gift_recv[2])
        with scope("value_sums_wait"):
            landed(value_sums.at[pl.ds(0, fs * chips - 1)], value_sum_recv)
        total = jnp.sum(jnp.sum(value_sums[...], axis=0), axis=1, keepdims=True)
        scale = lax.rsqrt(total / (rank * columns * tp) + 1e-06)
        for h, first_out, second_out in ((0, v_first, v_second), (1, back_first, back_second)):
            scaled = scale * proj_v[h, own_band, :]
            first_new = 0.9 * v1_v[h] + 0.1 * scaled
            second_new = 0.95 * v2_v[h] + 0.05 * scaled * scaled
            first_out[...] = first_new
            second_out[...] = second_new
            direction = first_new / (jnp.sqrt(second_new) + 1e-08)
            top = top_of(direction)
            dir_top[f, h] = top
            dir_code[f, h] = encode_even(direction, top)
        for d in fs_peers:
            send(dir_top.at[f], dir_top.at[f], dirt_send, dirt_recv, {"fs": d})
            send(dir_code.at[f], dir_code.at[f], dir_send, dir_recv, {"fs": d})
        send(back_first, v_first, back_send[0], back_recv.at[0], partner)
        send(back_second, v_second, back_send[0], back_recv.at[0], partner)
        rows = vfac_v[...]
        rows = jnp.concatenate([rows, rows], axis=1)
        with scope("dir_wait"):
            landed(dir_top.at[pl.ds(0, fs - 1)], dirt_recv)
            landed(dir_code.at[pl.ds(0, fs - 1)], dir_recv)
            landed(value_mast.at[pl.ds(0, fs - 1)], value_mast_recv)
            landed(value_mas.at[pl.ds(0, fs - 1)], value_mas_recv)

        for h, step_out, new_out, copy_out in ((1, back_step, back_new, back_copy), (0, v_step, v_new, v_copy)):
            direction = jnp.concatenate([decode_even(dir_code[g, h], dir_top[g, h]) for g in range(fs)], axis=0)
            direction = split(direction, 0)
            move_v[...] = jnp.dot(rows, direction, preferred_element_type=F32)
            move = own_rows(move_v)[...]
            step_out[...] = move
            new_out[...] = vm_v[h] - 0.002 * move
            for g in range(fs):
                these = pl.ds(g * v_rows, v_rows)
                old = decode_even(value_mas[g, h], value_mast[g, h])
                copy_out[these, :] = (old - 0.002 * move_v[these, :]).astype(BF16)
            if h == 1:
                send(back_copy, v_copy, copy_send, copy_recv, partner)
                send(back_step, v_step, back_send[1], back_recv.at[1], partner)
                send(back_new, v_new, back_send[1], back_recv.at[1], partner)

    with scope("masters_wait"):
        masters_end()
    with scope("mom_wait"):
        landed(mom_top.at[pl.ds(0, fs - 1)], momt_recv)
        landed(mom.at[pl.ds(0, fs - 1)], mom_recv)
        for i, whole in ((0, o1_all), (1, o2_all)):
            for g in range(fs):
                whole[pl.ds(g * band, band), :] = decode_even(mom[g, i], mom_top[g, i])
        left_here(mom_top.at[pl.ds(0, fs - 1)], momt_send)
        left_here(mom.at[pl.ds(0, fs - 1)], mom_send)

    n_sums = fs * chips
    bands = o_all.at[pl.ds(0, (fs - 1) * band)]
    with scope("drain"):
        @pl.when(aide)
        def _():
            left_here(heads_in, heads_send)
            left_here(ocot_in, ocot_send)
            left_here(value_in.at[pl.ds(0, fs - 1)], value_swap_send)
            left_here(value_top_in.at[pl.ds(0, fs - 1)], value_mark_send)
            left_here(dir_top.at[pl.ds(0, fs - 1)], dirt_send)
            left_here(dir_code.at[pl.ds(0, fs - 1)], dir_send)
            left_here(value_sums.at[pl.ds(0, n_sums - 1)], value_sum_send)
            for i in range(2):
                left_here(mas.at[pl.ds(0, fs - 1)], mas_send[i])
                left_here(mas_top.at[pl.ds(0, fs - 1)], mast_send[i])
            left_here(v1_v, back_send[0])
            left_here(vm_v, back_send[1])
            left_here(v_copy, copy_send)
            left_here(value_mast.at[pl.ds(0, fs - 1)], value_mast_send)
            left_here(value_mas.at[pl.ds(0, fs - 1)], value_mas_send)
            landed(o_all, all_recv)
            landed(sums.at[pl.ds(0, n_sums)], sum_recv)

        @pl.when(hub & (chip < last))
        def _():
            left_here(pre_out, pre_send)

        @pl.when(hub & (chip > 0))
        def _():
            left_here(suf_out, suf_send)

        @pl.when(hub)
        def _():
            for i, ref in enumerate((vin_v, v1_v, v2_v, vm_v)):
                left_here(ref.at[1], gift_send.at[i])
            left_here(pair_mast, give_send.at[0])
            left_here(pair_mas, give_send.at[1])
            left_here(part_top_in.at[pl.ds(0, fs - 1)], mark_send)
            left_here(part_in.at[pl.ds(0, fs - 1)], part_send)
            landed(v1_v, back_recv.at[0])
            landed(vm_v, back_recv.at[1])
            with scope("copy_wait"):
                landed(v_copy, copy_recv)
            with scope("all_wait"):
                landed(bands, all_recv)
                left_here(bands, all_send.at[0])
                left_here(o_all, all_send.at[1])
            with scope("sums_wait"):
                left_here(sums.at[pl.ds(0, 2 * n_sums - 1)], sum_send)
                landed(sums.at[pl.ds(0, n_sums - 1)], sum_recv)

    totals[...] = jnp.sum(sums[pl.ds(0, n_sums)], axis=0)


def finish_kernel(
    fs, tp,
    o_all, o1_all, o2_all, om_all, totals, ofac, omas, om1, om2, v_step, v_new, v_copy, v_first, v_second,
    v_step_out, v_new_out, v_copy_out, v_first_out, v_second_out,
    o_step_out, o_new_out, o_copy_out, o_first_out, o_second_out,
    step_v, new_v, copy_v, first_v, second_v, out_sem,
):
    f = lax.axis_index("fs")
    puts = []

    def put(src, dst):
        copy = pltpu.make_async_copy(src, dst, out_sem.at[len(puts)])
        copy.start()
        puts.append(copy)

    for src, dst in (
        (v_step, v_step_out), (v_new, v_new_out), (v_copy, v_copy_out), (v_first, v_first_out), (v_second, v_second_out),
    ):
        put(src, dst)
    rank, columns = o1_all.shape
    band = rank // fs
    total = jnp.sum(totals[...], axis=1, keepdims=True)
    scale = lax.rsqrt(total / (rank * columns * tp) + 1e-06)

    def moments(proj, first, second):
        scaled = scale * proj
        first_new = 0.9 * first + 0.1 * scaled
        second_new = 0.95 * second + 0.05 * scaled * scaled
        return first_new, second_new

    own_band = pl.ds(pl.multiple_of(f * band, band), band)
    with jax.named_scope("f_own"):
     first_v[...], second_v[...] = moments(o_all[own_band, :], om1[...], om2[...])
    put(first_v, o_first_out)
    put(second_v, o_second_out)
    first_new, second_new = moments(o_all[...], o1_all[...], o2_all[...])
    direction = split(first_new / (jnp.sqrt(second_new) + 1e-08), 0)

    def step_of(rows):
        left = ofac[rows, :]
        return jnp.dot(jnp.concatenate([left, left], axis=1), direction, preferred_element_type=F32)

    count = step_v.shape[0]
    own = pl.ds(pl.multiple_of(f * count, count), count)
    with jax.named_scope("f_step"):
        move = step_of(own)
        step_v[...] = move
    put(step_v, o_step_out)
    new_v[...] = omas[...] - 0.002 * move
    put(new_v, o_new_out)
    for i in range(fs):
        rows = pl.ds(i * count, count)
        copy_v[rows, :] = (om_all[rows, :] - 0.002 * step_of(rows)).astype(BF16)
        put(copy_v.at[rows], o_copy_out.at[rows])
    with jax.named_scope("f_wait"):
        for copy in puts:
            copy.wait()


def on_device(vin, vcot, vfac, vmas, vm1, vm2, heads, ocot, ofac, omas, om1, om2):
    fs = lax.axis_size("fs")
    tp = lax.axis_size("tp")
    rank = vfac.shape[1]
    band = rank // fs
    columns = vin.shape[1]
    tokens, width = heads.shape
    block = 128
    blocks = tokens // block
    stride = 256 if tokens % 256 == 0 else tokens

    def twice(array):
        return pltpu.VMEM((2, *array.shape), array.dtype)

    def like(array):
        return pltpu.VMEM(array.shape, array.dtype)

    def shape(*dims, kind=F32):
        return jax.ShapeDtypeStruct(dims, kind)

    def wide(*dims):
        return pltpu.VMEM(dims, F32)

    def coded():
        return pltpu.VMEM((blocks, rank, block), BF16)

    dma = pltpu.SemaphoreType.DMA
    v_rows, o_rows = vmas.shape[0], omas.shape[0]
    gathered = pl.pallas_call(
        functools.partial(gather_kernel, fs, tp),
        out_shape=(
            shape(rank, columns), shape(rank, columns), shape(rank, columns), shape(fs * o_rows, columns),
            shape(1, columns),
            shape(v_rows, columns), shape(v_rows, columns), shape(fs * v_rows, columns, kind=BF16),
            shape(band, columns), shape(band, columns),
        ),
        in_specs=[HBM] * 12,
        out_specs=(VMEM,) * 10,
        scratch_shapes=[
            like(vfac), like(ofac), twice(vin), like(vcot), pltpu.VMEM((tokens // stride, 2 * rank, stride), BF16),
            like(heads), like(heads), like(ocot), like(ocot), twice(vm1), twice(vm2), twice(vmas), like(omas), like(om1), like(om2),
            wide(blocks, rank, block), wide(blocks, rank, block), wide(blocks, rank, block),
            coded(), coded(), coded(), coded(), wide(1, block),
            wide(2 * rank, columns), wide(2 * rank, columns),
            wide(2, rank, columns), pltpu.VMEM((fs, 2, band, columns), BF16), wide(2, 1, columns),
            pltpu.VMEM((fs, 2, band, columns), BF16), wide(fs, 2, 1, columns), wide(band, columns),
            pltpu.VMEM((fs, 2, band, columns), BF16), wide(2, 1, columns),
            pltpu.VMEM((fs, 2, band, columns), BF16), wide(fs, 2, 1, columns), wide(2, rank, columns),
            pltpu.VMEM((fs, 2, band, columns), BF16), wide(fs, 2, 1, columns),
            pltpu.VMEM((fs, 2, band, columns), BF16), wide(fs, 2, 1, columns),
            wide(fs * tp, 1, columns), wide(fs * tp // 2, 1, columns),
            pltpu.VMEM((fs, o_rows, columns), BF16), wide(fs, 1, columns),
            pltpu.VMEM((o_rows, columns), BF16), wide(1, columns),
            wide(band, columns), wide(band, columns), wide(v_rows, columns), wide(v_rows, columns),
            pltpu.VMEM((fs * v_rows, columns), BF16),
            pltpu.VMEM((fs, 2, v_rows, columns), BF16), wide(fs, 2, 1, columns), wide(fs * v_rows, columns),
            dma((8 + len(growing(blocks)),)), dma((len(growing(blocks)),)), dma, dma((4,)),
            dma, dma((blocks,)), dma, dma((blocks,)),
            dma, dma, dma, dma, dma((2,)), dma, dma, dma, pltpu.SemaphoreType.REGULAR((2,)),
            dma, dma, dma, dma, dma, dma, dma((2,)), dma((2,)), dma,
        ],
        compiler_params=pltpu.CompilerParams(
            collective_id=0, has_side_effects=True, vmem_limit_bytes=32 * 1024 * 1024
        ),
    )(*(pltpu.with_memory_space_constraint(a, pltpu.HBM) for a in (
        vin, vcot, vfac, vmas, vm1, vm2, heads, ocot, ofac, omas, om1, om2
    )))
    o_all, o1_all, o2_all, om_all, totals, *values = gathered

    return pl.pallas_call(
        functools.partial(finish_kernel, fs, tp),
        out_shape=(
            shape(v_rows, columns), shape(v_rows, columns), shape(fs * v_rows, columns, kind=BF16),
            shape(band, columns), shape(band, columns),
            shape(o_rows, columns), shape(o_rows, columns), shape(fs * o_rows, columns, kind=BF16),
            shape(band, columns), shape(band, columns),
        ),
        in_specs=[VMEM] * 14,
        out_specs=(HBM,) * 10,
        scratch_shapes=[
            wide(o_rows, columns), wide(o_rows, columns), pltpu.VMEM((fs * o_rows, columns), BF16),
            wide(band, columns), wide(band, columns), dma((9 + fs,)),
        ],
        compiler_params=pltpu.CompilerParams(vmem_limit_bytes=24 * 1024 * 1024),
    )(o_all, o1_all, o2_all, om_all, totals, ofac, omas, om1, om2, *values)


def solution(mesh):
    both = P("fs", "tp")
    in_specs = (both, P("fs", None), P(), both, both, both, both, both, P(), both, both, both)
    out_specs = (
        both, both, P(None, "tp"), both, both, both, both, P(None, "tp"), both, both,
    )
    return jax.shard_map(
        on_device, mesh=mesh, in_specs=in_specs, out_specs=out_specs, check_vma=False
    )
```

```python
import functools

import jax
import jax.numpy as jnp
from jax import lax
from jax.experimental import pallas as pl
from jax.experimental.pallas import tpu as pltpu
from jax.sharding import PartitionSpec as P

MESH = pl.DeviceIdType.MESH
ANY = pl.BlockSpec(memory_space=pl.ANY)
HBM = pl.BlockSpec(memory_space=pltpu.HBM)
VMEM = pl.BlockSpec(memory_space=pltpu.VMEM)
BF16 = jnp.bfloat16
F32 = jnp.float32
PRE = 6
SUF = 7
LEVELS = 250.0
POWER = 7
PEAK = 240000.0
HEADS_BOUND = 6.0


def split(wide, axis):
    high = wide.astype(BF16)
    low = (wide - high.astype(F32)).astype(BF16)
    return jnp.concatenate([high, low], axis=axis)


def encode(x, top):
    u = x * (PEAK / top)
    u2 = u * u
    return (u2 * u2 * u2 * u).astype(BF16)


def decode(coded, top):
    y = coded.astype(F32)
    size = jnp.abs(y)
    root = jnp.exp(jnp.log(jnp.maximum(size, 1e-37)) * (1.0 / POWER))
    root = jnp.where(size < 2e-37, 0.0, root) * (top * (1.0 / PEAK))
    return jnp.where(y < 0.0, -root, root)


def encode_even(x, top):
    size = jnp.exp2(jnp.abs(x) * (LEVELS / top) - LEVELS / 2)
    return jnp.where(x < 0.0, -size, size).astype(BF16)


def decode_even(coded, top):
    y = coded.astype(F32)
    level = jnp.maximum(jnp.log2(jnp.maximum(jnp.abs(y), 1e-38)) + LEVELS / 2, 0.0)
    size = level * (top * (1.0 / LEVELS))
    return jnp.where(y < 0.0, -size, size)


def top_of(x):
    return jnp.max(jnp.abs(x), axis=0, keepdims=True) * 1.02 + 1e-30


def growing(blocks):
    sizes = [1]
    while sum(sizes) < blocks:
        sizes.append(min(sum(sizes), blocks - sum(sizes)))
    return sizes


def gather_kernel(
    fs, tp,
    vin, vcot, vfac, vmas, vm1, vm2, heads, ocot, ofac, omas, om1, om2,
    o_all, o1_all, o2_all, om_all, totals, v_step, v_new, v_copy, v_first, v_second,
    vfac_v, ofac_v, vin_v, vcot_v, image_v, heads_v, heads_in, ocot_v, ocot_in, v1_v, v2_v, vm_v, om_v, o1_v, o2_v,
    own_v, left_v, right_v, pre_in, pre_out, suf_in, suf_out, bound, acc_own, acc_pair,
    part, part_out, part_top, part_in, part_top_in, stage, value_out, value_top, value_in, value_top_in, proj_v, mom, mom_top, dir_code, dir_top, sums, value_sums, mas, mas_top,
    back_first, back_second, back_step, back_new, back_copy, value_mas, value_mast, move_v,
    load_sem, heads_recv, ocot_recv, gift_send, pre_send, pre_recv, suf_send, suf_recv,
    part_send, part_recv, mark_send, mark_recv, all_send, all_recv, sum_send, sum_recv, seen,
    mom_send, mom_recv, momt_send, momt_recv, mas_recv, mast_recv, give_send, back_recv, copy_recv,
):
    f = lax.axis_index("fs")
    t = lax.axis_index("tp")
    chip = t // 2
    core = t % 2
    chips = tp // 2
    last = chips - 1
    rank = vfac.shape[1]
    band = rank // fs
    tokens, width = heads.shape
    columns = vin.shape[1]
    blocks, _, block = own_v.shape
    o_rows = omas.shape[0]
    v_rows = vmas.shape[0]
    scope = jax.named_scope
    hub = core == 1
    aide = core == 0
    at_last = (last - chip + last) // chips
    at_first = (chip + last) // chips

    spare = iter([sems.at[i] for sems in (pre_recv, suf_recv, heads_recv) for i in range(sems.shape[0])])
    heads_send, ocot_send = next(spare), next(spare)
    gift_recv = [next(spare) for _ in range(4)]
    value_swap_send, value_swap_recv, value_mark_send, value_mark_recv = (next(spare) for _ in range(4))
    value_sum_send, value_sum_recv = next(spare), next(spare)
    dir_send, dir_recv, dirt_send, dirt_recv = (next(spare) for _ in range(4))
    mas_send, mast_send = next(spare), next(spare)
    back_send = [next(spare) for _ in range(2)]
    copy_send = next(spare)
    value_mas_send, value_mas_recv, value_mast_send, value_mast_recv = (next(spare) for _ in range(4))

    fs_peers = [3 - f, f + 1 - 2 * (f % 2), lax.rem(f + 2, fs)] if fs == 4 else [lax.rem(f + j, fs) for j in range(1, fs)]
    partner = {"tp": chip * 2 + (1 - core)}
    right = {"tp": lax.rem(t + 2, tp)}
    left = {"tp": lax.rem(t + tp - 2, tp)}

    def own_rows(ref):
        rows = ref.shape[0] // fs
        return ref.at[pl.ds(pl.multiple_of(f * rows, rows), rows)]

    sizes = growing(blocks)
    count = len(sizes)
    starts = [sum(sizes[:i]) for i in range(count)]
    pieces = [pl.ds(a * block, n * block) for a, n in zip(starts, sizes)]

    def loading(i, src, dst):
        return pltpu.make_async_copy(src, dst, load_sem.at[i])

    heads_load = [loading(i, heads.at[rows], heads_v.at[rows]) for i, rows in enumerate(pieces)]
    om1_load = loading(count, om1, o1_v)
    om2_load = loading(count, om2, o2_v)
    om12_load = loading(count, om_v.at[pl.ds(0, 2 * band)], om_v.at[pl.ds(0, 2 * band)])
    omas_load = loading(count + 1, omas, om_v)
    ocot_load = loading(count + 2, ocot, ocot_v)
    ofac_load = loading(count + 3, ofac, ofac_v)
    vfac_load = pltpu.make_async_copy(vfac, vfac_v, next(spare))
    vcot_load = pltpu.make_async_copy(vcot, vcot_v, next(spare))
    vin_load = pltpu.make_async_copy(vin, vin_v.at[0], next(spare))
    vmas_load = pltpu.make_async_copy(vmas, vm_v.at[0], next(spare))
    moments_sem = next(spare)
    vm1_load = pltpu.make_async_copy(vm1, v1_v.at[0], moments_sem)
    vm2_load = pltpu.make_async_copy(vm2, v2_v.at[0], moments_sem)
    vm12_load = pltpu.make_async_copy(v1_v, v1_v, moments_sem)

    heads_load[0].start()

    @pl.when(hub)
    def _():
        ofac_load.start()

    for load in (*heads_load[1:], om1_load, om2_load):
        load.start()

    @pl.when(hub)
    def _():
        for load in (omas_load, ocot_load):
            load.start()

    @pl.when(aide)
    def _():
        for load in (omas_load, ocot_load, vfac_load, vcot_load, vin_load, vm1_load, vm2_load, vmas_load):
            load.start()

    barrier = pltpu.get_barrier_semaphore()

    def signal(sem, where):
        pl.semaphore_signal(sem, inc=1, device_id=where, device_id_type=MESH)

    signal(barrier, partner)
    for d in fs_peers:
        signal(barrier, {"fs": d})

    @pl.when(chip > 0)
    def _():
        signal(barrier, left)

    @pl.when(chip < last)
    def _():
        signal(barrier, right)

    with scope("barrier"):
        pl.semaphore_wait(barrier, fs + at_first + at_last)

    def pass_right(where):
        @pl.when(where & (chip > 0))
        def _():
            pl.semaphore_wait(seen.at[0], 1)

        @pl.when(where & (chip < last))
        def _():
            signal(seen.at[0], right)

    def pass_left(where):
        @pl.when(where & (chip < last))
        def _():
            pl.semaphore_wait(seen.at[1], 1)

        @pl.when(where & (chip > 0))
        def _():
            signal(seen.at[1], left)

    near = chips // 2

    def remote(src, dst, send_sem, recv_sem, where):
        return pltpu.make_async_remote_copy(
            src_ref=src, dst_ref=dst, send_sem=send_sem, recv_sem=recv_sem,
            device_id=where, device_id_type=MESH,
        )

    def send(src, dst, send_sem, recv_sem, where):
        remote(src, dst, send_sem, recv_sem, where).start()

    def landed(dst, sem):
        remote(dst, dst, sem, sem, partner).wait_recv()

    def left_here(src, sem):
        remote(src, src, sem, sem, partner).wait_send()

    def factor_of(s):
        rows = ofac_v[pl.ds(pl.multiple_of(s * width, width), width), :]
        return rows.astype(F32).T.astype(BF16)

    def against(one, two):
        return lax.dot_general(one, two, (((1,), (1,)), ((), ())), preferred_element_type=F32)

    def to_right(k):
        return remote(pre_out.at[k], pre_in.at[k], pre_send, pre_recv.at[k], right)

    def to_left(k):
        return remote(suf_out.at[k], suf_in.at[k], suf_send, suf_recv.at[k], left)

    def send_moments():
        om12_load.wait()
        for i, local in enumerate((o1_v, o2_v)):
            top = top_of(local[...])
            mom_top[f, i] = top
            mom[f, i] = encode_even(local[...], top)
        for d in fs_peers:
            send(mom_top.at[f], mom_top.at[f], momt_send, momt_recv, {"fs": d})
            send(mom.at[f], mom.at[f], mom_send, mom_recv, {"fs": d})

    def masters_encode():
        omas_load.wait()
        top = top_of(om_v[...])
        mas_top[f] = top
        mas[f] = encode_even(om_v[...], top)

    def masters_end():
        landed(mas_top.at[pl.ds(0, fs - 1)], mast_recv)
        landed(mas.at[pl.ds(0, fs - 1)], mas_recv)
        for g in range(fs):
            om_all[pl.ds(g * o_rows, o_rows), :] = decode_even(mas[g], mas_top[g])

    late = at_first * at_last * SUF

    def step(i, _):
        k = i - PRE * chip

        @pl.when((chip > 0) & (k >= 0) & (k < blocks))
        def _():
            with scope("pre_wait"):
                landed(pre_in.at[k], pre_recv.at[k])
            left_v[k] = decode(pre_in[k], bound[...])

            @pl.when(chip < last)
            def _():
                pre_out[k] = encode(left_v[k] + own_v[k], bound[...])
                to_right(k).start()

        m = i - SUF * (last - chip)

        @pl.when((chip < last) & (m >= 0) & (m < blocks))
        def _():
            with scope("suf_wait"):
                landed(suf_in.at[m], suf_recv.at[m])
            right_v[m] = decode(suf_in[m], bound[...])

            @pl.when(chip > 0)
            def _():
                suf_out[m] = encode(right_v[m] + own_v[m], bound[...])
                to_left(m).start()

        n = i - late - jnp.maximum(PRE * chip, SUF * (last - chip))

        @pl.when((n >= 0) & (n < blocks) & (lax.rem(n + 2, 2) == 1))
        def _():
            with scope("acc"):
                image = jnp.concatenate([left_v[j] + own_v[j] + right_v[j] for j in (n - 1, n)], axis=1)
                two = split(image, 0)
                here = pl.ds(pl.multiple_of((n - 1) * block, block), 2 * block)
                acc_own[...] += jnp.dot(two, ocot_v[here, :], preferred_element_type=F32)
                acc_pair[...] += jnp.dot(two, ocot_in[here, :], preferred_element_type=F32)

        return 0

    steps = blocks + SUF * last

    @pl.when(hub)
    def _():
        for i, (src, dst) in enumerate(((vin, vin_v), (vm1, v1_v), (vm2, v2_v), (vmas, vm_v))):
            send(src, dst.at[1], gift_send.at[min(i, 1)], gift_recv[i], partner)
        send_moments()
        with scope("factor"):
            ofac_load.wait()
            reach = jnp.sum(jnp.abs(ofac_v[...].astype(F32)), axis=0, keepdims=True)
            top = jnp.max(reach, axis=1, keepdims=True) * (1.02 * HEADS_BOUND) + 1e-30
            bound[...] = jnp.broadcast_to(top, bound.shape)
            factor = jnp.concatenate([factor_of(t - 1), factor_of(t)], axis=1)
        for i, rows in enumerate(pieces):
            heads_load[i].wait()
            with scope("heads_in"):
                landed(heads_in.at[rows], heads_recv.at[i])
            with scope("own"):
                own = against(factor, jnp.concatenate([heads_in[rows, :], heads_v[rows, :]], axis=1))
                for k in range(sizes[i]):
                    own_v[starts[i] + k] = own[:, k * block:(k + 1) * block]

            @pl.when(chip == 0)
            def _():
                for k in range(starts[i], starts[i] + sizes[i]):
                    pre_out[k] = encode(own_v[k], bound[...])
                    to_right(k).start()

            @pl.when(chip == last)
            def _():
                for k in range(starts[i], starts[i] + sizes[i]):
                    suf_out[k] = encode(own_v[k], bound[...])
                    to_left(k).start()

        @pl.when(chip == 0)
        def _():
            left_v[...] = jnp.zeros_like(left_v)

        @pl.when(chip == last)
        def _():
            right_v[...] = jnp.zeros_like(right_v)

        acc_own[...] = jnp.zeros_like(acc_own)
        acc_pair[...] = jnp.zeros_like(acc_pair)
        with scope("masters_encode"):
            masters_encode()

        def hub_masters():
            for d in fs_peers:
                send(mas_top.at[f], mas_top.at[f], give_send.at[0], mast_recv, {"fs": d})
                send(mas.at[f], mas.at[f], give_send.at[1], mas_recv, {"fs": d})

        def output_cotangents():
            ocot_load.wait()
            landed(ocot_in, ocot_recv)

        done = 0
        for at, event in ((13, output_cotangents), (22, hub_masters)):
            at = min(at, steps)
            lax.fori_loop(done, at, step, 0)
            done = at
            with scope(f"event{at}"):
                event()
        lax.fori_loop(done, steps, step, 0)

        with scope("exchange"):
            mine = acc_own[:rank, :] + acc_own[rank:, :]
            pair = acc_pair[:rank, :] + acc_pair[rank:, :]
            for h, whole in enumerate((pair, mine)):
                part[h] = whole
                top = top_of(whole)
                part_top[h] = top
                coded_part = encode_even(whole, top)
                for g in range(fs):
                    part_out[g, h] = coded_part[g * band:(g + 1) * band]
            for d in fs_peers:
                send(part_top, part_top_in.at[f], mark_send, mark_recv, {"fs": d})
                send(part_out.at[d], part_in.at[f], part_send, part_recv, {"fs": d})
        with scope("part_wait"):
            landed(part_top_in.at[pl.ds(0, fs - 1)], mark_recv)
            landed(part_in.at[pl.ds(0, fs - 1)], part_recv)
        with scope("sum_out"):
            power = jnp.zeros((1, columns), F32)
            for h, out in ((0, stage), (1, own_rows(o_all))):
                whole = part[h, pl.ds(pl.multiple_of(f * band, band), band), :]
                for d in fs_peers:
                    whole = whole + decode_even(part_in[d, h], part_top_in[d, h])
                out[...] = whole
                power = power + jnp.sum(whole * whole, axis=0, keepdims=True)
            me = f * chips + chip
            sums[me] = power

            def spread(d, j, c):
                where = {"fs": d, "tp": 2 * lax.rem(chip + j, chips) + c}
                send(sums.at[me], sums.at[me], sum_send, sum_recv, where)

            if fs * chips <= 16:
                for j in range(chips - 1, -1, -1):
                    for d in (*fs_peers, f):
                        for c in range(2):
                            if d is not f or j > 0 or c == 0:
                                spread(d, j, c)
            else:
                def spread_one(k, _):
                    spread(lax.rem(f + k // (2 * chips), fs), (k // 2) % chips, k % 2)
                    return 0

                spread(f, 0, 0)
                lax.fori_loop(2, 2 * fs * chips, spread_one, 0)
            here = own_rows(o_all)
            for d in fs_peers:
                send(here, here, all_send.at[0], all_recv, {"fs": d})
                send(stage, here, all_send.at[1], all_recv, {"fs": d, "tp": t - 1})
            send(stage, here, all_send.at[1], all_recv, partner)

    @pl.when(aide)
    def _():
        pass_right(chip == 0)
        pass_left(chip == last)
        for i, rows in enumerate(pieces):
            heads_load[i].wait()
            send(heads_v.at[rows], heads_in.at[rows], heads_send, heads_recv.at[i], partner)
        send_moments()
        with scope("masters_encode"):
            masters_encode()
        for d in fs_peers:
            send(mas_top.at[f], mas_top.at[f], mast_send, mast_recv, {"fs": d})
            send(mas.at[f], mas.at[f], mas_send, mas_recv, {"fs": d})
        ocot_load.wait()
        send(ocot_v, ocot_in, ocot_send, ocot_recv, partner)
        pass_right((chip > 0) & (chip < near))
        pass_left((chip < last) & (chip >= near))
        with scope("value_load"):
            for load in (vfac_load, vcot_load, vin_load):
                load.wait()
        with scope("pass"):
            pass_right((chip >= near) & (chip < last))
            pass_left((chip > 0) & (chip < near))
        with scope("value_own"):
            total = jnp.zeros((2 * rank, columns), F32)
            stride = image_v.shape[2]
            value_factor = vfac_v[...].astype(F32).T.astype(BF16)
            for i in range(tokens // stride):
                rows = pl.ds(i * stride, stride)
                two = split(against(value_factor, vcot_v[rows, :]), 0)
                image_v[i] = two
                total = total + jnp.dot(two, vin_v[0, rows, :], preferred_element_type=F32)
            totals_v = [total]
        with scope("gift"):
            landed(vin_v.at[1], gift_recv[0])
        with scope("value_pair"):
            total = jnp.zeros((2 * rank, columns), F32)
            for i in range(tokens // stride):
                total = total + jnp.dot(image_v[i], vin_v[1, pl.ds(i * stride, stride), :], preferred_element_type=F32)
            totals_v.append(total)
            for h, total in enumerate(totals_v):
                mine = total[:rank] + total[rank:]
                proj_v[h] = mine
                top = top_of(mine)
                value_top[h] = top
                coded_part = encode_even(mine, top)
                for g in range(fs):
                    value_out[g, h] = coded_part[g * band:(g + 1) * band]
        with scope("seen"):
            @pl.when(chip == 0)
            def _():
                pl.semaphore_wait(seen.at[1], 1)

            @pl.when(chip == last)
            def _():
                pl.semaphore_wait(seen.at[0], 1)

        for d in fs_peers:
            send(value_top, value_top_in.at[f], value_mark_send, value_mark_recv, {"fs": d})
            send(value_out.at[d], value_in.at[f], value_swap_send, value_swap_recv, {"fs": d})
        with scope("value_masters"):
            vmas_load.wait()
            landed(vm_v.at[1], gift_recv[3])
            for h in range(2):
                top = top_of(vm_v[h])
                value_mast[f, h] = top
                value_mas[f, h] = encode_even(vm_v[h], top)
            for d in fs_peers:
                send(value_mast.at[f], value_mast.at[f], value_mast_send, value_mast_recv, {"fs": d})
                send(value_mas.at[f], value_mas.at[f], value_mas_send, value_mas_recv, {"fs": d})
        with scope("value_swap_wait"):
            landed(value_top_in.at[pl.ds(0, fs - 1)], value_mark_recv)
            landed(value_in.at[pl.ds(0, fs - 1)], value_swap_recv)
        power = jnp.zeros((1, columns), F32)
        own_band = pl.ds(pl.multiple_of(f * band, band), band)
        for h in range(2):
            whole = proj_v[h, own_band, :]
            for d in fs_peers:
                whole = whole + decode_even(value_in[d, h], value_top_in[d, h])
            proj_v[h, own_band, :] = whole
            power = power + jnp.sum(whole * whole, axis=0, keepdims=True)
        value_me = f * chips + chip
        value_sums[value_me] = power

        def value_spread(i, j):
            where = {"fs": lax.rem(f + i, fs), "tp": 2 * lax.rem(chip + j, chips)}
            send(value_sums.at[value_me], value_sums.at[value_me], value_sum_send, value_sum_recv, where)

        if fs * chips <= 16:
            for i in range(fs - 1, -1, -1):
                for j in range(chips):
                    if (i, j) != (0, 0):
                        value_spread(i, j)
        else:
            def value_spread_one(k, _):
                value_spread(k // chips, k % chips)
                return 0

            lax.fori_loop(1, fs * chips, value_spread_one, 0)
        vm12_load.wait()
        landed(v1_v.at[1], gift_recv[1])
        landed(v2_v.at[1], gift_recv[2])
        with scope("value_sums_wait"):
            landed(value_sums.at[pl.ds(0, fs * chips - 1)], value_sum_recv)
        total = jnp.sum(jnp.sum(value_sums[...], axis=0), axis=1, keepdims=True)
        scale = lax.rsqrt(total / (rank * columns * tp) + 1e-06)
        for h, first_out, second_out in ((0, v_first, v_second), (1, back_first, back_second)):
            scaled = scale * proj_v[h, own_band, :]
            first_new = 0.9 * v1_v[h] + 0.1 * scaled
            second_new = 0.95 * v2_v[h] + 0.05 * scaled * scaled
            first_out[...] = first_new
            second_out[...] = second_new
            direction = first_new / (jnp.sqrt(second_new) + 1e-08)
            top = top_of(direction)
            dir_top[f, h] = top
            dir_code[f, h] = encode_even(direction, top)
        for d in fs_peers:
            send(dir_top.at[f], dir_top.at[f], dirt_send, dirt_recv, {"fs": d})
            send(dir_code.at[f], dir_code.at[f], dir_send, dir_recv, {"fs": d})
        send(back_first, v_first, back_send[0], back_recv, partner)
        send(back_second, v_second, back_send[0], back_recv, partner)
        rows = vfac_v[...]
        rows = jnp.concatenate([rows, rows], axis=1)
        with scope("dir_wait"):
            landed(dir_top.at[pl.ds(0, fs - 1)], dirt_recv)
            landed(dir_code.at[pl.ds(0, fs - 1)], dir_recv)
            landed(value_mast.at[pl.ds(0, fs - 1)], value_mast_recv)
            landed(value_mas.at[pl.ds(0, fs - 1)], value_mas_recv)

        for h, step_out, new_out, copy_out in ((1, back_step, back_new, back_copy), (0, v_step, v_new, v_copy)):
            direction = jnp.concatenate([decode_even(dir_code[g, h], dir_top[g, h]) for g in range(fs)], axis=0)
            direction = split(direction, 0)
            move_v[...] = jnp.dot(rows, direction, preferred_element_type=F32)
            move = own_rows(move_v)[...]
            step_out[...] = move
            new_out[...] = vm_v[h] - 0.002 * move
            for g in range(fs):
                these = pl.ds(g * v_rows, v_rows)
                old = decode_even(value_mas[g, h], value_mast[g, h])
                copy_out[these, :] = (old - 0.002 * move_v[these, :]).astype(BF16)
            if h == 1:
                send(back_copy, v_copy, copy_send, copy_recv, partner)
                send(back_step, v_step, back_send[1], back_recv, partner)
                send(back_new, v_new, back_send[1], back_recv, partner)

    with scope("masters_wait"):
        masters_end()
    with scope("mom_wait"):
        landed(mom_top.at[pl.ds(0, fs - 1)], momt_recv)
        landed(mom.at[pl.ds(0, fs - 1)], mom_recv)
        for i, whole in ((0, o1_all), (1, o2_all)):
            for g in range(fs):
                whole[pl.ds(g * band, band), :] = decode_even(mom[g, i], mom_top[g, i])
        left_here(mom_top.at[pl.ds(0, fs - 1)], momt_send)
        left_here(mom.at[pl.ds(0, fs - 1)], mom_send)

    n_sums = fs * chips
    bands = o_all.at[pl.ds(0, (fs - 1) * band)]
    with scope("drain"):
        @pl.when(aide)
        def _():
            left_here(heads_in, heads_send)
            left_here(ocot_in, ocot_send)
            left_here(value_in.at[pl.ds(0, fs - 1)], value_swap_send)
            left_here(value_top_in.at[pl.ds(0, fs - 1)], value_mark_send)
            left_here(dir_top.at[pl.ds(0, fs - 1)], dirt_send)
            left_here(dir_code.at[pl.ds(0, fs - 1)], dir_send)
            left_here(value_sums.at[pl.ds(0, n_sums - 1)], value_sum_send)
            left_here(mas.at[pl.ds(0, fs - 1)], mas_send)
            left_here(mas_top.at[pl.ds(0, fs - 1)], mast_send)
            left_here(v1_v, back_send[0])
            left_here(vm_v, back_send[1])
            left_here(v_copy, copy_send)
            left_here(value_mast.at[pl.ds(0, fs - 1)], value_mast_send)
            left_here(value_mas.at[pl.ds(0, fs - 1)], value_mas_send)
            landed(o_all, all_recv)
            landed(sums.at[pl.ds(0, n_sums)], sum_recv)

        @pl.when(hub & (chip < last))
        def _():
            left_here(pre_out, pre_send)

        @pl.when(hub & (chip > 0))
        def _():
            left_here(suf_out, suf_send)

        @pl.when(hub)
        def _():
            left_here(vin_v.at[1], gift_send.at[0])
            left_here(om_v.at[pl.ds(0, 2 * band + v_rows)], gift_send.at[1])
            left_here(mas_top.at[pl.ds(0, fs - 1)], give_send.at[0])
            left_here(mas.at[pl.ds(0, fs - 1)], give_send.at[1])
            left_here(part_top_in.at[pl.ds(0, fs - 1)], mark_send)
            left_here(part_in.at[pl.ds(0, fs - 1)], part_send)
            landed(om_all.at[pl.ds(0, 2 * (band + v_rows))], back_recv)
            with scope("copy_wait"):
                landed(v_copy, copy_recv)
            with scope("all_wait"):
                landed(bands, all_recv)
                left_here(bands, all_send.at[0])
                left_here(o_all, all_send.at[1])
            with scope("sums_wait"):
                left_here(sums.at[pl.ds(0, 2 * n_sums - 1)], sum_send)
                landed(sums.at[pl.ds(0, n_sums - 1)], sum_recv)

    totals[...] = jnp.sum(sums[pl.ds(0, n_sums)], axis=0)


def finish_kernel(
    fs, tp,
    o_all, o1_all, o2_all, om_all, totals, ofac, omas, om1, om2, v_step, v_new, v_copy, v_first, v_second,
    v_step_out, v_new_out, v_copy_out, v_first_out, v_second_out,
    o_step_out, o_new_out, o_copy_out, o_first_out, o_second_out,
    move_v, new_v, copy_v, first_v, second_v, out_sem,
):
    f = lax.axis_index("fs")
    puts = []

    def put(src, dst):
        copy = pltpu.make_async_copy(src, dst, out_sem.at[len(puts)])
        copy.start()
        puts.append(copy)

    for src, dst in (
        (v_step, v_step_out), (v_new, v_new_out), (v_copy, v_copy_out), (v_first, v_first_out), (v_second, v_second_out),
    ):
        put(src, dst)
    rank, columns = o1_all.shape
    band = rank // fs
    total = jnp.sum(totals[...], axis=1, keepdims=True)
    scale = lax.rsqrt(total / (rank * columns * tp) + 1e-06)

    def moments(proj, first, second):
        scaled = scale * proj
        first_new = 0.9 * first + 0.1 * scaled
        second_new = 0.95 * second + 0.05 * scaled * scaled
        return first_new, second_new

    own_band = pl.ds(pl.multiple_of(f * band, band), band)
    with jax.named_scope("f_own"):
     first_v[...], second_v[...] = moments(o_all[own_band, :], om1[...], om2[...])
    put(first_v, o_first_out)
    put(second_v, o_second_out)
    first_new, second_new = moments(o_all[...], o1_all[...], o2_all[...])
    direction = split(first_new / (jnp.sqrt(second_new) + 1e-08), 0)

    def step_of(rows):
        left = ofac[rows, :]
        return jnp.dot(jnp.concatenate([left, left], axis=1), direction, preferred_element_type=F32)

    count = new_v.shape[0]
    for i in range(fs):
        rows = pl.ds(i * count, count)
        move_v[rows, :] = step_of(rows)
        copy_v[rows, :] = (om_all[rows, :] - 0.002 * move_v[rows, :]).astype(BF16)
        put(copy_v.at[rows], o_copy_out.at[rows])
    own = pl.ds(pl.multiple_of(f * count, count), count)
    put(move_v.at[own], o_step_out)
    new_v[...] = omas[...] - 0.002 * move_v[own, :]
    put(new_v, o_new_out)
    with jax.named_scope("f_wait"):
        for copy in puts:
            copy.wait()


def on_device(vin, vcot, vfac, vmas, vm1, vm2, heads, ocot, ofac, omas, om1, om2):
    fs = lax.axis_size("fs")
    tp = lax.axis_size("tp")
    rank = vfac.shape[1]
    band = rank // fs
    columns = vin.shape[1]
    tokens, width = heads.shape
    block = 128
    blocks = tokens // block
    stride = 256 if tokens % 256 == 0 else tokens

    def twice(array):
        return pltpu.VMEM((2, *array.shape), array.dtype)

    def like(array):
        return pltpu.VMEM(array.shape, array.dtype)

    def shape(*dims, kind=F32):
        return jax.ShapeDtypeStruct(dims, kind)

    def wide(*dims):
        return pltpu.VMEM(dims, F32)

    def coded():
        return pltpu.VMEM((blocks, rank, block), BF16)

    dma = pltpu.SemaphoreType.DMA
    v_rows, o_rows = vmas.shape[0], omas.shape[0]
    gathered = pl.pallas_call(
        functools.partial(gather_kernel, fs, tp),
        out_shape=(
            shape(rank, columns), shape(rank, columns), shape(rank, columns), shape(fs * o_rows, columns),
            shape(1, columns),
            shape(v_rows, columns), shape(v_rows, columns), shape(fs * v_rows, columns, kind=BF16),
            shape(band, columns), shape(band, columns),
        ),
        in_specs=[HBM] * 12,
        out_specs=(VMEM,) * 10,
        scratch_shapes=[
            like(vfac), like(ofac), twice(vin), like(vcot), pltpu.VMEM((tokens // stride, 2 * rank, stride), BF16),
            like(heads), like(heads), like(ocot), like(ocot), twice(vm1), twice(vm2), twice(vmas), like(omas), like(om1), like(om2),
            wide(blocks, rank, block), wide(blocks, rank, block), wide(blocks, rank, block),
            coded(), coded(), coded(), coded(), wide(1, block),
            wide(2 * rank, columns), wide(2 * rank, columns),
            wide(2, rank, columns), pltpu.VMEM((fs, 2, band, columns), BF16), wide(2, 1, columns),
            pltpu.VMEM((fs, 2, band, columns), BF16), wide(fs, 2, 1, columns), wide(band, columns),
            pltpu.VMEM((fs, 2, band, columns), BF16), wide(2, 1, columns),
            pltpu.VMEM((fs, 2, band, columns), BF16), wide(fs, 2, 1, columns), wide(2, rank, columns),
            pltpu.VMEM((fs, 2, band, columns), BF16), wide(fs, 2, 1, columns),
            pltpu.VMEM((fs, 2, band, columns), BF16), wide(fs, 2, 1, columns),
            wide(fs * tp, 1, columns), wide(fs * tp // 2, 1, columns),
            pltpu.VMEM((fs, o_rows, columns), BF16), wide(fs, 1, columns),
            wide(band, columns), wide(band, columns), wide(v_rows, columns), wide(v_rows, columns),
            pltpu.VMEM((fs * v_rows, columns), BF16),
            pltpu.VMEM((fs, 2, v_rows, columns), BF16), wide(fs, 2, 1, columns), wide(fs * v_rows, columns),
            dma((4 + len(growing(blocks)),)), dma((len(growing(blocks)),)), dma, dma((2,)),
            dma, dma((blocks,)), dma, dma((blocks,)),
            dma, dma, dma, dma, dma((2,)), dma, dma, dma, pltpu.SemaphoreType.REGULAR((2,)),
            dma, dma, dma, dma, dma, dma, dma((2,)), dma, dma,
        ],
        compiler_params=pltpu.CompilerParams(
            collective_id=0, has_side_effects=True, vmem_limit_bytes=32 * 1024 * 1024
        ),
    )(*(pltpu.with_memory_space_constraint(a, pltpu.HBM) for a in (
        vin, vcot, vfac, vmas, vm1, vm2, heads, ocot, ofac, omas, om1, om2
    )))
    o_all, o1_all, o2_all, om_all, totals, *values = gathered

    return pl.pallas_call(
        functools.partial(finish_kernel, fs, tp),
        out_shape=(
            shape(v_rows, columns), shape(v_rows, columns), shape(fs * v_rows, columns, kind=BF16),
            shape(band, columns), shape(band, columns),
            shape(o_rows, columns), shape(o_rows, columns), shape(fs * o_rows, columns, kind=BF16),
            shape(band, columns), shape(band, columns),
        ),
        in_specs=[VMEM] * 14,
        out_specs=(HBM,) * 10,
        scratch_shapes=[
            wide(fs * o_rows, columns), wide(o_rows, columns), pltpu.VMEM((fs * o_rows, columns), BF16),
            wide(band, columns), wide(band, columns), dma((9 + fs,)),
        ],
        compiler_params=pltpu.CompilerParams(vmem_limit_bytes=24 * 1024 * 1024),
    )(o_all, o1_all, o2_all, om_all, totals, ofac, omas, om1, om2, *values)


def solution(mesh):
    both = P("fs", "tp")
    in_specs = (both, P("fs", None), P(), both, both, both, both, both, P(), both, both, both)
    out_specs = (
        both, both, P(None, "tp"), both, both, both, both, P(None, "tp"), both, both,
    )
    return jax.shard_map(
        on_device, mesh=mesh, in_specs=in_specs, out_specs=out_specs, check_vma=False
    )
```

```python
import functools

import jax
import jax.numpy as jnp
from jax import lax
from jax.experimental import pallas as pl
from jax.experimental.pallas import tpu as pltpu
from jax.sharding import PartitionSpec as P

MESH = pl.DeviceIdType.MESH
ANY = pl.BlockSpec(memory_space=pl.ANY)
HBM = pl.BlockSpec(memory_space=pltpu.HBM)
VMEM = pl.BlockSpec(memory_space=pltpu.VMEM)
BF16 = jnp.bfloat16
F32 = jnp.float32
PRE = 6
SUF = 7
LEVELS = 250.0
POWER = 7
PEAK = 240000.0
HEADS_BOUND = 6.0


def split(wide, axis):
    high = wide.astype(BF16)
    low = (wide - high.astype(F32)).astype(BF16)
    return jnp.concatenate([high, low], axis=axis)


def encode(x, top):
    u = x * (PEAK / top)
    u2 = u * u
    return (u2 * u2 * u2 * u).astype(BF16)


def decode(coded, top):
    y = coded.astype(F32)
    size = jnp.abs(y)
    root = jnp.exp(jnp.log(jnp.maximum(size, 1e-37)) * (1.0 / POWER))
    root = jnp.where(size < 2e-37, 0.0, root) * (top * (1.0 / PEAK))
    return jnp.where(y < 0.0, -root, root)


def encode_even(x, top):
    size = jnp.exp2(jnp.abs(x) * (LEVELS / top) - LEVELS / 2)
    return jnp.where(x < 0.0, -size, size).astype(BF16)


def decode_even(coded, top):
    y = coded.astype(F32)
    level = jnp.maximum(jnp.log2(jnp.maximum(jnp.abs(y), 1e-38)) + LEVELS / 2, 0.0)
    size = level * (top * (1.0 / LEVELS))
    return jnp.where(y < 0.0, -size, size)


def top_of(x):
    return jnp.max(jnp.abs(x), axis=0, keepdims=True) * 1.02 + 1e-30


def growing(blocks):
    sizes = [1]
    while sum(sizes) < blocks:
        sizes.append(min(sum(sizes), blocks - sum(sizes)))
    return sizes


def gather_kernel(
    fs, tp,
    vin, vcot, vfac, vmas, vm1, vm2, heads, ocot, ofac, omas, om1, om2,
    o_all, o1_all, o2_all, om_all, totals, v_step, v_new, v_copy, v_first, v_second,
    vfac_v, ofac_v, vin_v, vcot_v, image_v, heads_v, heads_in, ocot_v, ocot_in, v1_v, v2_v, vm_v, om_v, o1_v, o2_v,
    own_v, left_v, right_v, pre_in, pre_out, suf_in, suf_out, bound, acc_own, acc_pair,
    part, part_out, part_top, part_in, part_top_in, stage, value_out, value_top, value_in, value_top_in, proj_v, mom, mom_top, dir_code, dir_top, sums, value_sums, mas, mas_top,
    pair_mas, pair_mast, back_first, back_second, back_step, back_new, back_copy, value_mas, value_mast, move_v,
    load_sem, heads_recv, ocot_recv, gift_send, pre_send, pre_recv, suf_send, suf_recv,
    part_send, part_recv, mark_send, mark_recv, all_send, all_recv, sum_send, sum_recv, seen,
    mom_send, mom_recv, momt_send, momt_recv, mas_recv, mast_recv, give_send, back_recv, copy_recv,
):
    f = lax.axis_index("fs")
    t = lax.axis_index("tp")
    chip = t // 2
    core = t % 2
    chips = tp // 2
    last = chips - 1
    rank = vfac.shape[1]
    band = rank // fs
    tokens, width = heads.shape
    columns = vin.shape[1]
    blocks, _, block = own_v.shape
    o_rows = omas.shape[0]
    v_rows = vmas.shape[0]
    scope = jax.named_scope
    hub = core == 1
    aide = core == 0
    at_last = (last - chip + last) // chips
    at_first = (chip + last) // chips

    spare = iter([sems.at[i] for sems in (pre_recv, suf_recv) for i in range(blocks)])
    heads_send, ocot_send = next(spare), next(spare)
    gift_recv = [next(spare) for _ in range(4)]
    value_swap_send, value_swap_recv, value_mark_send, value_mark_recv = (next(spare) for _ in range(4))
    value_sum_send, value_sum_recv = next(spare), next(spare)
    dir_send, dir_recv, dirt_send, dirt_recv = (next(spare) for _ in range(4))
    mas_send, mast_send, give_recv = ([next(spare) for _ in range(2)] for _ in range(3))
    back_send = [next(spare) for _ in range(2)]
    copy_send = next(spare)
    value_mas_send, value_mas_recv, value_mast_send, value_mast_recv = (next(spare) for _ in range(4))

    fs_peers = [3 - f, f + 1 - 2 * (f % 2), lax.rem(f + 2, fs)] if fs == 4 else [lax.rem(f + j, fs) for j in range(1, fs)]
    partner = {"tp": chip * 2 + (1 - core)}
    right = {"tp": lax.rem(t + 2, tp)}
    left = {"tp": lax.rem(t + tp - 2, tp)}

    def own_rows(ref):
        rows = ref.shape[0] // fs
        return ref.at[pl.ds(pl.multiple_of(f * rows, rows), rows)]

    sizes = growing(blocks)
    count = len(sizes)
    starts = [sum(sizes[:i]) for i in range(count)]
    pieces = [pl.ds(a * block, n * block) for a, n in zip(starts, sizes)]

    def loading(i, src, dst):
        return pltpu.make_async_copy(src, dst, load_sem.at[i])

    heads_load = [loading(i, heads.at[rows], heads_v.at[rows]) for i, rows in enumerate(pieces)]
    om1_load = loading(count, om1, o1_v)
    om2_load = loading(count, om2, o2_v)
    om12_load = loading(count, om_v.at[pl.ds(0, 2 * band)], om_v.at[pl.ds(0, 2 * band)])
    omas_load = loading(count + 2, omas, om_v)
    ocot_load = loading(count + 3, ocot, ocot_v)
    ofac_load = loading(count + 4, ofac, ofac_v)
    vfac_load = loading(count + 4, vfac, vfac_v)
    vcot_load = loading(count + 5, vcot, vcot_v)
    vin_load = loading(count + 6, vin, vin_v.at[0])
    vm1_load = loading(count + 1, vm1, v1_v.at[0])
    vm2_load = loading(count + 1, vm2, v2_v.at[0])
    vm12_load = loading(count + 1, v1_v, v1_v)
    vmas_load = loading(count + 7, vmas, vm_v.at[0])

    heads_load[0].start()

    @pl.when(hub)
    def _():
        ofac_load.start()

    for load in (*heads_load[1:], om1_load, om2_load):
        load.start()

    @pl.when(hub)
    def _():
        for load in (omas_load, ocot_load):
            load.start()

    @pl.when(aide)
    def _():
        for load in (omas_load, ocot_load, vfac_load, vcot_load, vin_load, vm1_load, vm2_load, vmas_load):
            load.start()

    barrier = pltpu.get_barrier_semaphore()

    def signal(sem, where):
        pl.semaphore_signal(sem, inc=1, device_id=where, device_id_type=MESH)

    signal(barrier, partner)
    for d in fs_peers:
        signal(barrier, {"fs": d})

    @pl.when(chip > 0)
    def _():
        signal(barrier, left)

    @pl.when(chip < last)
    def _():
        signal(barrier, right)

    with scope("barrier"):
        pl.semaphore_wait(barrier, fs + at_first + at_last)

    def pass_right(where):
        @pl.when(where & (chip > 0))
        def _():
            pl.semaphore_wait(seen.at[0], 1)

        @pl.when(where & (chip < last))
        def _():
            signal(seen.at[0], right)

    def pass_left(where):
        @pl.when(where & (chip < last))
        def _():
            pl.semaphore_wait(seen.at[1], 1)

        @pl.when(where & (chip > 0))
        def _():
            signal(seen.at[1], left)

    near = chips // 2

    def remote(src, dst, send_sem, recv_sem, where):
        return pltpu.make_async_remote_copy(
            src_ref=src, dst_ref=dst, send_sem=send_sem, recv_sem=recv_sem,
            device_id=where, device_id_type=MESH,
        )

    def send(src, dst, send_sem, recv_sem, where):
        remote(src, dst, send_sem, recv_sem, where).start()

    def landed(dst, sem):
        remote(dst, dst, sem, sem, partner).wait_recv()

    def left_here(src, sem):
        remote(src, src, sem, sem, partner).wait_send()

    def factor_of(s):
        rows = ofac_v[pl.ds(pl.multiple_of(s * width, width), width), :]
        return rows.astype(F32).T.astype(BF16)

    def against(one, two):
        return lax.dot_general(one, two, (((1,), (1,)), ((), ())), preferred_element_type=F32)

    def to_right(k):
        return remote(pre_out.at[k], pre_in.at[k], pre_send, pre_recv.at[k], right)

    def to_left(k):
        return remote(suf_out.at[k], suf_in.at[k], suf_send, suf_recv.at[k], left)

    def send_moments():
        om12_load.wait()
        for i, local in enumerate((o1_v, o2_v)):
            top = top_of(local[...])
            mom_top[f, i] = top
            mom[f, i] = encode_even(local[...], top)
        for d in fs_peers:
            send(mom_top.at[f], mom_top.at[f], momt_send, momt_recv, {"fs": d})
            send(mom.at[f], mom.at[f], mom_send, mom_recv, {"fs": d})

    def masters_encode():
        omas_load.wait()
        top = top_of(om_v[...])
        mas_top[f] = top
        mas[f] = encode_even(om_v[...], top)

    def masters_end():
        landed(mas_top.at[pl.ds(0, fs - 1)], mast_recv)
        landed(mas.at[pl.ds(0, fs - 1)], mas_recv)
        for g in range(fs):
            om_all[pl.ds(g * o_rows, o_rows), :] = decode_even(mas[g], mas_top[g])

    late = at_first * at_last * SUF

    def step(i, _):
        k = i - PRE * chip

        @pl.when((chip > 0) & (k >= 0) & (k < blocks))
        def _():
            with scope("pre_wait"):
                landed(pre_in.at[k], pre_recv.at[k])
            left_v[k] = decode(pre_in[k], bound[...])

            @pl.when(chip < last)
            def _():
                pre_out[k] = encode(left_v[k] + own_v[k], bound[...])
                to_right(k).start()

        m = i - SUF * (last - chip)

        @pl.when((chip < last) & (m >= 0) & (m < blocks))
        def _():
            with scope("suf_wait"):
                landed(suf_in.at[m], suf_recv.at[m])
            right_v[m] = decode(suf_in[m], bound[...])

            @pl.when(chip > 0)
            def _():
                suf_out[m] = encode(right_v[m] + own_v[m], bound[...])
                to_left(m).start()

        n = i - late - jnp.maximum(PRE * chip, SUF * (last - chip))

        @pl.when((n >= 0) & (n < blocks) & (lax.rem(n + 2, 2) == 1))
        def _():
            with scope("acc"):
                image = jnp.concatenate([left_v[j] + own_v[j] + right_v[j] for j in (n - 1, n)], axis=1)
                two = split(image, 0)
                here = pl.ds(pl.multiple_of((n - 1) * block, block), 2 * block)
                acc_own[...] += jnp.dot(two, ocot_v[here, :], preferred_element_type=F32)
                acc_pair[...] += jnp.dot(two, ocot_in[here, :], preferred_element_type=F32)

        return 0

    steps = blocks + SUF * last

    @pl.when(hub)
    def _():
        for i, (src, dst) in enumerate(((vin, vin_v), (vm1, v1_v), (vm2, v2_v), (vmas, vm_v))):
            send(src, dst.at[1], gift_send.at[i], gift_recv[i], partner)
        send_moments()
        with scope("factor"):
            ofac_load.wait()
            reach = jnp.sum(jnp.abs(ofac_v[...].astype(F32)), axis=0, keepdims=True)
            top = jnp.max(reach, axis=1, keepdims=True) * (1.02 * HEADS_BOUND) + 1e-30
            bound[...] = jnp.broadcast_to(top, bound.shape)
            factor = jnp.concatenate([factor_of(t - 1), factor_of(t)], axis=1)
        for i, rows in enumerate(pieces):
            heads_load[i].wait()
            with scope("heads_in"):
                landed(heads_in.at[rows], heads_recv.at[i])
            with scope("own"):
                own = against(factor, jnp.concatenate([heads_in[rows, :], heads_v[rows, :]], axis=1))
                for k in range(sizes[i]):
                    own_v[starts[i] + k] = own[:, k * block:(k + 1) * block]

            @pl.when(chip == 0)
            def _():
                for k in range(starts[i], starts[i] + sizes[i]):
                    pre_out[k] = encode(own_v[k], bound[...])
                    to_right(k).start()

            @pl.when(chip == last)
            def _():
                for k in range(starts[i], starts[i] + sizes[i]):
                    suf_out[k] = encode(own_v[k], bound[...])
                    to_left(k).start()

        @pl.when(chip == 0)
        def _():
            left_v[...] = jnp.zeros_like(left_v)

        @pl.when(chip == last)
        def _():
            right_v[...] = jnp.zeros_like(right_v)

        acc_own[...] = jnp.zeros_like(acc_own)
        acc_pair[...] = jnp.zeros_like(acc_pair)
        with scope("masters_encode"):
            masters_encode()
        send(mas_top.at[f], pair_mast, give_send.at[0], give_recv[0], partner)
        send(mas.at[f], pair_mas, give_send.at[1], give_recv[1], partner)

        def output_cotangents():
            ocot_load.wait()
            landed(ocot_in, ocot_recv)

        done = 0
        for at, event in ((13, output_cotangents),):
            at = min(at, steps)
            lax.fori_loop(done, at, step, 0)
            done = at
            with scope(f"event{at}"):
                event()
        lax.fori_loop(done, steps, step, 0)

        with scope("exchange"):
            mine = acc_own[:rank, :] + acc_own[rank:, :]
            pair = acc_pair[:rank, :] + acc_pair[rank:, :]
            for h, whole in enumerate((pair, mine)):
                part[h] = whole
                top = top_of(whole)
                part_top[h] = top
                coded_part = encode_even(whole, top)
                for g in range(fs):
                    part_out[g, h] = coded_part[g * band:(g + 1) * band]
            for d in fs_peers:
                send(part_top, part_top_in.at[f], mark_send, mark_recv, {"fs": d})
                send(part_out.at[d], part_in.at[f], part_send, part_recv, {"fs": d})
        with scope("part_wait"):
            landed(part_top_in.at[pl.ds(0, fs - 1)], mark_recv)
            landed(part_in.at[pl.ds(0, fs - 1)], part_recv)
        with scope("sum_out"):
            power = jnp.zeros((1, columns), F32)
            for h, out in ((0, stage), (1, own_rows(o_all))):
                whole = part[h, pl.ds(pl.multiple_of(f * band, band), band), :]
                for d in fs_peers:
                    whole = whole + decode_even(part_in[d, h], part_top_in[d, h])
                out[...] = whole
                power = power + jnp.sum(whole * whole, axis=0, keepdims=True)
            me = f * chips + chip
            sums[me] = power

            def spread(i, j, c):
                where = {"fs": lax.rem(f + i, fs), "tp": 2 * lax.rem(chip + j, chips) + c}
                send(sums.at[me], sums.at[me], sum_send, sum_recv, where)

            if fs * chips <= 16:
                for i in range(fs - 1, -1, -1):
                    for j in range(chips):
                        for c in range(2):
                            if (i, j, c) != (0, 0, 1):
                                spread(i, j, c)
            else:
                def spread_one(k, _):
                    spread(k // (2 * chips), (k // 2) % chips, k % 2)
                    return 0

                spread(0, 0, 0)
                lax.fori_loop(2, 2 * fs * chips, spread_one, 0)
            here = own_rows(o_all)
            for d in fs_peers:
                send(here, here, all_send.at[0], all_recv, {"fs": d})
                send(stage, here, all_send.at[1], all_recv, {"fs": d, "tp": t - 1})
            send(stage, here, all_send.at[1], all_recv, partner)

    @pl.when(aide)
    def _():
        pass_right(chip == 0)
        pass_left(chip == last)
        for i, rows in enumerate(pieces):
            heads_load[i].wait()
            send(heads_v.at[rows], heads_in.at[rows], heads_send, heads_recv.at[i], partner)
        send_moments()
        with scope("masters_encode"):
            masters_encode()
        for d in fs_peers:
            send(mas_top.at[f], mas_top.at[f], mast_send[0], mast_recv, {"fs": d})
            send(mas.at[f], mas.at[f], mas_send[0], mas_recv, {"fs": d})
        ocot_load.wait()
        send(ocot_v, ocot_in, ocot_send, ocot_recv, partner)
        pass_right((chip > 0) & (chip < near))
        pass_left((chip < last) & (chip >= near))
        with scope("value_load"):
            for load in (vfac_load, vcot_load, vin_load):
                load.wait()
        with scope("pass"):
            pass_right((chip >= near) & (chip < last))
            pass_left((chip > 0) & (chip < near))
        with scope("value_own"):
            total = jnp.zeros((2 * rank, columns), F32)
            stride = image_v.shape[2]
            value_factor = vfac_v[...].astype(F32).T.astype(BF16)
            for i in range(tokens // stride):
                rows = pl.ds(i * stride, stride)
                two = split(against(value_factor, vcot_v[rows, :]), 0)
                image_v[i] = two
                total = total + jnp.dot(two, vin_v[0, rows, :], preferred_element_type=F32)
            totals_v = [total]
        with scope("gift"):
            landed(vin_v.at[1], gift_recv[0])
        with scope("value_pair"):
            total = jnp.zeros((2 * rank, columns), F32)
            for i in range(tokens // stride):
                total = total + jnp.dot(image_v[i], vin_v[1, pl.ds(i * stride, stride), :], preferred_element_type=F32)
            totals_v.append(total)
            for h, total in enumerate(totals_v):
                mine = total[:rank] + total[rank:]
                proj_v[h] = mine
                top = top_of(mine)
                value_top[h] = top
                coded_part = encode_even(mine, top)
                for g in range(fs):
                    value_out[g, h] = coded_part[g * band:(g + 1) * band]
        with scope("seen"):
            @pl.when(chip == 0)
            def _():
                pl.semaphore_wait(seen.at[1], 1)

            @pl.when(chip == last)
            def _():
                pl.semaphore_wait(seen.at[0], 1)

        for d in fs_peers:
            send(value_top, value_top_in.at[f], value_mark_send, value_mark_recv, {"fs": d})
            send(value_out.at[d], value_in.at[f], value_swap_send, value_swap_recv, {"fs": d})
        with scope("give"):
            landed(pair_mast, give_recv[0])
            landed(pair_mas, give_recv[1])
        for d in fs_peers:
            there = {"fs": d, "tp": t + 1}
            send(pair_mast, mas_top.at[f], mast_send[1], mast_recv, there)
            send(pair_mas, mas.at[f], mas_send[1], mas_recv, there)
        with scope("value_masters"):
            vmas_load.wait()
            landed(vm_v.at[1], gift_recv[3])
            for h in range(2):
                top = top_of(vm_v[h])
                value_mast[f, h] = top
                value_mas[f, h] = encode_even(vm_v[h], top)
        with scope("value_swap_wait"):
            landed(value_top_in.at[pl.ds(0, fs - 1)], value_mark_recv)
            landed(value_in.at[pl.ds(0, fs - 1)], value_swap_recv)
        power = jnp.zeros((1, columns), F32)
        own_band = pl.ds(pl.multiple_of(f * band, band), band)
        for h in range(2):
            whole = proj_v[h, own_band, :]
            for d in fs_peers:
                whole = whole + decode_even(value_in[d, h], value_top_in[d, h])
            proj_v[h, own_band, :] = whole
            power = power + jnp.sum(whole * whole, axis=0, keepdims=True)
        value_me = f * chips + chip
        value_sums[value_me] = power

        def value_spread(i, j):
            where = {"fs": lax.rem(f + i, fs), "tp": 2 * lax.rem(chip + j, chips)}
            send(value_sums.at[value_me], value_sums.at[value_me], value_sum_send, value_sum_recv, where)

        if fs * chips <= 16:
            for i in range(fs - 1, -1, -1):
                for j in range(chips):
                    if (i, j) != (0, 0):
                        value_spread(i, j)
        else:
            def value_spread_one(k, _):
                value_spread(k // chips, k % chips)
                return 0

            lax.fori_loop(1, fs * chips, value_spread_one, 0)
        for d in fs_peers:
            send(value_mast.at[f], value_mast.at[f], value_mast_send, value_mast_recv, {"fs": d})
            send(value_mas.at[f], value_mas.at[f], value_mas_send, value_mas_recv, {"fs": d})
        vm12_load.wait()
        landed(v1_v.at[1], gift_recv[1])
        landed(v2_v.at[1], gift_recv[2])
        with scope("value_sums_wait"):
            landed(value_sums.at[pl.ds(0, fs * chips - 1)], value_sum_recv)
        total = jnp.sum(jnp.sum(value_sums[...], axis=0), axis=1, keepdims=True)
        scale = lax.rsqrt(total / (rank * columns * tp) + 1e-06)
        for h, first_out, second_out in ((0, v_first, v_second), (1, back_first, back_second)):
            scaled = scale * proj_v[h, own_band, :]
            first_new = 0.9 * v1_v[h] + 0.1 * scaled
            second_new = 0.95 * v2_v[h] + 0.05 * scaled * scaled
            first_out[...] = first_new
            second_out[...] = second_new
            direction = first_new / (jnp.sqrt(second_new) + 1e-08)
            top = top_of(direction)
            dir_top[f, h] = top
            dir_code[f, h] = encode_even(direction, top)
        for d in fs_peers:
            send(dir_top.at[f], dir_top.at[f], dirt_send, dirt_recv, {"fs": d})
            send(dir_code.at[f], dir_code.at[f], dir_send, dir_recv, {"fs": d})
        send(back_first, v_first, back_send[0], back_recv.at[0], partner)
        send(back_second, v_second, back_send[0], back_recv.at[0], partner)
        rows = vfac_v[...]
        rows = jnp.concatenate([rows, rows], axis=1)
        with scope("dir_wait"):
            landed(dir_top.at[pl.ds(0, fs - 1)], dirt_recv)
            landed(dir_code.at[pl.ds(0, fs - 1)], dir_recv)
            landed(value_mast.at[pl.ds(0, fs - 1)], value_mast_recv)
            landed(value_mas.at[pl.ds(0, fs - 1)], value_mas_recv)

        for h, step_out, new_out, copy_out in ((1, back_step, back_new, back_copy), (0, v_step, v_new, v_copy)):
            direction = jnp.concatenate([decode_even(dir_code[g, h], dir_top[g, h]) for g in range(fs)], axis=0)
            direction = split(direction, 0)
            move_v[...] = jnp.dot(rows, direction, preferred_element_type=F32)
            move = own_rows(move_v)[...]
            step_out[...] = move
            new_out[...] = vm_v[h] - 0.002 * move
            for g in range(fs):
                these = pl.ds(g * v_rows, v_rows)
                old = decode_even(value_mas[g, h], value_mast[g, h])
                copy_out[these, :] = (old - 0.002 * move_v[these, :]).astype(BF16)
            if h == 1:
                send(back_copy, v_copy, copy_send, copy_recv, partner)
                send(back_step, v_step, back_send[1], back_recv.at[1], partner)
                send(back_new, v_new, back_send[1], back_recv.at[1], partner)

    with scope("masters_wait"):
        masters_end()
    with scope("mom_wait"):
        landed(mom_top.at[pl.ds(0, fs - 1)], momt_recv)
        landed(mom.at[pl.ds(0, fs - 1)], mom_recv)
        for i, whole in ((0, o1_all), (1, o2_all)):
            for g in range(fs):
                whole[pl.ds(g * band, band), :] = decode_even(mom[g, i], mom_top[g, i])
        left_here(mom_top.at[pl.ds(0, fs - 1)], momt_send)
        left_here(mom.at[pl.ds(0, fs - 1)], mom_send)

    n_sums = fs * chips
    bands = o_all.at[pl.ds(0, (fs - 1) * band)]
    with scope("drain"):
        @pl.when(aide)
        def _():
            left_here(heads_in, heads_send)
            left_here(ocot_in, ocot_send)
            left_here(value_in.at[pl.ds(0, fs - 1)], value_swap_send)
            left_here(value_top_in.at[pl.ds(0, fs - 1)], value_mark_send)
            left_here(dir_top.at[pl.ds(0, fs - 1)], dirt_send)
            left_here(dir_code.at[pl.ds(0, fs - 1)], dir_send)
            left_here(value_sums.at[pl.ds(0, n_sums - 1)], value_sum_send)
            for i in range(2):
                left_here(mas.at[pl.ds(0, fs - 1)], mas_send[i])
                left_here(mas_top.at[pl.ds(0, fs - 1)], mast_send[i])
            left_here(v1_v, back_send[0])
            left_here(vm_v, back_send[1])
            left_here(v_copy, copy_send)
            left_here(value_mast.at[pl.ds(0, fs - 1)], value_mast_send)
            left_here(value_mas.at[pl.ds(0, fs - 1)], value_mas_send)
            landed(o_all, all_recv)
            landed(sums.at[pl.ds(0, n_sums)], sum_recv)

        @pl.when(hub & (chip < last))
        def _():
            left_here(pre_out, pre_send)

        @pl.when(hub & (chip > 0))
        def _():
            left_here(suf_out, suf_send)

        @pl.when(hub)
        def _():
            for i, ref in enumerate((vin_v, v1_v, v2_v, vm_v)):
                left_here(ref.at[1], gift_send.at[i])
            left_here(pair_mast, give_send.at[0])
            left_here(pair_mas, give_send.at[1])
            left_here(part_top_in.at[pl.ds(0, fs - 1)], mark_send)
            left_here(part_in.at[pl.ds(0, fs - 1)], part_send)
            landed(v1_v, back_recv.at[0])
            landed(vm_v, back_recv.at[1])
            with scope("copy_wait"):
                landed(v_copy, copy_recv)
            with scope("all_wait"):
                landed(bands, all_recv)
                left_here(bands, all_send.at[0])
                left_here(o_all, all_send.at[1])
            with scope("sums_wait"):
                left_here(sums.at[pl.ds(0, 2 * n_sums - 1)], sum_send)
                landed(sums.at[pl.ds(0, n_sums - 1)], sum_recv)

    totals[...] = jnp.sum(sums[pl.ds(0, n_sums)], axis=0)


def finish_kernel(
    fs, tp,
    o_all, o1_all, o2_all, om_all, totals, ofac, omas, om1, om2, v_step, v_new, v_copy, v_first, v_second,
    v_step_out, v_new_out, v_copy_out, v_first_out, v_second_out,
    o_step_out, o_new_out, o_copy_out, o_first_out, o_second_out,
    step_v, new_v, copy_v, first_v, second_v, out_sem,
):
    f = lax.axis_index("fs")
    puts = []

    def put(src, dst):
        copy = pltpu.make_async_copy(src, dst, out_sem.at[len(puts)])
        copy.start()
        puts.append(copy)

    for src, dst in (
        (v_step, v_step_out), (v_new, v_new_out), (v_copy, v_copy_out), (v_first, v_first_out), (v_second, v_second_out),
    ):
        put(src, dst)
    rank, columns = o1_all.shape
    band = rank // fs
    total = jnp.sum(totals[...], axis=1, keepdims=True)
    scale = lax.rsqrt(total / (rank * columns * tp) + 1e-06)

    def moments(proj, first, second):
        scaled = scale * proj
        first_new = 0.9 * first + 0.1 * scaled
        second_new = 0.95 * second + 0.05 * scaled * scaled
        return first_new, second_new

    own_band = pl.ds(pl.multiple_of(f * band, band), band)
    with jax.named_scope("f_own"):
     first_v[...], second_v[...] = moments(o_all[own_band, :], om1[...], om2[...])
    put(first_v, o_first_out)
    put(second_v, o_second_out)
    first_new, second_new = moments(o_all[...], o1_all[...], o2_all[...])
    direction = split(first_new / (jnp.sqrt(second_new) + 1e-08), 0)

    def step_of(rows):
        left = ofac[rows, :]
        return jnp.dot(jnp.concatenate([left, left], axis=1), direction, preferred_element_type=F32)

    count = step_v.shape[0]
    own = pl.ds(pl.multiple_of(f * count, count), count)
    with jax.named_scope("f_step"):
        move = step_of(own)
        step_v[...] = move
    put(step_v, o_step_out)
    new_v[...] = omas[...] - 0.002 * move
    put(new_v, o_new_out)
    for i in range(fs):
        rows = pl.ds(i * count, count)
        copy_v[rows, :] = (om_all[rows, :] - 0.002 * step_of(rows)).astype(BF16)
        put(copy_v.at[rows], o_copy_out.at[rows])
    with jax.named_scope("f_wait"):
        for copy in puts:
            copy.wait()


def on_device(vin, vcot, vfac, vmas, vm1, vm2, heads, ocot, ofac, omas, om1, om2):
    fs = lax.axis_size("fs")
    tp = lax.axis_size("tp")
    rank = vfac.shape[1]
    band = rank // fs
    columns = vin.shape[1]
    tokens, width = heads.shape
    block = 128
    blocks = tokens // block
    stride = 256 if tokens % 256 == 0 else tokens

    def twice(array):
        return pltpu.VMEM((2, *array.shape), array.dtype)

    def like(array):
        return pltpu.VMEM(array.shape, array.dtype)

    def shape(*dims, kind=F32):
        return jax.ShapeDtypeStruct(dims, kind)

    def wide(*dims):
        return pltpu.VMEM(dims, F32)

    def coded():
        return pltpu.VMEM((blocks, rank, block), BF16)

    dma = pltpu.SemaphoreType.DMA
    v_rows, o_rows = vmas.shape[0], omas.shape[0]
    gathered = pl.pallas_call(
        functools.partial(gather_kernel, fs, tp),
        out_shape=(
            shape(rank, columns), shape(rank, columns), shape(rank, columns), shape(fs * o_rows, columns),
            shape(1, columns),
            shape(v_rows, columns), shape(v_rows, columns), shape(fs * v_rows, columns, kind=BF16),
            shape(band, columns), shape(band, columns),
        ),
        in_specs=[HBM] * 12,
        out_specs=(VMEM,) * 10,
        scratch_shapes=[
            like(vfac), like(ofac), twice(vin), like(vcot), pltpu.VMEM((tokens // stride, 2 * rank, stride), BF16),
            like(heads), like(heads), like(ocot), like(ocot), twice(vm1), twice(vm2), twice(vmas), like(omas), like(om1), like(om2),
            wide(blocks, rank, block), wide(blocks, rank, block), wide(blocks, rank, block),
            coded(), coded(), coded(), coded(), wide(1, block),
            wide(2 * rank, columns), wide(2 * rank, columns),
            wide(2, rank, columns), pltpu.VMEM((fs, 2, band, columns), BF16), wide(2, 1, columns),
            pltpu.VMEM((fs, 2, band, columns), BF16), wide(fs, 2, 1, columns), wide(band, columns),
            pltpu.VMEM((fs, 2, band, columns), BF16), wide(2, 1, columns),
            pltpu.VMEM((fs, 2, band, columns), BF16), wide(fs, 2, 1, columns), wide(2, rank, columns),
            pltpu.VMEM((fs, 2, band, columns), BF16), wide(fs, 2, 1, columns),
            pltpu.VMEM((fs, 2, band, columns), BF16), wide(fs, 2, 1, columns),
            wide(fs * tp, 1, columns), wide(fs * tp // 2, 1, columns),
            pltpu.VMEM((fs, o_rows, columns), BF16), wide(fs, 1, columns),
            pltpu.VMEM((o_rows, columns), BF16), wide(1, columns),
            wide(band, columns), wide(band, columns), wide(v_rows, columns), wide(v_rows, columns),
            pltpu.VMEM((fs * v_rows, columns), BF16),
            pltpu.VMEM((fs, 2, v_rows, columns), BF16), wide(fs, 2, 1, columns), wide(fs * v_rows, columns),
            dma((8 + len(growing(blocks)),)), dma((len(growing(blocks)),)), dma, dma((4,)),
            dma, dma((blocks,)), dma, dma((blocks,)),
            dma, dma, dma, dma, dma((2,)), dma, dma, dma, pltpu.SemaphoreType.REGULAR((2,)),
            dma, dma, dma, dma, dma, dma, dma((2,)), dma((2,)), dma,
        ],
        compiler_params=pltpu.CompilerParams(
            collective_id=0, has_side_effects=True, vmem_limit_bytes=32 * 1024 * 1024
        ),
    )(*(pltpu.with_memory_space_constraint(a, pltpu.HBM) for a in (
        vin, vcot, vfac, vmas, vm1, vm2, heads, ocot, ofac, omas, om1, om2
    )))
    o_all, o1_all, o2_all, om_all, totals, *values = gathered

    return pl.pallas_call(
        functools.partial(finish_kernel, fs, tp),
        out_shape=(
            shape(v_rows, columns), shape(v_rows, columns), shape(fs * v_rows, columns, kind=BF16),
            shape(band, columns), shape(band, columns),
            shape(o_rows, columns), shape(o_rows, columns), shape(fs * o_rows, columns, kind=BF16),
            shape(band, columns), shape(band, columns),
        ),
        in_specs=[VMEM] * 14,
        out_specs=(HBM,) * 10,
        scratch_shapes=[
            wide(o_rows, columns), wide(o_rows, columns), pltpu.VMEM((fs * o_rows, columns), BF16),
            wide(band, columns), wide(band, columns), dma((9 + fs,)),
        ],
        compiler_params=pltpu.CompilerParams(vmem_limit_bytes=24 * 1024 * 1024),
    )(o_all, o1_all, o2_all, om_all, totals, ofac, omas, om1, om2, *values)


def solution(mesh):
    both = P("fs", "tp")
    in_specs = (both, P("fs", None), P(), both, both, both, both, both, P(), both, both, both)
    out_specs = (
        both, both, P(None, "tp"), both, both, both, both, P(None, "tp"), both, both,
    )
    return jax.shard_map(
        on_device, mesh=mesh, in_specs=in_specs, out_specs=out_specs, check_vma=False
    )
```
